128 devices in a mesh: sp: 16 (over z, y), tp: 8 (over x, core).
Axes of the slice: x: 4, y: 4, z: 4, core: 2. Of those that a mesh axis runs over, the one named last changes fastest.
Arguments:
- skip_stream_vector: bfloat16 [16384, 2048], P(('sp', 'tp')), may hold values from -6 to 6
- probe_preactivation: bfloat16 [16384, 1024], P('sp', 'tp'), may hold values from -6 to 6
- retention_preactivation: bfloat16 [16384, 1024], P('sp', 'tp'), may hold values from -4.5 to 4.5
- content_vector: bfloat16 [16384, 1024], P('sp', 'tp'), may hold values from -6 to 6
- emission_preactivation: bfloat16 [16384, 1024], P('sp', 'tp'), may hold values from -6 to 6
- retention_slack: float32 [1024], P('tp'), may hold values from 0 to 0.12
- surge_rate: float32 [16384, 1024], P('sp', 'tp'), may hold values from -1.2 to 0
- subspace_scaling_factor: float32 [1024], P('tp'), may hold values from 0.1 to 1.9
- emission_matrix: bfloat16 [1024, 2048], replicated, may hold values from -0.1875 to 0.1875
- mlp_scaling_factor: float32 [2048], replicated, may hold values from 0.1 to 1.9
- switch_matrix: bfloat16 [2048, 5632], P('sp', 'tp'), may hold values from -0.125 to 0.125
- expansion_matrix: bfloat16 [2048, 5632], P('sp', 'tp'), may hold values from -0.125 to 0.125
- contraction_matrix: bfloat16 [5632, 2048], P('tp', 'sp'), may hold values from -0.078125 to 0.078125
Outputs:
- stream_out: bfloat16 [16384, 2048], P(('sp', 'tp'))
The draws below stay inside these ranges and needn't reach their ends.
All inputs are finite; a program needn't handle non-finite values.
Results may differ from the reference program's by a relative error of at most 0.017.
Values may be sent and summed in bfloat16 or wider, within the bound.
A program may use at most 128 MiB of HBM per device.

```python
import jax
import jax.numpy as jnp
from jax import lax

D = 2048
HEADS = 8
HEAD_DIM = 128
FF = 5632
BLOCK = 64
TOK_DEV = 1024
D_HGRN = 1024
TOKENS = 16384
N_TP = 8


def draw_retention_slack(key, part):
    first_key, second_key, third_key = jax.random.split(jax.random.fold_in(key, 11), 3)
    ranking = jax.random.permutation(first_key, HEADS)
    slow_heads = ranking < HEADS // 2
    slow_gap = jnp.exp(jax.random.uniform(second_key, (HEADS, HEAD_DIM), jnp.float32, jnp.log(0.2), jnp.log(0.8))) / TOKENS
    fast_gap = jnp.exp(jax.random.uniform(third_key, (HEADS, HEAD_DIM), jnp.float32, jnp.log(0.04), jnp.log(0.12)))
    chosen = jnp.where(slow_heads[:, None], slow_gap, fast_gap)
    return jnp.minimum(chosen, 0.12).reshape(HEADS * HEAD_DIM)


def draw_retention_preactivation(key, part):
    first_key, second_key = jax.random.split(jax.random.fold_in(key, 21))
    noise = jnp.clip(0.8 * jax.random.normal(first_key, (TOKENS, HEADS * HEAD_DIM), jnp.float32), -3.0, 3.0)
    offsets = jax.random.uniform(second_key, (TOKENS // TOK_DEV, HEADS), jnp.float32, -1.2, 1.2)
    spread_rows = jnp.repeat(jnp.repeat(offsets, TOK_DEV, axis=0), HEAD_DIM, axis=1)
    return (noise + spread_rows).astype(jnp.bfloat16)


def draw_surge_rate(key, part):
    first_key, second_key = jax.random.split(jax.random.fold_in(key, 31))
    positions = jax.random.randint(first_key, (2, HEADS), 0, TOKENS)
    strength = jnp.log(jax.random.uniform(second_key, (2, HEADS), jnp.float32, 0.55, 0.8))
    places = jnp.arange(TOKENS, dtype=jnp.int32)[:, None, None]
    hits = jnp.sum(jnp.where(places == positions[None, :, :], strength[None, :, :], 0.0), axis=1)
    return jnp.repeat(hits, HEAD_DIM, axis=1)


def levels(rng, shape, pieces, low, largest):
    loudness, own = 1.0, jax.random.fold_in(rng, 6)
    for position, shards_of in pieces:
        draws = jnp.exp(jax.random.uniform(jax.random.fold_in(own, position), (shards_of,), jnp.float32, low / len(pieces), largest / len(pieces)))
        loudness = loudness * jnp.repeat(draws, shape[position] // shards_of).reshape([-1 if axis == position else 1 for axis in range(len(shape))])
    return loudness


def normal_values(own_key, extent, width, limit, shards=(), kind=jnp.bfloat16):
    drawn = width * jax.random.normal(own_key, extent, jnp.float32)
    if shards:
        drawn = drawn * levels(own_key, extent, shards, -0.22, 0.18)
    return jnp.clip(drawn, -limit, limit).astype(kind)


def setup_inputs(seed: int = 0) -> dict:
    key_of = jax.random.split(jax.random.key(seed), 14)
    return {
        "skip_stream_vector": normal_values(key_of[0], (TOKENS, D), 1.0, 6.0, ((0, 128),)),
        "probe_preactivation": normal_values(key_of[1], (TOKENS, D_HGRN), 1.0, 6.0, ((0, 16), (1, 8))),
        "retention_preactivation": draw_retention_preactivation(jax.random.fold_in(key_of[13], 71), 0),
        "content_vector": normal_values(key_of[3], (TOKENS, D_HGRN), 1.0, 6.0, ((0, 16), (1, 8))),
        "emission_preactivation": normal_values(key_of[4], (TOKENS, D_HGRN), 1.0, 6.0, ((0, 16), (1, 8))),
        "retention_slack": draw_retention_slack(jax.random.fold_in(key_of[13], 71), 0),
        "surge_rate": draw_surge_rate(jax.random.fold_in(key_of[13], 71), 0),
        "subspace_scaling_factor": jnp.clip(1.0 + 0.18 * jax.random.normal(key_of[7], (D_HGRN,), jnp.float32), 0.1, 1.9),
        "emission_matrix": normal_values(key_of[8], (D_HGRN, D), D_HGRN ** -0.5, 0.1875),
        "mlp_scaling_factor": jnp.clip(1.0 + 0.18 * jax.random.normal(key_of[9], (D,), jnp.float32), 0.1, 1.9),
        "switch_matrix": normal_values(key_of[10], (D, FF), D ** -0.5, 0.125, ((0, 16), (1, 8))),
        "expansion_matrix": normal_values(key_of[11], (D, FF), D ** -0.5, 0.125, ((0, 16), (1, 8))),
        "contraction_matrix": normal_values(key_of[12], (FF, D), FF ** -0.5, 0.078125, ((0, 8), (1, 16))),
    }


EPSILON = 1e-06
TOP_PRECISION = lax.Precision.HIGHEST

def block_step(carry, inputs):
    memory_state, offsets = carry
    query_block, input_gate_block, value_block, log_blk = inputs
    cumulative_decay = jnp.cumsum(log_blk, axis=1)
    length = log_blk.shape[1]
    carried_share = jnp.einsum('eia,eax->eix', query_block * jnp.exp(cumulative_decay), memory_state, precision=TOP_PRECISION)
    middle = cumulative_decay[:, length // 2, :][:, None, :]
    left_side = query_block * jnp.exp(cumulative_decay - middle)
    right_side = input_gate_block * jnp.exp(middle - cumulative_decay)
    causal = (jnp.arange(length)[:, None] >= jnp.arange(length)[None, :])[None, :, :]
    scores = jnp.einsum('htk,hsk->hts', left_side, right_side, precision=TOP_PRECISION)
    scores = jnp.where(causal, scores, 0.0)
    outputs = carried_share + jnp.einsum('hts,hsv->htv', scores, value_block, precision=TOP_PRECISION)
    closing_log_decay = cumulative_decay[:, -1, :]
    updated_memory_state = jnp.exp(closing_log_decay)[:, :, None] * memory_state + jnp.einsum('qnj,qnl->qjl', input_gate_block * jnp.exp(closing_log_decay[:, None, :] - cumulative_decay), value_block, precision=TOP_PRECISION)
    return ((updated_memory_state, offsets + closing_log_decay), (outputs, cumulative_decay + offsets[:, None, :]))

def split_blocks(values, heads_here):
    count = values.shape[0]
    return values.reshape(count // BLOCK, BLOCK, heads_here, HEAD_DIM).transpose(0, 2, 1, 3)

def admission_source_matrix(probe_preactivation, retention_preactivation, content_vector, retention_slack, surge_rate):
    query_act = jax.nn.silu(probe_preactivation.astype(jnp.float32))
    admission_factor = retention_slack[None, :] * jax.nn.sigmoid(-retention_preactivation.astype(jnp.float32))
    retention_logarithm = jnp.log1p(-admission_factor) + surge_rate
    return (query_act, admission_factor, content_vector.astype(jnp.float32), retention_logarithm)

def head_output(outputs, subspace_scaling_factor, emission_preactivation):
    count, heads_here = (outputs.shape[0], outputs.shape[1])
    squares = lax.optimization_barrier(jnp.mean(outputs * outputs, axis=-1, keepdims=True))
    scaled = outputs * lax.rsqrt(squares + EPSILON) * subspace_scaling_factor.reshape(heads_here, HEAD_DIM)
    scaled = scaled.reshape(count, heads_here * HEAD_DIM)
    return (scaled * jax.nn.silu(emission_preactivation.astype(jnp.float32))).astype(jnp.bfloat16)

def row_norm(stream, mlp_scaling_factor):
    streamf = stream.astype(jnp.float32)
    squares = lax.optimization_barrier(jnp.mean(streamf * streamf, axis=-1, keepdims=True))
    return (streamf * lax.rsqrt(squares + EPSILON) * mlp_scaling_factor).astype(jnp.bfloat16)

def reference(skip_stream_vector, probe_preactivation, retention_preactivation, content_vector, emission_preactivation, retention_slack, surge_rate, subspace_scaling_factor, emission_matrix, mlp_scaling_factor, switch_matrix, expansion_matrix, contraction_matrix):
    arranged_sources = admission_source_matrix(probe_preactivation, retention_preactivation, content_vector, retention_slack, surge_rate)
    block_list = tuple((split_blocks(item, HEADS) for item in arranged_sources))
    start_carry = (jnp.zeros((HEADS, HEAD_DIM, HEAD_DIM), jnp.float32), jnp.zeros((HEADS, HEAD_DIM), jnp.float32))
    _, (outputs, _) = lax.scan(block_step, start_carry, block_list)
    outputs = outputs.transpose(0, 2, 1, 3).reshape(TOKENS, HEADS, HEAD_DIM)
    mixed = head_output(outputs, subspace_scaling_factor, emission_preactivation)
    projected = jnp.dot(mixed, emission_matrix, preferred_element_type=jnp.float32)
    stream = (skip_stream_vector.astype(jnp.float32) + projected).astype(jnp.bfloat16)
    normed = row_norm(stream, mlp_scaling_factor)
    gate_proj = jnp.dot(normed, switch_matrix, preferred_element_type=jnp.float32)
    up_proj = jnp.dot(normed, expansion_matrix, preferred_element_type=jnp.float32)
    hidden = (jax.nn.silu(gate_proj) * up_proj).astype(jnp.bfloat16)
    slice_width = FF // N_TP
    summed = jnp.zeros((TOKENS, D), jnp.float32)
    for member in range(N_TP):
        lower = member * slice_width
        partial_sum = jnp.dot(hidden[:, lower:lower + slice_width], contraction_matrix[lower:lower + slice_width], preferred_element_type=jnp.float32)
        summed = summed + partial_sum.astype(jnp.bfloat16).astype(jnp.float32)
    return (stream.astype(jnp.float32) + summed).astype(jnp.bfloat16)
```

```python
import functools

import jax
import jax.numpy as jnp
from jax import lax
from jax.experimental import pallas as pl
from jax.experimental.pallas import tpu as pltpu
from jax.sharding import Mesh
from jax.sharding import PartitionSpec as P

MESH = pl.DeviceIdType.MESH
F32 = jnp.float32
BF16 = jnp.bfloat16
EPSILON = 1e-06
HD = 128
BLOCK = 64
TOK = 1024
ROWS = 512
D = 2048
GU, DOWN = 0, 1
PLUS = {GU: +1, DOWN: -1}


def wrap(value, n=4):
    return lax.rem(value + n, n)


def nt(a, b):
    return lax.dot_general(a, b, (((1,), (1,)), ((), ())), preferred_element_type=F32)


def tn(a, b):
    return lax.dot_general(a, b, (((0,), (0,)), ((), ())), preferred_element_type=F32)


def mm(a, b):
    return jnp.dot(a, b, preferred_element_type=F32)


def kernel(
    skip_ref, q_ref, r_ref, v_ref, e_ref, slack_ref, surge_ref, gain_ref, emission_ref,
    norm_gain_ref, gate_ref, up_ref, down_ref,
    out_ref,
    W, DN, EB, SK, MX, MIXS, STREAM, NORM, ACC, HID, SSQ, RES,
    CUM, IG, DS, SB, ST, STR, SIN, OL, QC, GT,
    OPPS, OPPR, OWN, PN, NBS, NBR,
    w_recv, w_side, w_send, state_recv, state_send, skip_sem, skip_send, mix_recv, mix_send,
    e_sem, opp_recv, opp_send, nb_recv, nb_send,
):
    z, y, x, c = (lax.axis_index(name) for name in ("z", "y", "x", "c"))
    sp = z * 4 + y
    other = 1 - c
    sends = []

    barrier = pltpu.get_barrier_semaphore()
    for k in range(1, 16):
        to = lax.rem(sp + k, 16)
        pl.semaphore_signal(barrier, inc=1, device_id={"z": to // 4, "y": lax.rem(to, 4)}, device_id_type=MESH)
    for step in (1, -1):
        for core in (0, 1):
            pl.semaphore_signal(barrier, inc=1, device_id={"x": wrap(x + step), "c": jnp.int32(core)}, device_id_type=MESH)
    pl.semaphore_signal(barrier, inc=1, device_id={"c": other}, device_id_type=MESH)

    loads = [
        pltpu.make_async_copy(emission_ref.at[:, pl.ds(n * 256, 256)], EB.at[n], e_sem.at[n])
        for n in range(8)
    ]
    for load in loads:
        load.start()

    own_rows = pl.ds(pl.multiple_of(sp * 128, 128), 128)
    for j in range(5):
        W[c, own_rows, j * 256 : j * 256 + 128] = gate_ref[:, j * 128 : (j + 1) * 128]
        W[c, own_rows, j * 256 + 128 : (j + 1) * 256] = up_ref[:, j * 128 : (j + 1) * 128]
    W[c, own_rows, 1280:1408] = jnp.concatenate([gate_ref[:, 640:704], up_ref[:, 640:704]], axis=1)
    DN[c, sp] = down_ref[...]
    SK[x] = skip_ref[...]

    pl.semaphore_wait(barrier, 20)

    AXES = {0: ("y", "z"), 1: ("z", "y")}
    here = {"z": z, "y": y}

    def unit(kind, color, core, rel):
        origin = wrap(z + rel["z"]) * 4 + wrap(y + rel["y"])
        if kind == GU:
            start = pl.multiple_of(origin * 128 + color * 64, 64)
            return W.at[core, pl.ds(start, 64), :]
        return DN.at[core, origin, pl.ds(color * 352, 352), :]

    def number(rel):
        return (rel["z"] % 4) * 4 + rel["y"] % 4

    counter = [0]

    def push(kind, color, rel, axis, step):
        there = dict(rel)
        there[axis] = rel[axis] - step
        ref = unit(kind, color, c, rel)
        copy = pltpu.make_async_remote_copy(
            src_ref=ref, dst_ref=ref,
            send_sem=w_send.at[counter[0]],
            recv_sem=w_recv.at[kind, color, number(there)],
            device_id={axis: wrap(here[axis] + step)}, device_id_type=MESH,
        )
        counter[0] += 1
        copy.start()
        sends.append(copy)

    def side(kind, color, rel):
        ref = unit(kind, color, c, rel)
        copy = pltpu.make_async_remote_copy(
            src_ref=ref, dst_ref=ref,
            send_sem=w_send.at[counter[0]],
            recv_sem=w_side.at[kind, color, number(rel)],
            device_id={"c": other}, device_id_type=MESH,
        )
        counter[0] += 1
        copy.start()
        sends.append(copy)

    def arrived(kind, color, rel):
        ref = unit(kind, color, c, rel)
        pltpu.make_async_copy(ref, ref, w_recv.at[kind, color, number(rel)]).wait()

    def side_arrived(kind, color, rel):
        ref = unit(kind, color, other, rel)
        pltpu.make_async_copy(ref, ref, w_side.at[kind, color, number(rel)]).wait()

    def at(color, first, second):
        one, two = AXES[color]
        return {one: first, two: second}

    def turn(kind, second_offset):
        return PLUS[kind] * {0: 1, -1: -1, 1: 1, 2: -1}[second_offset]

    def stage(kind, n):
        for color in (0, 1):
            one, two = AXES[color]
            own = at(color, 0, 0)
            if n == 0:
                for step in (1, -1):
                    push(kind, color, own, one, step)
            elif n == 1:
                for step in (1, -1):
                    push(kind, color, own, two, step)
                side(kind, color, own)
        if n == 2:
            for f in (-1, 1):
                for color in (0, 1):
                    one, two = AXES[color]
                    rel = at(color, f, 0)
                    arrived(kind, color, rel)
                    if PLUS[kind] == -f:
                        push(kind, color, rel, one, -f)
                    for step in (1, -1):
                        push(kind, color, rel, two, step)
                    side(kind, color, rel)
        if n == 4:
            for color in (0, 1):
                two = AXES[color][1]
                rel = at(color, 2, 0)
                arrived(kind, color, rel)
                for step in (1, -1):
                    push(kind, color, rel, two, step)
                side(kind, color, rel)
        for first in {3: (0,), 5: (-1, 1), 6: (2,)}.get(n, ()):
            for s in (-1, 1):
                for color in (0, 1):
                    two = AXES[color][1]
                    rel = at(color, first, s)
                    arrived(kind, color, rel)
                    if turn(kind, first) == -s:
                        push(kind, color, rel, two, -s)
                    side(kind, color, rel)
        for first in {5: (0,), 6: (-1, 1), 7: (2,)}.get(n, ()):
            for color in (0, 1):
                rel = at(color, first, 2)
                arrived(kind, color, rel)
                side(kind, color, rel)

    stage(GU, 0)

    def skip_copy(source, slot, rows, sem, count, step):
        return pltpu.make_async_remote_copy(
            src_ref=source, dst_ref=SK.at[slot, rows, :],
            send_sem=skip_send.at[count], recv_sem=skip_sem.at[sem],
            device_id={"x": wrap(x + step)}, device_id_type=MESH,
        )

    for i, step in enumerate((1, -1)):
        copy = skip_copy(skip_ref, x, pl.ds(0, 128), i, i, step)
        copy.start()
        sends.append(copy)

    def skip_arrived(slot, rows, sem):
        ref = SK.at[slot, rows, :]
        pltpu.make_async_copy(ref, ref, skip_sem.at[sem]).wait()

    def skip_relay():
        left, right = wrap(x - 1), wrap(x + 1)
        first, second = pl.ds(0, 64), pl.ds(64, 64)
        skip_arrived(left, pl.ds(0, 128), 0)
        copy = skip_copy(SK.at[left, first, :], left, first, 2, 2, 1)
        copy.start()
        sends.append(copy)
        skip_arrived(right, pl.ds(0, 128), 1)
        copy = skip_copy(SK.at[right, second, :], right, second, 3, 3, -1)
        copy.start()
        sends.append(copy)

    i256 = lax.broadcasted_iota(jnp.int32, (256, 256), 0)
    j256 = lax.broadcasted_iota(jnp.int32, (256, 256), 1)
    causal = jnp.logical_and(i256 >= j256, i256 // BLOCK == j256 // BLOCK)
    triangle = jnp.where(causal, 1.0, 0.0).astype(BF16)
    upper_half = lax.broadcasted_iota(jnp.int32, (128, 128), 0) < BLOCK
    closings = []
    for s in range(4):
        rows = slice(s * 256, (s + 1) * 256)
        ig = slack_ref[...] * jax.nn.sigmoid(-r_ref[rows].astype(F32))
        lf = jnp.log1p(-ig) + surge_ref[rows]
        high = lf.astype(BF16)
        rest = lf - high.astype(F32)
        mid = rest.astype(BF16)
        low = (rest - mid.astype(F32)).astype(BF16)
        parts = mm(triangle, jnp.concatenate([high, mid, low], axis=1))
        cum = parts[:, :128] + parts[:, 128:256] + parts[:, 256:]
        CUM[rows] = cum
        IG[rows] = ig
        blocks = cum.reshape(4, BLOCK, HD)
        last = blocks[:, BLOCK - 1 : BLOCK, :]
        closings += [last[b] for b in range(4)]
        keys = (ig * jnp.exp(last - blocks).reshape(256, HD)).astype(BF16)
        for p in range(2):
            pair = keys[p * 128 : (p + 1) * 128]
            none = jnp.zeros_like(pair)
            both = jnp.concatenate(
                [jnp.where(upper_half, pair, none), jnp.where(upper_half, none, pair)], axis=1
            )
            grown = tn(v_ref[s * 256 + p * 128 : s * 256 + (p + 1) * 128], both)
            DS[s * 4 + p * 2] = grown[:, :128]
            DS[s * 4 + p * 2 + 1] = grown[:, 128:]
    state = jnp.zeros((HD, HD), F32)
    passed = jnp.zeros((1, HD), F32)
    offsets = []
    for b in range(16):
        SB[b] = state.astype(BF16)
        offsets.append(passed)
        state = state * jnp.exp(closings[b]) + DS[b]
        passed = passed + closings[b]
    ST[0:128] = state.astype(BF16)
    high = passed.astype(BF16)
    rest = passed - high.astype(F32)
    mid = rest.astype(BF16)
    low = (rest - mid.astype(F32)).astype(BF16)
    which = lax.broadcasted_iota(jnp.int32, (16, HD), 0)
    ST[128:144] = jnp.where(
        which == 0, high.astype(F32), jnp.where(which == 1, mid.astype(F32), jnp.where(which == 2, low.astype(F32), 0.0))
    ).astype(BF16)

    def state_copy(k):
        to = sp + k
        return pltpu.make_async_remote_copy(
            src_ref=ST, dst_ref=STR.at[k - 1],
            send_sem=state_send.at[k - 1], recv_sem=state_recv.at[k - 1],
            device_id={"z": to // 4, "y": lax.rem(to, 4)}, device_id_type=MESH,
        )

    for k in range(15, 0, -1):

        @pl.when(sp + k < 16)
        def _():
            state_copy(k).start()

    stage(GU, 1)

    for s in range(4):
        rows = slice(s * 256, (s + 1) * 256)
        q = q_ref[rows].astype(F32)
        qa = q * jax.nn.sigmoid(q)
        cum = CUM[rows]
        ig = IG[rows]
        blocks = cum.reshape(4, BLOCK, HD)
        middle = blocks[:, BLOCK // 2 : BLOCK // 2 + 1, :]
        centred = (blocks - middle).reshape(256, HD)
        left = (qa * jnp.exp(centred)).astype(BF16)
        right = (ig * jnp.exp(-centred)).astype(BF16)
        scores = jnp.where(causal, nt(left, right), 0.0).astype(BF16)
        local = mm(scores, v_ref[rows])
        faded = qa * jnp.exp(cum)
        before = jnp.concatenate([offsets[s * 4 + b].reshape(1, 1, HD) for b in range(4)], axis=0)
        QC[rows] = (qa * jnp.exp(blocks + before).reshape(256, HD)).astype(BF16)
        faded = faded.astype(BF16)
        for p in range(2):
            pair = faded[p * 128 : (p + 1) * 128]
            none = jnp.zeros_like(pair)
            both = jnp.concatenate(
                [jnp.where(upper_half, pair, none), jnp.where(upper_half, none, pair)], axis=1
            )
            b = s * 4 + p * 2
            carried = nt(both, jnp.concatenate([SB[b], SB[b + 1]], axis=1))
            OL[s * 256 + p * 128 : s * 256 + (p + 1) * 128] = local[p * 128 : (p + 1) * 128] + carried
        emission = e_ref[rows].astype(F32)
        GT[rows] = gain_ref[...] * emission * jax.nn.sigmoid(emission)

    stage(GU, 2)
    skip_relay()

    SIN[0:128] = jnp.zeros((HD, HD), F32)
    SIN[128:136] = jnp.zeros((8, HD), F32)
    for k in range(1, 16):

        @pl.when(sp >= k)
        def _():
            ref = STR.at[k - 1]
            pltpu.make_async_copy(ref, ref, state_recv.at[k - 1]).wait()
            since = SIN[128:129]
            SIN[0:128] = SIN[0:128] + STR[k - 1, 0:128].astype(F32) * jnp.exp(since)
            tail = STR[k - 1, 128:144].astype(F32)
            SIN[128:129] = since + (tail[0:1] + tail[1:2] + tail[2:3])

    incoming = SIN[0:128].astype(BF16)
    for s in range(4):
        rows = slice(s * 256, (s + 1) * 256)
        o = OL[rows] + nt(QC[rows], incoming)
        squares = jnp.mean(o * o, axis=-1, keepdims=True)
        mixed = (o * lax.rsqrt(squares + EPSILON) * GT[rows]).astype(BF16)
        for core in (0, 1):
            MIXS[core, s * 128 : (s + 1) * 128] = mixed[core * 128 : (core + 1) * 128]

    head = x * 2 + c
    MX[head] = MIXS[c]

    def mix_copy(source, slab, sem, count, device):
        copy = pltpu.make_async_remote_copy(
            src_ref=source, dst_ref=MX.at[slab],
            send_sem=mix_send.at[count], recv_sem=mix_recv.at[sem],
            device_id=device, device_id_type=MESH,
        )
        copy.start()
        sends.append(copy)

    count = 0
    for i, step in enumerate((1, -1)):
        for core in (0, 1):
            mix_copy(MIXS.at[core], head, i * 2 + c, count, {"x": wrap(x + step), "c": jnp.int32(core)})
            count += 1
    mix_copy(MIXS.at[other], head, 4, count, {"c": other})
    count += 1

    def mix_arrived(slab, sem):
        ref = MX.at[slab]
        pltpu.make_async_copy(ref, ref, mix_recv.at[sem]).wait()

    stage(GU, 3)
    left, right = wrap(x - 1), wrap(x + 1)
    mix_arrived(left * 2, 0)
    mix_copy(MX.at[left * 2], left * 2, 5, count, {"x": right})
    mix_arrived(right * 2 + 1, 3)
    mix_copy(MX.at[right * 2 + 1], right * 2 + 1, 6, count + 1, {"x": left})
    stage(GU, 4)
    for load in loads:
        load.wait()
    opposite = wrap(x + 2)
    skip_arrived(opposite, pl.ds(0, 64), 2)
    skip_arrived(opposite, pl.ds(64, 64), 3)
    mix_arrived(left * 2 + 1, 1)
    mix_arrived(right * 2, 2)
    mix_arrived(x * 2 + other, 4)
    stage(GU, 5)
    mix_arrived(opposite * 2, 5)
    mix_arrived(opposite * 2 + 1, 6)

    SSQ[...] = jnp.zeros((ROWS, 128), F32)

    def project(n, carry):
        mixed = jnp.concatenate([MX[h] for h in range(8)], axis=1)
        skipped = SK[:, :, pl.ds(pl.multiple_of(n * 256, 256), 256)].reshape(ROWS, 256)
        stream = (skipped.astype(F32) + mm(mixed, EB[n])).astype(BF16)
        STREAM[n] = stream
        wide = stream.astype(F32)
        wide = wide * wide
        SSQ[...] += wide[:, :128] + wide[:, 128:]
        return carry

    lax.fori_loop(0, 8, project, 0)
    scale = lax.rsqrt(jnp.sum(SSQ[...], axis=1, keepdims=True) * (1.0 / D) + EPSILON)

    for n in range(8):
        gain = norm_gain_ref[:, n * 256 : (n + 1) * 256]
        NORM[n] = (STREAM[n].astype(F32) * scale * gain).astype(BF16)

    stage(DOWN, 0)
    stage(DOWN, 1)

    GROUPS = (0, -1, 1, 2)

    def await_sides(kind, dz):
        for dy in (0, -1, 1, 2):
            for color in (0, 1):
                side_arrived(kind, color, {"z": dz, "y": dy})

    lane = lax.broadcasted_iota(jnp.int32, (ROWS, 128), 1)

    def silu(a):
        return a * jax.nn.sigmoid(a)

    def gate_up(index, dz):
        plane = wrap(z + dz)
        deep = pl.ds(pl.multiple_of(plane * 512, 512), 512)

        def take(acc):
            if index == 0:
                return acc
            return None

        def partial(weights):
            rows = jnp.concatenate([NORM[plane * 2], NORM[plane * 2 + 1]], axis=1)
            return mm(rows, weights)

        def tile(t, carry):
            h = t // 5
            columns = pl.ds(pl.multiple_of(lax.rem(t, 5) * 256, 256), 256)
            part = partial(W[h, deep, columns])
            if index > 0:
                part = part + ACC[t]
            if index < 3:
                ACC[t] = part
            else:
                HID[t] = (silu(part[:, :128]) * part[:, 128:]).astype(BF16)
            return carry

        lax.fori_loop(0, 10, tile, 0)
        part = partial(jnp.concatenate([W[0, deep, 1280:1408], W[1, deep, 1280:1408]], axis=1))
        if index > 0:
            part = part + ACC[10]
        if index < 3:
            ACC[10] = part
        else:
            a, b = part[:, :128], part[:, 128:]
            gates = jnp.where(lane < 64, a, pltpu.roll(b, 64, 1))
            ups = jnp.where(lane < 64, pltpu.roll(a, 64, 1), b)
            HID[10] = (silu(gates) * ups).astype(BF16)

    await_sides(GU, 0)
    gate_up(0, 0)
    stage(GU, 6)
    await_sides(GU, -1)
    gate_up(1, -1)
    await_sides(GU, 1)
    stage(GU, 7)
    stage(DOWN, 2)
    gate_up(2, 1)
    await_sides(GU, 2)
    stage(DOWN, 3)
    gate_up(3, 2)
    stage(DOWN, 4)
    stage(DOWN, 5)

    def chunk(xi):
        return pl.ds(pl.multiple_of(xi * 128, 128), 128)

    def down(index, dz):
        plane = wrap(z + dz)

        def pair(p, carry):
            def block(yy):
                at_column = plane * 4 + p * 2 + yy
                return jnp.concatenate(
                    [DN[0, at_column, 0:640], DN[1, at_column, 0:640],
                     DN[0, at_column, 640:704], DN[1, at_column, 640:704]], axis=0,
                )

            weights = jnp.concatenate([block(0), block(1)], axis=1)
            hidden = jnp.concatenate([HID[t] for t in range(11)], axis=1)
            RES[...] = mm(hidden, weights)
            OPPS[index, p] = RES[chunk(opposite)].astype(BF16)
            OWN[index, p] = RES[chunk(x)]
            PN[0, index, p] = RES[chunk(right)]
            PN[1, index, p] = RES[chunk(left)]
            return carry

        lax.fori_loop(0, 2, pair, 0)
        for p, step in enumerate((1, -1)):
            copy = pltpu.make_async_remote_copy(
                src_ref=OPPS.at[index, p], dst_ref=OPPR.at[index, p],
                send_sem=opp_send.at[index, p], recv_sem=opp_recv.at[index, p],
                device_id={"x": wrap(x + step)}, device_id_type=MESH,
            )
            copy.start()
            sends.append(copy)

    def hand_on(index):
        for p, step in enumerate((1, -1)):
            ref = OPPR.at[index, p]
            pltpu.make_async_copy(ref, ref, opp_recv.at[index, p]).wait()
            NBS[p, index, p] = (PN[p, index, p] + OPPR[index, p].astype(F32)).astype(BF16)
            NBS[p, index, 1 - p] = PN[p, index, 1 - p].astype(BF16)
            copy = pltpu.make_async_remote_copy(
                src_ref=NBS.at[p, index], dst_ref=NBR.at[p, index],
                send_sem=nb_send.at[p, index], recv_sem=nb_recv.at[p, index],
                device_id={"x": wrap(x + step)}, device_id_type=MESH,
            )
            copy.start()
            sends.append(copy)

    def finish(index, dz):
        plane = wrap(z + dz)
        for p in range(2):
            ref = NBR.at[p, index]
            pltpu.make_async_copy(ref, ref, nb_recv.at[p, index]).wait()
        for p in range(2):
            summed = OWN[index, p] + NBR[0, index, p].astype(F32) + NBR[1, index, p].astype(F32)
            stream = STREAM[plane * 2 + p, chunk(x)].astype(F32)
            columns = pl.ds(pl.multiple_of(plane * 512 + p * 256, 256), 256)
            out_ref[:, columns] = (stream + summed).astype(BF16)

    await_sides(DOWN, 0)
    down(0, 0)
    stage(DOWN, 6)
    await_sides(DOWN, -1)
    down(1, -1)
    hand_on(0)
    await_sides(DOWN, 1)
    down(2, 1)
    hand_on(1)
    stage(DOWN, 7)
    await_sides(DOWN, 2)
    down(3, 2)
    hand_on(2)
    hand_on(3)
    for index, dz in enumerate(GROUPS):
        finish(index, dz)

    for copy in sends:
        copy.wait_send()
    for k in range(15, 0, -1):

        @pl.when(sp + k < 16)
        def _():
            state_copy(k).wait_send()


def on_device(skip, q, r, v, e, slack, surge, gain, emission, norm_gain, gate, up, down):
    vmem = pl.BlockSpec(memory_space=pltpu.VMEM)
    dma = pltpu.SemaphoreType.DMA
    return pl.pallas_call(
        kernel,
        out_shape=jax.ShapeDtypeStruct((128, D), BF16),
        in_specs=[vmem] * 8 + [pl.BlockSpec(memory_space=pl.ANY)] + [vmem] * 4,
        out_specs=vmem,
        scratch_shapes=[
            pltpu.VMEM((2, D, 1408), BF16),
            pltpu.VMEM((2, 16, 704, 128), BF16),
            pltpu.VMEM((8, 1024, 256), BF16),
            pltpu.VMEM((4, 128, D), BF16),
            pltpu.VMEM((8, ROWS, 128), BF16),
            pltpu.VMEM((2, ROWS, 128), BF16),
            pltpu.VMEM((8, ROWS, 256), BF16),
            pltpu.VMEM((8, ROWS, 256), BF16),
            pltpu.VMEM((11, ROWS, 256), F32),
            pltpu.VMEM((11, ROWS, 128), BF16),
            pltpu.VMEM((ROWS, 128), F32),
            pltpu.VMEM((ROWS, 256), F32),
            pltpu.VMEM((TOK, HD), F32),
            pltpu.VMEM((TOK, HD), F32),
            pltpu.VMEM((16, HD, HD), F32),
            pltpu.VMEM((16, HD, HD), BF16),
            pltpu.VMEM((144, HD), BF16),
            pltpu.VMEM((15, 144, HD), BF16),
            pltpu.VMEM((136, HD), F32),
            pltpu.VMEM((TOK, HD), F32),
            pltpu.VMEM((TOK, HD), BF16),
            pltpu.VMEM((TOK, HD), F32),
            pltpu.VMEM((4, 2, 128, 256), BF16),
            pltpu.VMEM((4, 2, 128, 256), BF16),
            pltpu.VMEM((4, 2, 128, 256), F32),
            pltpu.VMEM((2, 4, 2, 128, 256), F32),
            pltpu.VMEM((2, 4, 2, 128, 256), BF16),
            pltpu.VMEM((2, 4, 2, 128, 256), BF16),
            dma((2, 2, 16)),
            dma((2, 2, 16)),
            dma((124,)),
            dma((15,)),
            dma((15,)),
            dma((4,)),
            dma((4,)),
            dma((7,)),
            dma((7,)),
            dma((8,)),
            dma((4, 2)),
            dma((4, 2)),
            dma((2, 4)),
            dma((2, 4)),
        ],
        compiler_params=pltpu.CompilerParams(
            collective_id=0, has_side_effects=True, vmem_limit_bytes=67043328
        ),
        name="layer",
    )(
        skip, q, r, v, e, slack.reshape(1, -1), surge, gain.reshape(1, -1), emission,
        norm_gain.reshape(1, -1), gate, up, down,
    )


def solution(mesh):
    split = Mesh(mesh.devices.reshape(4, 4, 4, 2), ("z", "y", "x", "c"))
    sp, tp = ("z", "y"), ("x", "c")
    return jax.shard_map(
        on_device,
        mesh=split,
        in_specs=(
            P(sp + tp, None),
            P(sp, tp),
            P(sp, tp),
            P(sp, tp),
            P(sp, tp),
            P(tp),
            P(sp, tp),
            P(tp),
            P(),
            P(),
            P(sp, tp),
            P(sp, tp),
            P(tp, sp),
        ),
        out_specs=P(sp + tp, None),
        check_vma=False,
    )
```

```python
import functools

import jax
import jax.numpy as jnp
from jax import lax
from jax.experimental import pallas as pl
from jax.experimental.pallas import tpu as pltpu
from jax.sharding import Mesh
from jax.sharding import PartitionSpec as P

MESH = pl.DeviceIdType.MESH
F32 = jnp.float32
BF16 = jnp.bfloat16
EPSILON = 1e-06
HD = 128
BLOCK = 64
TOK = 1024
ROWS = 512
D = 2048
GU, DOWN = 0, 1
PLUS = {GU: +1, DOWN: -1}


def wrap(value, n=4):
    return lax.rem(value + n, n)


def nt(a, b):
    return lax.dot_general(a, b, (((1,), (1,)), ((), ())), preferred_element_type=F32)


def tn(a, b):
    return lax.dot_general(a, b, (((0,), (0,)), ((), ())), preferred_element_type=F32)


def mm(a, b):
    return jnp.dot(a, b, preferred_element_type=F32)


def kernel(
    skip_in, q_in, r_in, v_in, e_in, slack_in, surge_in, gain_in, emission_ref,
    norm_gain_in, gate_in, up_in, down_in,
    out_ref,
    skip_ref, QE, RV, slack_ref, surge_ref, gain_ref, norm_gain_ref, OWNED,
    W, DN, EB, SK, MX, MIXS, STREAM, NORM, ACC, HID, SSQ, RES,
    CUM, IG, DS, SB, STR, TOT, OL, QC, GT,
    OPPS, OPPR, OWN, PN, NBS, NBR,
    w_recv, side_gu, side_down, w_send, state_recv, state_send, total_recv, total_send,
    skip_sem, skip_send, mix_recv, mix_send, e_sem, in_sem, opp_recv, opp_send, nb_recv, nb_send,
):
    z, y, x, c = (lax.axis_index(name) for name in ("z", "y", "x", "c"))
    sp = z * 4 + y
    other = 1 - c
    q_ref, e_ref, r_ref, v_ref = QE.at[0], QE.at[1], RV.at[0], RV.at[1]
    gate_ref, up_ref, down_ref = (OWNED.at[i] for i in range(3))

    def arrive(ref, sem):
        pltpu.make_async_copy(ref, ref, sem).wait()

    barrier = pltpu.get_barrier_semaphore()
    for k in range(1, 4):
        pl.semaphore_signal(barrier, inc=1, device_id={"y": wrap(y + k)}, device_id_type=MESH)
        pl.semaphore_signal(barrier, inc=1, device_id={"z": wrap(z + k)}, device_id_type=MESH)
    for step in (1, -1):
        for core in (0, 1):
            pl.semaphore_signal(barrier, inc=1, device_id={"x": wrap(x + step), "c": jnp.int32(core)}, device_id_type=MESH)
    pl.semaphore_signal(barrier, inc=1, device_id={"c": other}, device_id_type=MESH)

    def load(source, target, sem):
        pltpu.make_async_copy(source, target, in_sem.at[sem]).start()

    load(gate_in, gate_ref, 0)
    load(up_in, up_ref, 0)
    load(down_in, down_ref, 0)
    load(r_in, r_ref, 1)
    load(v_in, v_ref, 1)
    load(surge_in, surge_ref, 2)
    load(slack_in, slack_ref, 3)
    load(skip_in, skip_ref, 4)
    load(q_in, q_ref, 5)
    load(e_in, e_ref, 5)
    load(gain_in, gain_ref, 6)
    load(norm_gain_in, norm_gain_ref, 7)
    for n in range(8):
        source = emission_ref.at[:, pl.ds(n * 256, 256)]
        pltpu.make_async_copy(source, EB.at[n], e_sem.at[0]).start()

    arrive(OWNED, in_sem.at[0])
    own_rows = pl.ds(pl.multiple_of(c * D + sp * 128, 128), 128)
    for j in range(5):
        W[own_rows, j * 256 : j * 256 + 128] = gate_ref[j * 128 : (j + 1) * 128].T
        W[own_rows, j * 256 + 128 : (j + 1) * 256] = up_ref[j * 128 : (j + 1) * 128].T
    W[own_rows, 1280:1408] = jnp.concatenate([gate_ref[640:704], up_ref[640:704]], axis=0).T
    DN[c * 16 + sp] = down_ref[...]
    arrive(RV, in_sem.at[1])
    arrive(surge_ref, in_sem.at[2])
    arrive(slack_ref, in_sem.at[3])

    i256 = lax.broadcasted_iota(jnp.int32, (256, 256), 0)
    j256 = lax.broadcasted_iota(jnp.int32, (256, 256), 1)
    causal = jnp.logical_and(i256 >= j256, i256 // BLOCK == j256 // BLOCK)
    triangle = jnp.where(causal, 1.0, 0.0).astype(BF16)
    upper_half = lax.broadcasted_iota(jnp.int32, (128, 128), 0) < BLOCK
    closings = []
    for s in range(4):
        rows = slice(s * 256, (s + 1) * 256)
        ig = slack_ref[...] * jax.nn.sigmoid(-r_ref[rows].astype(F32))
        lf = jnp.log1p(-ig) + surge_ref[rows]
        high = lf.astype(BF16)
        rest = lf - high.astype(F32)
        mid = rest.astype(BF16)
        low = (rest - mid.astype(F32)).astype(BF16)
        parts = mm(triangle, jnp.concatenate([high, mid, low], axis=1))
        cum = parts[:, :128] + parts[:, 128:256] + parts[:, 256:]
        CUM[rows] = cum
        IG[rows] = ig
        blocks = cum.reshape(4, BLOCK, HD)
        last = blocks[:, BLOCK - 1 : BLOCK, :]
        closings += [last[b] for b in range(4)]
        keys = (ig * jnp.exp(last - blocks).reshape(256, HD)).astype(BF16)
        for p in range(2):
            pair = keys[p * 128 : (p + 1) * 128]
            none = jnp.zeros_like(pair)
            both = jnp.concatenate(
                [jnp.where(upper_half, pair, none), jnp.where(upper_half, none, pair)], axis=1
            )
            grown = tn(v_ref[s * 256 + p * 128 : s * 256 + (p + 1) * 128], both)
            DS[s * 4 + p * 2] = grown[:, :128]
            DS[s * 4 + p * 2 + 1] = grown[:, 128:]
    state = jnp.zeros((HD, HD), F32)
    passed = jnp.zeros((1, HD), F32)
    offsets = []
    for b in range(16):
        SB[b] = state.astype(BF16)
        offsets.append(passed)
        state = state * jnp.exp(closings[b]) + DS[b]
        passed = passed + closings[b]
    STR[0, 0:128] = state.astype(BF16)
    which = lax.broadcasted_iota(jnp.int32, (16, HD), 0)

    def spread(value):
        high = value.astype(BF16)
        rest = value - high.astype(F32)
        mid = rest.astype(BF16)
        low = rest - mid.astype(F32)
        rows = jnp.where(which == 2, low, 0.0)
        rows = jnp.where(which == 1, mid.astype(F32), rows)
        return jnp.where(which == 0, high.astype(F32), rows).astype(BF16)

    def joined(rows):
        rows = rows.astype(F32)
        return rows[0:1] + rows[1:2] + rows[2:3]

    STR[0, 128:144] = spread(passed)

    pl.semaphore_wait(barrier, 11)

    for k in range(1, 4):
        pltpu.make_async_remote_copy(
            src_ref=STR.at[0], dst_ref=STR.at[k],
            send_sem=state_send.at[0], recv_sem=state_recv.at[k - 1],
            device_id={"y": wrap(y + k)}, device_id_type=MESH,
        ).start()

    AXES = {0: ("y", "z"), 1: ("z", "y")}
    ORDER = (
        (0, 0), (1, 0), (-1, 0), (0, 1), (0, -1), (2, 0), (0, 2), (1, 1),
        (-1, -1), (1, -1), (-1, 1), (2, 1), (2, -1), (1, 2), (-1, 2), (2, 2),
    )
    here = {"z": z, "y": y}

    def short(offset):
        return (offset + 1) % 4 - 1

    def unit(kind, color, rel):
        origin = wrap(z + rel["z"]) * 4 + wrap(y + rel["y"])
        if kind == GU:
            start = pl.multiple_of(c * D + origin * 128 + color * 64, 64)
            return W.at[pl.ds(start, 64), :]
        return DN.at[c * 16 + origin, pl.ds(color * 352, 352), :]

    def units(kind, count):
        return W.at[pl.ds(0, 64 * count), :] if kind == GU else DN.at[pl.ds(0, count // 2)]

    counts = {GU: 0, DOWN: 0}

    def lot(kind, color, rel):
        one, two = AXES[color]
        first, second = short(rel[one]), short(rel[two])
        if second == 0:
            return {-PLUS[kind]: 0, PLUS[kind]: 1, 2: 3}[first]
        if second == 2:
            return {0: 6, -1: 8, 1: 8, 2: 9}[first]
        return {0: 2, -1: 4, 1: 5, 2: 7}[first]

    LOTS = (2, 2, 4, 2, 4, 4, 2, 4, 4, 2)

    def arrived(kind, number):
        arrive(units(kind, LOTS[number]), w_recv.at[kind, number])

    def start_unit(kind, color, rel, recv_sem, device):
        ref = unit(kind, color, rel)
        pltpu.make_async_remote_copy(
            src_ref=ref, dst_ref=ref, send_sem=w_send.at[kind], recv_sem=recv_sem,
            device_id=device, device_id_type=MESH,
        ).start()
        counts[kind] += 1

    def push(kind, color, rel, axis, step):
        there = dict(rel)
        there[axis] = rel[axis] - step
        sem = w_recv.at[kind, lot(kind, color, there)]
        start_unit(kind, color, rel, sem, {axis: wrap(here[axis] + step)})

    def side(kind, color, rel):
        place = (short(rel["y"]), short(rel["z"]))
        sem = side_gu.at[place[1] % 4] if kind == GU else side_down.at[ORDER.index(place) // 2]
        start_unit(kind, color, rel, sem, {"c": other})

    def at(color, first, second):
        one, two = AXES[color]
        return {one: first, two: second}

    def turn(kind, second_offset):
        return PLUS[kind] * {0: 1, -1: -1, 1: 1, 2: -1}[second_offset]

    def stage(kind, n):
        if n in (0, 1):
            for color in (0, 1):
                for step in (1, -1):
                    push(kind, color, at(color, 0, 0), AXES[color][n], step)
                if n == 1:
                    side(kind, color, at(color, 0, 0))
        if n == 2:
            f = -PLUS[kind]
            arrived(kind, 0)
            for color in (0, 1):
                push(kind, color, at(color, f, 0), AXES[color][0], -f)
        for number, f in {2: ((0, -PLUS[kind]), (1, PLUS[kind])), 4: ((3, 2),)}.get(n, ()):
            if number > 0:
                arrived(kind, number)
            for color in (0, 1):
                for step in (1, -1):
                    push(kind, color, at(color, f, 0), AXES[color][1], step)
                side(kind, color, at(color, f, 0))
        for number, first in {3: ((2, 0),), 5: ((4, -1), (5, 1)), 6: ((7, 2),)}.get(n, ()):
            arrived(kind, number)
            for s in (-1, 1):
                for color in (0, 1):
                    if turn(kind, first) == -s:
                        push(kind, color, at(color, first, s), AXES[color][1], -s)
            for s in (-1, 1):
                for color in (0, 1):
                    side(kind, color, at(color, first, s))
        for number, firsts in {5: ((6, (0,)),), 6: ((8, (-1, 1)),), 7: ((9, (2,)),)}.get(n, ()):
            arrived(kind, number)
            for first in firsts:
                for color in (0, 1):
                    side(kind, color, at(color, first, 2))

    stage(GU, 0)

    def skip_copy(source, slot, rows, sem, step):
        return pltpu.make_async_remote_copy(
            src_ref=source, dst_ref=SK.at[slot, rows, :],
            send_sem=skip_send.at[0], recv_sem=skip_sem.at[sem],
            device_id={"x": wrap(x + step)}, device_id_type=MESH,
        )

    arrive(skip_ref, in_sem.at[4])
    for i, step in enumerate((1, -1)):
        skip_copy(skip_ref, x, pl.ds(0, 128), i, step).start()

    def skip_arrived(slot, rows, sem):
        arrive(SK.at[slot, rows, :], skip_sem.at[sem])

    def skip_relay():
        left, right = wrap(x - 1), wrap(x + 1)
        first, second = pl.ds(0, 64), pl.ds(64, 64)
        skip_arrived(left, pl.ds(0, 128), 0)
        skip_copy(SK.at[left, first, :], left, first, 2, 1).start()
        skip_arrived(right, pl.ds(0, 128), 1)
        skip_copy(SK.at[right, second, :], right, second, 3, -1).start()

    for k in range(1, 4):
        arrive(STR.at[k], state_recv.at[k - 1])
    plane = jnp.zeros((HD, HD), F32)
    plane_log = jnp.zeros((1, HD), F32)
    before, before_log = plane, plane_log
    for yy in range(4):
        slot = wrap(y - yy)
        before = jnp.where(y == yy, plane, before)
        before_log = jnp.where(y == yy, plane_log, before_log)
        log = joined(STR[slot, 128:144])
        plane = plane * jnp.exp(log) + STR[slot, 0:128].astype(F32)
        plane_log = plane_log + log
    TOT[0, 0:128] = plane.astype(BF16)
    TOT[0, 128:144] = spread(plane_log)

    def total_copy(k):
        return pltpu.make_async_remote_copy(
            src_ref=TOT.at[0], dst_ref=TOT.at[k],
            send_sem=total_send.at[k - 1], recv_sem=total_recv.at[k - 1],
            device_id={"z": wrap(z + k)}, device_id_type=MESH,
        )

    for k in range(1, 4):

        @pl.when(z + k < 4)
        def _():
            total_copy(k).start()

        @pl.when(z < k)
        def _():
            TOT[k] = jnp.zeros((144, HD), BF16)

    stage(GU, 1)
    SK[x] = skip_ref[...]
    arrive(QE, in_sem.at[5])
    arrive(gain_ref, in_sem.at[6])
    arrive(norm_gain_ref, in_sem.at[7])
    for s in range(4):
        rows = slice(s * 256, (s + 1) * 256)
        q = q_ref[rows].astype(F32)
        qa = q * jax.nn.sigmoid(q)
        cum = CUM[rows]
        ig = IG[rows]
        blocks = cum.reshape(4, BLOCK, HD)
        middle = blocks[:, BLOCK // 2 : BLOCK // 2 + 1, :]
        centred = (blocks - middle).reshape(256, HD)
        left = (qa * jnp.exp(centred)).astype(BF16)
        right = (ig * jnp.exp(-centred)).astype(BF16)
        scores = jnp.where(causal, nt(left, right), 0.0).astype(BF16)
        local = mm(scores, v_ref[rows])
        faded = qa * jnp.exp(cum)
        faded_by = jnp.concatenate([offsets[s * 4 + b].reshape(1, 1, HD) for b in range(4)], axis=0)
        QC[rows] = (qa * jnp.exp(blocks + faded_by).reshape(256, HD)).astype(BF16)
        faded = faded.astype(BF16)
        for p in range(2):
            pair = faded[p * 128 : (p + 1) * 128]
            none = jnp.zeros_like(pair)
            both = jnp.concatenate(
                [jnp.where(upper_half, pair, none), jnp.where(upper_half, none, pair)], axis=1
            )
            b = s * 4 + p * 2
            carried = nt(both, jnp.concatenate([SB[b], SB[b + 1]], axis=1))
            OL[s * 256 + p * 128 : s * 256 + (p + 1) * 128] = local[p * 128 : (p + 1) * 128] + carried
        emission = e_ref[rows].astype(F32)
        GT[rows] = gain_ref[...] * emission * jax.nn.sigmoid(emission)

    for k in range(1, 4):

        @pl.when(z >= k)
        def _():
            arrive(TOT.at[k], total_recv.at[k - 1])

    since = before_log
    for k in range(1, 4):
        before = before + TOT[k, 0:128].astype(F32) * jnp.exp(since)
        since = since + joined(TOT[k, 128:144])
    incoming = before.astype(BF16)
    for s in range(4):
        rows = slice(s * 256, (s + 1) * 256)
        o = OL[rows] + nt(QC[rows], incoming)
        squares = jnp.mean(o * o, axis=-1, keepdims=True)
        mixed = (o * lax.rsqrt(squares + EPSILON) * GT[rows]).astype(BF16)
        for core in (0, 1):
            MIXS[core, s * 128 : (s + 1) * 128] = mixed[core * 128 : (core + 1) * 128]

    head = x * 2 + c
    MX[head] = MIXS[c]

    def mix_copy(source, slab, sem, device):
        pltpu.make_async_remote_copy(
            src_ref=source, dst_ref=MX.at[slab],
            send_sem=mix_send.at[0], recv_sem=mix_recv.at[sem],
            device_id=device, device_id_type=MESH,
        ).start()

    for i, step in enumerate((1, -1)):
        for core in (0, 1):
            mix_copy(MIXS.at[core], head, i * 2 + c, {"x": wrap(x + step), "c": jnp.int32(core)})
    mix_copy(MIXS.at[other], head, 4, {"c": other})

    def mix_arrived(slab, sem):
        arrive(MX.at[slab], mix_recv.at[sem])

    stage(GU, 2)
    stage(GU, 3)
    skip_relay()
    stage(GU, 4)
    left, right = wrap(x - 1), wrap(x + 1)
    mix_arrived(left * 2, 0)
    mix_copy(MX.at[left * 2], left * 2, 5, {"x": right})
    mix_arrived(right * 2 + 1, 3)
    mix_copy(MX.at[right * 2 + 1], right * 2 + 1, 6, {"x": left})
    stage(GU, 5)
    arrive(EB, e_sem.at[0])
    opposite = wrap(x + 2)
    skip_arrived(opposite, pl.ds(0, 64), 2)
    skip_arrived(opposite, pl.ds(64, 64), 3)
    mix_arrived(left * 2 + 1, 1)
    mix_arrived(right * 2, 2)
    mix_arrived(x * 2 + other, 4)
    mix_arrived(opposite * 2, 5)
    mix_arrived(opposite * 2 + 1, 6)

    SSQ[...] = jnp.zeros((ROWS, 128), F32)

    def project(n, carry):
        mixed = jnp.concatenate([MX[h] for h in range(8)], axis=1)
        skipped = SK[:, :, pl.ds(pl.multiple_of(n * 256, 256), 256)].reshape(ROWS, 256)
        stream = (skipped.astype(F32) + mm(mixed, EB[n])).astype(BF16)
        STREAM[n] = stream
        wide = stream.astype(F32)
        wide = wide * wide
        SSQ[...] += wide[:, :128] + wide[:, 128:]
        return carry

    lax.fori_loop(0, 8, project, 0)
    scale = lax.rsqrt(jnp.sum(SSQ[...], axis=1, keepdims=True) * (1.0 / D) + EPSILON)

    for n in range(8):
        gain = norm_gain_ref[:, n * 256 : (n + 1) * 256]
        NORM[n] = (STREAM[n].astype(F32) * scale * gain).astype(BF16)

    def await_sides(dz):
        arrive(units(GU, 8), side_gu.at[dz % 4])

    lane = lax.broadcasted_iota(jnp.int32, (ROWS, 128), 1)

    def silu(a):
        return a * jax.nn.sigmoid(a)

    def gate_up(planes, first, last):
        places = [wrap(z + dz) for dz in planes]
        rows = [
            [pl.ds(pl.multiple_of(h * D + p * 512, 512), 512) for p in places] for h in (0, 1)
        ]

        def partial(weights):
            normed = [NORM[p * 2 + i] for p in places for i in (0, 1)]
            return mm(jnp.concatenate(normed, axis=1), jnp.concatenate(weights, axis=0))

        def tile(j, carry):
            columns = pl.ds(pl.multiple_of(j * 256, 256), 256)
            for h in (0, 1):
                t = h * 5 + j
                part = partial([W[deep, columns] for deep in rows[h]])
                if not first:
                    part = part + ACC[t]
                if not last:
                    ACC[t] = part
                else:
                    HID[t] = (silu(part[:, :128]) * part[:, 128:]).astype(BF16)
            return carry

        lax.fori_loop(0, 5, tile, 0)
        part = partial(
            [
                jnp.concatenate([W[one, 1280:1408], W[two, 1280:1408]], axis=1)
                for one, two in zip(*rows)
            ]
        )
        if not first:
            part = part + ACC[10]
        if not last:
            ACC[10] = part
        else:
            a, b = part[:, :128], part[:, 128:]
            gates = jnp.where(lane < 64, a, pltpu.roll(b, 64, 1))
            ups = jnp.where(lane < 64, pltpu.roll(a, 64, 1), b)
            HID[10] = (silu(gates) * ups).astype(BF16)

    def chunk(xi):
        return pl.ds(pl.multiple_of(xi * 128, 128), 128)

    def column_of(i):
        dy, dz = ORDER[i]
        return wrap(z + dz) * 4 + wrap(y + dy)

    def down(i):
        arrive(units(DOWN, 4), side_down.at[i])

        def block(at_column):
            one, two = at_column, 16 + at_column
            return jnp.concatenate(
                [DN[one, 0:640], DN[two, 0:640], DN[one, 640:704], DN[two, 640:704]], axis=0
            )

        weights = jnp.concatenate([block(column_of(2 * i)), block(column_of(2 * i + 1))], axis=1)
        hidden = jnp.concatenate([HID[t] for t in range(11)], axis=1)
        res = RES.at[i % 2]
        res[...] = mm(hidden, weights)
        far = res[chunk(opposite)].astype(BF16)
        for half, step in enumerate((1, -1)):
            OPPS[i, half] = far[:, half * 128 : (half + 1) * 128]
            pltpu.make_async_remote_copy(
                src_ref=OPPS.at[i, half], dst_ref=OPPR.at[i, half],
                send_sem=opp_send.at[0], recv_sem=opp_recv.at[i],
                device_id={"x": wrap(x + step)}, device_id_type=MESH,
            ).start()
        OWN[i] = res[chunk(x)]
        PN[0, i] = res[chunk(right)]
        PN[1, i] = res[chunk(left)]

    def hand_on(i):
        arrive(OPPR.at[i], opp_recv.at[i])
        for half, step in enumerate((1, -1)):
            mine = slice(half * 128, (half + 1) * 128)
            rest = slice(128 - half * 128, 256 - half * 128)
            NBS[i, half, :, mine] = (PN[half, i, :, mine] + OPPR[i, half].astype(F32)).astype(BF16)
            NBS[i, half, :, rest] = PN[half, i, :, rest].astype(BF16)
            pltpu.make_async_remote_copy(
                src_ref=NBS.at[i, half], dst_ref=NBR.at[i, half],
                send_sem=nb_send.at[0], recv_sem=nb_recv.at[i],
                device_id={"x": wrap(x + step)}, device_id_type=MESH,
            ).start()

    def finish(i):
        arrive(NBR.at[i], nb_recv.at[i])
        summed = OWN[i] + NBR[i, 0].astype(F32) + NBR[i, 1].astype(F32)
        for half in (0, 1):
            column = column_of(2 * i + half)
            lanes = pl.ds(pl.multiple_of(lax.rem(column, 2) * 128, 128), 128)
            stream = STREAM[column // 2, chunk(x), lanes].astype(F32)
            columns = pl.ds(pl.multiple_of(column * 128, 128), 128)
            out_ref[:, columns] = (stream + summed[:, half * 128 : (half + 1) * 128]).astype(BF16)

    stage(DOWN, 0)
    await_sides(0)
    gate_up((0,), True, False)
    stage(GU, 6)
    stage(DOWN, 1)
    await_sides(-1)
    await_sides(1)
    gate_up((-1, 1), False, False)
    stage(DOWN, 2)
    stage(GU, 7)
    stage(DOWN, 3)
    await_sides(2)
    gate_up((2,), False, True)
    down(0)
    stage(DOWN, 4)
    down(1)
    stage(DOWN, 5)
    down(2)
    hand_on(0)
    down(3)
    hand_on(1)
    down(4)
    stage(DOWN, 6)
    hand_on(2)
    down(5)
    hand_on(3)
    down(6)
    stage(DOWN, 7)
    hand_on(4)
    down(7)
    hand_on(5)
    finish(0)
    finish(1)
    hand_on(6)
    hand_on(7)
    for i in range(2, 8):
        finish(i)

    for kind in (GU, DOWN):
        arrive(units(kind, counts[kind]), w_send.at[kind])
    arrive(STR.at[pl.ds(0, 3)], state_send.at[0])
    arrive(SK.at[pl.ds(0, 3)], skip_send.at[0])
    arrive(MX.at[pl.ds(0, 7)], mix_send.at[0])
    arrive(OPPS, opp_send.at[0])
    arrive(NBS, nb_send.at[0])
    for k in range(1, 4):

        @pl.when(z + k < 4)
        def _():
            total_copy(k).wait_send()


def on_device(skip, q, r, v, e, slack, surge, gain, emission, norm_gain, gate, up, down):
    vmem = pl.BlockSpec(memory_space=pltpu.VMEM)
    dma = pltpu.SemaphoreType.DMA
    return pl.pallas_call(
        kernel,
        out_shape=jax.ShapeDtypeStruct((128, D), BF16),
        in_specs=[pl.BlockSpec(memory_space=pltpu.HBM)] * 13,
        out_specs=vmem,
        scratch_shapes=[
            pltpu.VMEM((128, D), BF16),
            pltpu.VMEM((2, TOK, HD), BF16),
            pltpu.VMEM((2, TOK, HD), BF16),
            pltpu.VMEM((1, HD), F32),
            pltpu.VMEM((TOK, HD), F32),
            pltpu.VMEM((1, HD), F32),
            pltpu.VMEM((1, D), F32),
            pltpu.VMEM((3, 704, 128), BF16),
            pltpu.VMEM((2 * D, 1408), BF16),
            pltpu.VMEM((32, 704, 128), BF16),
            pltpu.VMEM((8, 1024, 256), BF16),
            pltpu.VMEM((4, 128, D), BF16),
            pltpu.VMEM((8, ROWS, 128), BF16),
            pltpu.VMEM((2, ROWS, 128), BF16),
            pltpu.VMEM((8, ROWS, 256), BF16),
            pltpu.VMEM((8, ROWS, 256), BF16),
            pltpu.VMEM((11, ROWS, 256), F32),
            pltpu.VMEM((11, ROWS, 128), BF16),
            pltpu.VMEM((ROWS, 128), F32),
            pltpu.VMEM((2, ROWS, 256), F32),
            pltpu.VMEM((TOK, HD), F32),
            pltpu.VMEM((TOK, HD), F32),
            pltpu.VMEM((16, HD, HD), F32),
            pltpu.VMEM((16, HD, HD), BF16),
            pltpu.VMEM((4, 144, HD), BF16),
            pltpu.VMEM((4, 144, HD), BF16),
            pltpu.VMEM((TOK, HD), F32),
            pltpu.VMEM((TOK, HD), BF16),
            pltpu.VMEM((TOK, HD), F32),
            pltpu.VMEM((8, 2, 128, 128), BF16),
            pltpu.VMEM((8, 2, 128, 128), BF16),
            pltpu.VMEM((8, 128, 256), F32),
            pltpu.VMEM((2, 8, 128, 256), F32),
            pltpu.VMEM((8, 2, 128, 256), BF16),
            pltpu.VMEM((8, 2, 128, 256), BF16),
            dma((2, 10)),
            dma((4,)),
            dma((8,)),
            dma((2,)),
            dma((3,)),
            dma((1,)),
            dma((3,)),
            dma((3,)),
            dma((4,)),
            dma((1,)),
            dma((7,)),
            dma((1,)),
            dma((1,)),
            dma((8,)),
            dma((8,)),
            dma((1,)),
            dma((8,)),
            dma((1,)),
        ],
        compiler_params=pltpu.CompilerParams(
            collective_id=0, has_side_effects=True, vmem_limit_bytes=58000000
        ),
        name="layer",
    )(
        skip, q, r, v, e, slack.reshape(1, -1), surge, gain.reshape(1, -1), emission,
        norm_gain.reshape(1, -1), gate.T, up.T, down,
    )


def solution(mesh):
    split = Mesh(mesh.devices.reshape(4, 4, 4, 2), ("z", "y", "x", "c"))
    sp, tp = ("z", "y"), ("x", "c")
    return jax.shard_map(
        on_device,
        mesh=split,
        in_specs=(
            P(sp + tp, None),
            P(sp, tp),
            P(sp, tp),
            P(sp, tp),
            P(sp, tp),
            P(tp),
            P(sp, tp),
            P(tp),
            P(),
            P(),
            P(sp, tp),
            P(sp, tp),
            P(tp, sp),
        ),
        out_specs=P(sp + tp, None),
        check_vma=False,
    )
```

```python
import functools

import jax
import jax.numpy as jnp
from jax import lax
from jax.experimental import pallas as pl
from jax.experimental.pallas import tpu as pltpu
from jax.sharding import Mesh
from jax.sharding import PartitionSpec as P

MESH = pl.DeviceIdType.MESH
F32 = jnp.float32
BF16 = jnp.bfloat16
EPSILON = 1e-06
HD = 128
BLOCK = 64
TOK = 1024
ROWS = 512
D = 2048
GU, DOWN = 0, 1
PLUS = {GU: +1, DOWN: -1}


def wrap(value, n=4):
    return lax.rem(value + n, n)


def nt(a, b):
    return lax.dot_general(a, b, (((1,), (1,)), ((), ())), preferred_element_type=F32)


def tn(a, b):
    return lax.dot_general(a, b, (((0,), (0,)), ((), ())), preferred_element_type=F32)


def mm(a, b):
    return jnp.dot(a, b, preferred_element_type=F32)


def kernel(
    skip_in, q_in, r_in, v_in, e_in, slack_in, surge_in, gain_in, emission_ref,
    norm_gain_in, gate_in, up_in, down_in,
    out_ref,
    skip_ref, QE, RV, slack_ref, surge_ref, gain_ref, norm_gain_ref, OWNED,
    W, DN, EB, SK, MX, MIXS, STREAM, NORM, ACC, HID, SSQ, RES,
    CUM, IG, DS, SB, STR, TOT, OL, QC, GT,
    OPPS, OPPR, OWN, PN, NBS, NBR,
    w_recv, side_gu, side_down, w_send, state_recv, state_send, total_recv, total_send,
    skip_sem, skip_send, mix_recv, mix_send, e_sem, in_sem, opp_recv, opp_send, nb_recv, nb_send,
):
    z, y, x, c = (lax.axis_index(name) for name in ("z", "y", "x", "c"))
    sp = z * 4 + y
    other = 1 - c
    q_ref, e_ref, r_ref, v_ref = QE.at[0], QE.at[1], RV.at[0], RV.at[1]
    gate_ref, up_ref, down_ref = (OWNED.at[i] for i in range(3))

    def arrive(ref, sem):
        pltpu.make_async_copy(ref, ref, sem).wait()

    barrier = pltpu.get_barrier_semaphore()
    for k in range(1, 4):
        pl.semaphore_signal(barrier, inc=1, device_id={"y": wrap(y + k)}, device_id_type=MESH)
        pl.semaphore_signal(barrier, inc=1, device_id={"z": wrap(z + k)}, device_id_type=MESH)
    for step in (1, -1):
        for core in (0, 1):
            pl.semaphore_signal(barrier, inc=1, device_id={"x": wrap(x + step), "c": jnp.int32(core)}, device_id_type=MESH)
    pl.semaphore_signal(barrier, inc=1, device_id={"c": other}, device_id_type=MESH)

    def load(source, target, sem):
        pltpu.make_async_copy(source, target, in_sem.at[sem]).start()

    load(gate_in, gate_ref, 0)
    load(up_in, up_ref, 0)
    load(down_in, down_ref, 0)
    load(r_in, r_ref, 1)
    load(v_in, v_ref, 1)
    load(surge_in, surge_ref, 2)
    load(slack_in, slack_ref, 3)
    load(skip_in, skip_ref, 4)
    load(q_in, q_ref, 5)
    load(e_in, e_ref, 5)
    load(gain_in, gain_ref, 6)
    load(norm_gain_in, norm_gain_ref, 7)

    arrive(OWNED, in_sem.at[0])
    own_rows = pl.ds(pl.multiple_of(c * D + sp * 128, 128), 128)
    for j in range(5):
        W[own_rows, j * 256 : j * 256 + 128] = gate_ref[j * 128 : (j + 1) * 128].T
        W[own_rows, j * 256 + 128 : (j + 1) * 256] = up_ref[j * 128 : (j + 1) * 128].T
    W[own_rows, 1280:1408] = jnp.concatenate([gate_ref[640:704], up_ref[640:704]], axis=0).T
    DN[c * 16 + sp] = down_ref[...]

    pl.semaphore_wait(barrier, 11)

    AXES = {0: ("y", "z"), 1: ("z", "y")}
    ORDER = (
        (0, 0), (1, 0), (-1, 0), (0, 1), (0, -1), (2, 0), (0, 2), (1, 1),
        (-1, -1), (1, -1), (-1, 1), (2, 1), (2, -1), (1, 2), (-1, 2), (2, 2),
    )
    here = {"z": z, "y": y}

    def short(offset):
        return (offset + 1) % 4 - 1

    def unit(kind, color, rel):
        origin = wrap(z + rel["z"]) * 4 + wrap(y + rel["y"])
        if kind == GU:
            start = pl.multiple_of(c * D + origin * 128 + color * 64, 64)
            return W.at[pl.ds(start, 64), :]
        return DN.at[c * 16 + origin, pl.ds(color * 352, 352), :]

    def units(kind, count):
        return W.at[pl.ds(0, 64 * count), :] if kind == GU else DN.at[pl.ds(0, count // 2)]

    counts = {GU: 0, DOWN: 0}

    def lot(kind, color, rel):
        one, two = AXES[color]
        first, second = short(rel[one]), short(rel[two])
        if second == 0:
            return {-PLUS[kind]: 0, PLUS[kind]: 1, 2: 3}[first]
        if second == 2:
            return {0: 6, -1: 8, 1: 8, 2: 9}[first]
        return {0: 2, -1: 4, 1: 5, 2: 7}[first]

    LOTS = (2, 2, 4, 2, 4, 4, 2, 4, 4, 2)

    def arrived(kind, number):
        arrive(units(kind, LOTS[number]), w_recv.at[kind, number])

    def start_unit(kind, color, rel, recv_sem, device):
        ref = unit(kind, color, rel)
        pltpu.make_async_remote_copy(
            src_ref=ref, dst_ref=ref, send_sem=w_send.at[kind], recv_sem=recv_sem,
            device_id=device, device_id_type=MESH,
        ).start()
        counts[kind] += 1

    def push(kind, color, rel, axis, step):
        there = dict(rel)
        there[axis] = rel[axis] - step
        sem = w_recv.at[kind, lot(kind, color, there)]
        start_unit(kind, color, rel, sem, {axis: wrap(here[axis] + step)})

    def side(kind, color, rel):
        place = (short(rel["y"]), short(rel["z"]))
        sem = side_gu.at[place[1] % 4] if kind == GU else side_down.at[ORDER.index(place) // 2]
        start_unit(kind, color, rel, sem, {"c": other})

    def at(color, first, second):
        one, two = AXES[color]
        return {one: first, two: second}

    def turn(kind, second_offset):
        return PLUS[kind] * {0: 1, -1: -1, 1: 1, 2: -1}[second_offset]

    def stage(kind, n):
        if n in (0, 1):
            for color in (0, 1):
                for step in (1, -1):
                    push(kind, color, at(color, 0, 0), AXES[color][n], step)
                if n == 1:
                    side(kind, color, at(color, 0, 0))
        if n == 2:
            f = -PLUS[kind]
            arrived(kind, 0)
            for color in (0, 1):
                push(kind, color, at(color, f, 0), AXES[color][0], -f)
        for number, f in {2: ((0, -PLUS[kind]), (1, PLUS[kind])), 4: ((3, 2),)}.get(n, ()):
            if number > 0:
                arrived(kind, number)
            for color in (0, 1):
                for step in (1, -1):
                    push(kind, color, at(color, f, 0), AXES[color][1], step)
                side(kind, color, at(color, f, 0))
        for number, first in {3: ((2, 0),), 5: ((4, -1),), 8: ((5, 1),), 6: ((7, 2),)}.get(n, ()):
            arrived(kind, number)
            for s in (-1, 1):
                for color in (0, 1):
                    if turn(kind, first) == -s:
                        push(kind, color, at(color, first, s), AXES[color][1], -s)
            for s in (-1, 1):
                for color in (0, 1):
                    side(kind, color, at(color, first, s))
        for number, firsts in {8: ((6, (0,)),), 6: ((8, (-1, 1)),), 7: ((9, (2,)),)}.get(n, ()):
            arrived(kind, number)
            for first in firsts:
                for color in (0, 1):
                    side(kind, color, at(color, first, 2))

    stage(GU, 0)

    def skip_copy(source, slot, rows, sem, step):
        return pltpu.make_async_remote_copy(
            src_ref=source, dst_ref=SK.at[slot, rows, :],
            send_sem=skip_send.at[0], recv_sem=skip_sem.at[sem],
            device_id={"x": wrap(x + step)}, device_id_type=MESH,
        )

    arrive(skip_ref, in_sem.at[4])
    for i, step in enumerate((1, -1)):
        skip_copy(skip_ref, x, pl.ds(0, 128), i, step).start()

    def skip_arrived(slot, rows, sem):
        arrive(SK.at[slot, rows, :], skip_sem.at[sem])

    def skip_relay(part):
        left, right = wrap(x - 1), wrap(x + 1)
        first, second = pl.ds(part * 32, 32), pl.ds(64 + part * 32, 32)
        if part == 0:
            skip_arrived(left, pl.ds(0, 128), 0)
            skip_arrived(right, pl.ds(0, 128), 1)
        skip_copy(SK.at[left, first, :], left, first, 2 + part, 1).start()
        skip_copy(SK.at[right, second, :], right, second, 2 + part, -1).start()

    i256 = lax.broadcasted_iota(jnp.int32, (256, 256), 0)
    j256 = lax.broadcasted_iota(jnp.int32, (256, 256), 1)
    causal = jnp.logical_and(i256 >= j256, i256 // BLOCK == j256 // BLOCK)
    triangle = jnp.where(causal, 1.0, 0.0).astype(BF16)
    upper_half = lax.broadcasted_iota(jnp.int32, (128, 128), 0) < BLOCK
    arrive(RV, in_sem.at[1])
    arrive(surge_ref, in_sem.at[2])
    arrive(slack_ref, in_sem.at[3])
    closings = []
    for s in range(4):
        rows = slice(s * 256, (s + 1) * 256)
        ig = slack_ref[...] * jax.nn.sigmoid(-r_ref[rows].astype(F32))
        lf = jnp.log1p(-ig) + surge_ref[rows]
        high = lf.astype(BF16)
        rest = lf - high.astype(F32)
        mid = rest.astype(BF16)
        low = (rest - mid.astype(F32)).astype(BF16)
        parts = mm(triangle, jnp.concatenate([high, mid, low], axis=1))
        cum = parts[:, :128] + parts[:, 128:256] + parts[:, 256:]
        CUM[rows] = cum
        IG[rows] = ig
        blocks = cum.reshape(4, BLOCK, HD)
        last = blocks[:, BLOCK - 1 : BLOCK, :]
        closings += [last[b] for b in range(4)]
        keys = (ig * jnp.exp(last - blocks).reshape(256, HD)).astype(BF16)
        for p in range(2):
            pair = keys[p * 128 : (p + 1) * 128]
            none = jnp.zeros_like(pair)
            both = jnp.concatenate(
                [jnp.where(upper_half, pair, none), jnp.where(upper_half, none, pair)], axis=1
            )
            grown = tn(v_ref[s * 256 + p * 128 : s * 256 + (p + 1) * 128], both)
            DS[s * 4 + p * 2] = grown[:, :128]
            DS[s * 4 + p * 2 + 1] = grown[:, 128:]
    state = jnp.zeros((HD, HD), F32)
    passed = jnp.zeros((1, HD), F32)
    offsets = []
    for b in range(16):
        SB[b] = state.astype(BF16)
        offsets.append(passed)
        state = state * jnp.exp(closings[b]) + DS[b]
        passed = passed + closings[b]
    STR[0, 0:128] = state.astype(BF16)
    which = lax.broadcasted_iota(jnp.int32, (16, HD), 0)

    def spread(value):
        high = value.astype(BF16)
        rest = value - high.astype(F32)
        mid = rest.astype(BF16)
        low = rest - mid.astype(F32)
        rows = jnp.where(which == 2, low, 0.0)
        rows = jnp.where(which == 1, mid.astype(F32), rows)
        return jnp.where(which == 0, high.astype(F32), rows).astype(BF16)

    def joined(rows):
        rows = rows.astype(F32)
        return rows[0:1] + rows[1:2] + rows[2:3]

    STR[0, 128:144] = spread(passed)

    for k in range(1, 4):
        pltpu.make_async_remote_copy(
            src_ref=STR.at[0], dst_ref=STR.at[k],
            send_sem=state_send.at[0], recv_sem=state_recv.at[k - 1],
            device_id={"y": wrap(y + k)}, device_id_type=MESH,
        ).start()

    for n in range(8):
        source = emission_ref.at[:, pl.ds(n * 256, 256)]
        pltpu.make_async_copy(source, EB.at[n], e_sem.at[0]).start()
    stage(GU, 1)
    SK[x] = skip_ref[...]
    arrive(QE, in_sem.at[5])
    arrive(gain_ref, in_sem.at[6])
    arrive(norm_gain_ref, in_sem.at[7])
    for s in range(4):
        rows = slice(s * 256, (s + 1) * 256)
        q = q_ref[rows].astype(F32)
        qa = q * jax.nn.sigmoid(q)
        cum = CUM[rows]
        ig = IG[rows]
        blocks = cum.reshape(4, BLOCK, HD)
        middle = blocks[:, BLOCK // 2 : BLOCK // 2 + 1, :]
        centred = (blocks - middle).reshape(256, HD)
        left = (qa * jnp.exp(centred)).astype(BF16)
        right = (ig * jnp.exp(-centred)).astype(BF16)
        scores = jnp.where(causal, nt(left, right), 0.0).astype(BF16)
        local = mm(scores, v_ref[rows])
        faded = qa * jnp.exp(cum)
        faded_by = jnp.concatenate([offsets[s * 4 + b].reshape(1, 1, HD) for b in range(4)], axis=0)
        QC[rows] = (qa * jnp.exp(blocks + faded_by).reshape(256, HD)).astype(BF16)
        faded = faded.astype(BF16)
        for p in range(2):
            pair = faded[p * 128 : (p + 1) * 128]
            none = jnp.zeros_like(pair)
            both = jnp.concatenate(
                [jnp.where(upper_half, pair, none), jnp.where(upper_half, none, pair)], axis=1
            )
            b = s * 4 + p * 2
            carried = nt(both, jnp.concatenate([SB[b], SB[b + 1]], axis=1))
            OL[s * 256 + p * 128 : s * 256 + (p + 1) * 128] = local[p * 128 : (p + 1) * 128] + carried
        emission = e_ref[rows].astype(F32)
        GT[rows] = gain_ref[...] * emission * jax.nn.sigmoid(emission)

    for k in range(1, 4):
        arrive(STR.at[k], state_recv.at[k - 1])
    plane = jnp.zeros((HD, HD), F32)
    plane_log = jnp.zeros((1, HD), F32)
    before, before_log = plane, plane_log
    for yy in range(4):
        slot = wrap(y - yy)
        before = jnp.where(y == yy, plane, before)
        before_log = jnp.where(y == yy, plane_log, before_log)
        log = joined(STR[slot, 128:144])
        plane = plane * jnp.exp(log) + STR[slot, 0:128].astype(F32)
        plane_log = plane_log + log
    TOT[0, 0:128] = plane.astype(BF16)
    TOT[0, 128:144] = spread(plane_log)

    def total_copy(k):
        return pltpu.make_async_remote_copy(
            src_ref=TOT.at[0], dst_ref=TOT.at[k],
            send_sem=total_send.at[k - 1], recv_sem=total_recv.at[k - 1],
            device_id={"z": wrap(z + k)}, device_id_type=MESH,
        )

    for k in range(1, 4):

        @pl.when(z + k < 4)
        def _():
            total_copy(k).start()

        @pl.when(z < k)
        def _():
            TOT[k] = jnp.zeros((144, HD), BF16)

    stage(GU, 2)
    for k in range(1, 4):

        @pl.when(z >= k)
        def _():
            arrive(TOT.at[k], total_recv.at[k - 1])

    since = before_log
    for k in range(1, 4):
        before = before + TOT[k, 0:128].astype(F32) * jnp.exp(since)
        since = since + joined(TOT[k, 128:144])
    incoming = before.astype(BF16)
    for s in range(4):
        rows = slice(s * 256, (s + 1) * 256)
        o = OL[rows] + nt(QC[rows], incoming)
        squares = jnp.mean(o * o, axis=-1, keepdims=True)
        mixed = (o * lax.rsqrt(squares + EPSILON) * GT[rows]).astype(BF16)
        for core in (0, 1):
            MIXS[core, s * 128 : (s + 1) * 128] = mixed[core * 128 : (core + 1) * 128]

    head = x * 2 + c
    MX[head] = MIXS[c]

    def mix_copy(source, slab, sem, device):
        pltpu.make_async_remote_copy(
            src_ref=source, dst_ref=MX.at[slab],
            send_sem=mix_send.at[0], recv_sem=mix_recv.at[sem],
            device_id=device, device_id_type=MESH,
        ).start()

    for i, step in enumerate((1, -1)):
        for core in (0, 1):
            mix_copy(MIXS.at[core], head, i * 2 + c, {"x": wrap(x + step), "c": jnp.int32(core)})
    mix_copy(MIXS.at[other], head, 4, {"c": other})

    def mix_arrived(slab, sem):
        arrive(MX.at[slab], mix_recv.at[sem])

    stage(GU, 3)
    skip_relay(0)
    stage(GU, 4)
    left, right = wrap(x - 1), wrap(x + 1)
    mix_arrived(left * 2, 0)
    mix_copy(MX.at[left * 2], left * 2, 5, {"x": right})
    mix_arrived(right * 2 + 1, 3)
    mix_copy(MX.at[right * 2 + 1], right * 2 + 1, 6, {"x": left})
    skip_relay(1)
    stage(GU, 5)
    arrive(EB, e_sem.at[0])
    opposite = wrap(x + 2)
    mix_arrived(left * 2 + 1, 1)
    mix_arrived(right * 2, 2)
    mix_arrived(x * 2 + other, 4)
    mix_arrived(opposite * 2, 5)
    mix_arrived(opposite * 2 + 1, 6)

    def project(n, carry):
        mixed = jnp.concatenate([MX[h] for h in range(8)], axis=1)
        ACC[n] = mm(mixed, EB[n])
        return carry

    lax.fori_loop(0, 4, project, 0, unroll=True)
    stage(GU, 8)
    lax.fori_loop(4, 8, project, 0, unroll=True)
    stage(DOWN, 0)
    skip_arrived(opposite, pl.ds(0, 64), 2)
    skip_arrived(opposite, pl.ds(64, 64), 3)
    SSQ[...] = jnp.zeros((ROWS, 128), F32)

    def add(n, carry):
        skipped = SK[:, :, pl.ds(pl.multiple_of(n * 256, 256), 256)].reshape(ROWS, 256)
        stream = (skipped.astype(F32) + ACC[n]).astype(BF16)
        STREAM[n] = stream
        wide = stream.astype(F32)
        wide = wide * wide
        SSQ[...] += wide[:, :128] + wide[:, 128:]
        return carry

    lax.fori_loop(0, 8, add, 0)
    scale = lax.rsqrt(jnp.sum(SSQ[...], axis=1, keepdims=True) * (1.0 / D) + EPSILON)

    for n in range(8):
        gain = norm_gain_ref[:, n * 256 : (n + 1) * 256]
        NORM[n] = (STREAM[n].astype(F32) * scale * gain).astype(BF16)

    def await_sides(dz):
        arrive(units(GU, 8), side_gu.at[dz % 4])

    lane = lax.broadcasted_iota(jnp.int32, (ROWS, 128), 1)

    def silu(a):
        return a * jax.nn.sigmoid(a)

    def gate_up(planes, first, last, begin=0, end=6):
        places = [wrap(z + dz) for dz in planes]
        rows = [
            [pl.ds(pl.multiple_of(h * D + p * 512, 512), 512) for p in places] for h in (0, 1)
        ]

        def partial(weights):
            normed = [NORM[p * 2 + i] for p in places for i in (0, 1)]
            return mm(jnp.concatenate(normed, axis=1), jnp.concatenate(weights, axis=0))

        def tile(j, carry):
            columns = pl.ds(pl.multiple_of(j * 256, 256), 256)
            for h in (0, 1):
                t = h * 5 + j
                part = partial([W[deep, columns] for deep in rows[h]])
                if not first:
                    part = part + ACC[t]
                if not last:
                    ACC[t] = part
                else:
                    HID[t] = (silu(part[:, :128]) * part[:, 128:]).astype(BF16)
            return carry

        lax.fori_loop(begin, min(end, 5), tile, 0, unroll=True)
        if end < 6:
            return
        part = partial(
            [
                jnp.concatenate([W[one, 1280:1408], W[two, 1280:1408]], axis=1)
                for one, two in zip(*rows)
            ]
        )
        if not first:
            part = part + ACC[10]
        if not last:
            ACC[10] = part
        else:
            a, b = part[:, :128], part[:, 128:]
            gates = jnp.where(lane < 64, a, pltpu.roll(b, 64, 1))
            ups = jnp.where(lane < 64, pltpu.roll(a, 64, 1), b)
            HID[10] = (silu(gates) * ups).astype(BF16)

    def chunk(xi):
        return pl.ds(pl.multiple_of(xi * 128, 128), 128)

    def column_of(i):
        dy, dz = ORDER[i]
        return wrap(z + dz) * 4 + wrap(y + dy)

    def down(i):
        arrive(units(DOWN, 4), side_down.at[i])

        def block(at_column):
            one, two = at_column, 16 + at_column
            return jnp.concatenate(
                [DN[one, 0:640], DN[two, 0:640], DN[one, 640:704], DN[two, 640:704]], axis=0
            )

        weights = jnp.concatenate([block(column_of(2 * i)), block(column_of(2 * i + 1))], axis=1)
        hidden = jnp.concatenate([HID[t] for t in range(11)], axis=1)
        res = RES.at[i % 2]
        res[...] = mm(hidden, weights)
        far = res[chunk(opposite)].astype(BF16)
        for half, step in enumerate((1, -1)):
            OPPS[i, half] = far[:, half * 128 : (half + 1) * 128]
            pltpu.make_async_remote_copy(
                src_ref=OPPS.at[i, half], dst_ref=OPPR.at[i, half],
                send_sem=opp_send.at[0], recv_sem=opp_recv.at[i],
                device_id={"x": wrap(x + step)}, device_id_type=MESH,
            ).start()
        OWN[i] = res[chunk(x)]
        PN[0, i] = res[chunk(right)]
        PN[1, i] = res[chunk(left)]

    def hand_on(i):
        arrive(OPPR.at[i], opp_recv.at[i])
        for half, step in enumerate((1, -1)):
            mine = slice(half * 128, (half + 1) * 128)
            rest = slice(128 - half * 128, 256 - half * 128)
            NBS[i, half, :, mine] = (PN[half, i, :, mine] + OPPR[i, half].astype(F32)).astype(BF16)
            NBS[i, half, :, rest] = PN[half, i, :, rest].astype(BF16)
            pltpu.make_async_remote_copy(
                src_ref=NBS.at[i, half], dst_ref=NBR.at[i, half],
                send_sem=nb_send.at[0], recv_sem=nb_recv.at[i],
                device_id={"x": wrap(x + step)}, device_id_type=MESH,
            ).start()

    def finish(i):
        arrive(NBR.at[i], nb_recv.at[i])
        summed = OWN[i] + NBR[i, 0].astype(F32) + NBR[i, 1].astype(F32)
        for half in (0, 1):
            column = column_of(2 * i + half)
            lanes = pl.ds(pl.multiple_of(lax.rem(column, 2) * 128, 128), 128)
            stream = STREAM[column // 2, chunk(x), lanes].astype(F32)
            columns = pl.ds(pl.multiple_of(column * 128, 128), 128)
            out_ref[:, columns] = (stream + summed[:, half * 128 : (half + 1) * 128]).astype(BF16)

    stage(DOWN, 1)
    await_sides(0)
    gate_up((0,), True, False)
    stage(GU, 6)
    await_sides(-1)
    await_sides(1)
    stage(DOWN, 2)
    gate_up((-1, 1), False, False, 0, 3)
    stage(DOWN, 3)
    gate_up((-1, 1), False, False, 3, 6)
    stage(GU, 7)
    await_sides(2)
    stage(DOWN, 4)
    gate_up((2,), False, True)
    down(0)
    stage(DOWN, 5)
    down(1)
    stage(DOWN, 8)
    down(2)
    hand_on(0)
    stage(DOWN, 6)
    down(3)
    hand_on(1)
    down(4)
    hand_on(2)
    stage(DOWN, 7)
    down(5)
    hand_on(3)
    down(6)
    hand_on(4)
    down(7)
    hand_on(5)
    finish(0)
    hand_on(6)
    finish(1)
    finish(2)
    hand_on(7)
    finish(3)
    finish(4)
    finish(5)
    finish(6)
    finish(7)

    for kind in (GU, DOWN):
        arrive(units(kind, counts[kind]), w_send.at[kind])
    arrive(STR.at[pl.ds(0, 3)], state_send.at[0])
    arrive(SK.at[pl.ds(0, 3)], skip_send.at[0])
    arrive(MX.at[pl.ds(0, 7)], mix_send.at[0])
    arrive(OPPS, opp_send.at[0])
    arrive(NBS, nb_send.at[0])
    for k in range(1, 4):

        @pl.when(z + k < 4)
        def _():
            total_copy(k).wait_send()


def on_device(skip, q, r, v, e, slack, surge, gain, emission, norm_gain, gate, up, down):
    vmem = pl.BlockSpec(memory_space=pltpu.VMEM)
    dma = pltpu.SemaphoreType.DMA
    return pl.pallas_call(
        kernel,
        out_shape=jax.ShapeDtypeStruct((128, D), BF16),
        in_specs=[pl.BlockSpec(memory_space=pltpu.HBM)] * 13,
        out_specs=vmem,
        scratch_shapes=[
            pltpu.VMEM((128, D), BF16),
            pltpu.VMEM((2, TOK, HD), BF16),
            pltpu.VMEM((2, TOK, HD), BF16),
            pltpu.VMEM((1, HD), F32),
            pltpu.VMEM((TOK, HD), F32),
            pltpu.VMEM((1, HD), F32),
            pltpu.VMEM((1, D), F32),
            pltpu.VMEM((3, 704, 128), BF16),
            pltpu.VMEM((2 * D, 1408), BF16),
            pltpu.VMEM((32, 704, 128), BF16),
            pltpu.VMEM((8, 1024, 256), BF16),
            pltpu.VMEM((4, 128, D), BF16),
            pltpu.VMEM((8, ROWS, 128), BF16),
            pltpu.VMEM((2, ROWS, 128), BF16),
            pltpu.VMEM((8, ROWS, 256), BF16),
            pltpu.VMEM((8, ROWS, 256), BF16),
            pltpu.VMEM((11, ROWS, 256), F32),
            pltpu.VMEM((11, ROWS, 128), BF16),
            pltpu.VMEM((ROWS, 128), F32),
            pltpu.VMEM((2, ROWS, 256), F32),
            pltpu.VMEM((TOK, HD), F32),
            pltpu.VMEM((TOK, HD), F32),
            pltpu.VMEM((16, HD, HD), F32),
            pltpu.VMEM((16, HD, HD), BF16),
            pltpu.VMEM((4, 144, HD), BF16),
            pltpu.VMEM((4, 144, HD), BF16),
            pltpu.VMEM((TOK, HD), F32),
            pltpu.VMEM((TOK, HD), BF16),
            pltpu.VMEM((TOK, HD), F32),
            pltpu.VMEM((8, 2, 128, 128), BF16),
            pltpu.VMEM((8, 2, 128, 128), BF16),
            pltpu.VMEM((8, 128, 256), F32),
            pltpu.VMEM((2, 8, 128, 256), F32),
            pltpu.VMEM((8, 2, 128, 256), BF16),
            pltpu.VMEM((8, 2, 128, 256), BF16),
            dma((2, 10)),
            dma((4,)),
            dma((8,)),
            dma((2,)),
            dma((3,)),
            dma((1,)),
            dma((3,)),
            dma((3,)),
            dma((4,)),
            dma((1,)),
            dma((7,)),
            dma((1,)),
            dma((1,)),
            dma((8,)),
            dma((8,)),
            dma((1,)),
            dma((8,)),
            dma((1,)),
        ],
        compiler_params=pltpu.CompilerParams(
            collective_id=0, has_side_effects=True, vmem_limit_bytes=54000000
        ),
        name="layer",
    )(
        *(
            pltpu.with_memory_space_constraint(a, pltpu.HBM)
            for a in (skip, q, r, v, e, slack.reshape(1, -1), surge, gain.reshape(1, -1), emission,
                      norm_gain.reshape(1, -1), gate.T, up.T, down)
        )
    )


def solution(mesh):
    split = Mesh(mesh.devices.reshape(4, 4, 4, 2), ("z", "y", "x", "c"))
    sp, tp = ("z", "y"), ("x", "c")
    return jax.shard_map(
        on_device,
        mesh=split,
        in_specs=(
            P(sp + tp, None),
            P(sp, tp),
            P(sp, tp),
            P(sp, tp),
            P(sp, tp),
            P(tp),
            P(sp, tp),
            P(tp),
            P(),
            P(),
            P(sp, tp),
            P(sp, tp),
            P(tp, sp),
        ),
        out_specs=P(sp + tp, None),
        check_vma=False,
    )
```

```python
import functools

import jax
import jax.numpy as jnp
from jax import lax
from jax.experimental import pallas as pl
from jax.experimental.pallas import tpu as pltpu
from jax.sharding import Mesh
from jax.sharding import PartitionSpec as P

MESH = pl.DeviceIdType.MESH
F32 = jnp.float32
BF16 = jnp.bfloat16
EPSILON = 1e-06
HD = 128
BLOCK = 64
TOK = 1024
ROWS = 512
D = 2048
GU, DOWN = 0, 1


def wrap(value, n=4):
    return lax.rem(value + n, n)


def nt(a, b):
    return lax.dot_general(a, b, (((1,), (1,)), ((), ())), preferred_element_type=F32)


def tn(a, b):
    return lax.dot_general(a, b, (((0,), (0,)), ((), ())), preferred_element_type=F32)


def mm(a, b):
    return jnp.dot(a, b, preferred_element_type=F32)


def kernel(
    skip_in, q_in, r_in, v_in, e_in, slack_in, surge_in, gain_in, emission_ref,
    norm_gain_in, gate_in, up_in, down_in,
    out_ref,
    skip_ref, QE, RV, slack_ref, surge_ref, gain_ref, norm_gain_ref, OWNED,
    W, DN, EB, SK, MX, MIXS, STREAM, NORM, ACC, HID, SSQ, RES,
    CUM, IG, DS, SB, STR, TOT, OL, QC, GT,
    OPPS, OPPR, OWN, PN, NBS, NBR,
    w_recv, side_gu, side_down, w_send, state_recv, state_send, total_recv, total_send,
    skip_sem, skip_send, mix_recv, mix_send, e_sem, in_sem, opp_recv, opp_send, nb_recv, nb_send,
):
    z, y, x, c = (lax.axis_index(name) for name in ("z", "y", "x", "c"))
    sp = z * 4 + y
    other = 1 - c
    q_ref, e_ref, r_ref, v_ref = QE.at[0], QE.at[1], RV.at[0], RV.at[1]
    gate_ref, up_ref, down_ref = (OWNED.at[i] for i in range(3))

    def arrive(ref, sem):
        pltpu.make_async_copy(ref, ref, sem).wait()

    barrier = pltpu.get_barrier_semaphore()
    for k in range(1, 4):
        pl.semaphore_signal(barrier, inc=1, device_id={"y": wrap(y + k)}, device_id_type=MESH)
        pl.semaphore_signal(barrier, inc=1, device_id={"z": wrap(z + k)}, device_id_type=MESH)
    for step in (1, -1):
        for core in (0, 1):
            pl.semaphore_signal(barrier, inc=1, device_id={"x": wrap(x + step), "c": jnp.int32(core)}, device_id_type=MESH)
    pl.semaphore_signal(barrier, inc=1, device_id={"c": other}, device_id_type=MESH)

    def load(source, target, sem):
        pltpu.make_async_copy(source, target, in_sem.at[sem]).start()

    load(gate_in, gate_ref, 0)
    load(up_in, up_ref, 0)
    load(down_in, down_ref, 0)
    load(r_in, r_ref, 1)
    load(v_in, v_ref, 1)
    load(surge_in, surge_ref, 2)
    load(slack_in, slack_ref, 3)
    load(skip_in, skip_ref, 4)
    load(q_in, q_ref, 5)
    load(e_in, e_ref, 5)
    load(gain_in, gain_ref, 6)
    load(norm_gain_in, norm_gain_ref, 7)

    arrive(OWNED, in_sem.at[0])
    own_rows = pl.ds(pl.multiple_of(c * D + sp * 128, 128), 128)
    for j in range(5):
        W[own_rows, j * 256 : j * 256 + 128] = gate_ref[j * 128 : (j + 1) * 128].T
        W[own_rows, j * 256 + 128 : (j + 1) * 256] = up_ref[j * 128 : (j + 1) * 128].T
    W[own_rows, 1280:1408] = jnp.concatenate([gate_ref[640:704], up_ref[640:704]], axis=0).T
    DN[c * 16 + sp] = down_ref[...]

    pl.semaphore_wait(barrier, 11)

    AXES = {0: ("y", "z"), 1: ("z", "y")}
    ORDER = (
        (0, 0), (1, 0), (-1, 0), (0, 1), (0, -1), (2, 0), (0, 2), (1, 1),
        (-1, -1), (1, -1), (-1, 1), (2, 1), (2, -1), (1, 2), (-1, 2), (2, 2),
    )
    here = {"z": z, "y": y}

    def short(offset):
        return (offset + 1) % 4 - 1

    def unit(kind, color, rel, half):
        origin = wrap(z + rel["z"]) * 4 + wrap(y + rel["y"])
        size, skipped = (1, 0) if half is None else (2, half)
        if kind == GU:
            start = pl.multiple_of(c * D + origin * 128 + color * 64 + skipped * 32, 32)
            return W.at[pl.ds(start, 64 // size), :]
        return DN.at[c * 16 + origin, pl.ds(color * 352 + skipped * 176, 352 // size), :]

    def units(kind, count):
        return W.at[pl.ds(0, 64 * count), :] if kind == GU else DN.at[pl.ds(0, count // 2)]

    counts = {GU: 0, DOWN: 0}

    def lot(color, rel):
        one, two = AXES[color]
        first, second = short(rel[one]), short(rel[two])
        if second == 0:
            return {-1: 0, 1: 1, 2: 3}[first]
        if second == 2:
            return {0: 6, -1: 8, 1: 8, 2: 9}[first]
        return {0: 2, -1: 4, 1: 5, 2: 7}[first]

    LOTS = (2, 2, 4, 2, 4, 4, 2, 4, 4, 2)

    def arrived(kind, number):
        arrive(units(kind, LOTS[number]), w_recv.at[kind, number])

    def start_unit(kind, color, rel, recv_sem, device, half=None):
        ref = unit(kind, color, rel, half)
        pltpu.make_async_remote_copy(
            src_ref=ref, dst_ref=ref, send_sem=w_send.at[kind], recv_sem=recv_sem,
            device_id=device, device_id_type=MESH,
        ).start()
        counts[kind] += 2 if half is None else 1

    def push(kind, color, rel, axis, step, half=None):
        there = dict(rel)
        there[axis] = rel[axis] - step
        sem = w_recv.at[kind, lot(color, there)]
        start_unit(kind, color, rel, sem, {axis: wrap(here[axis] + step)}, half)

    def side(kind, color, rel):
        place = (short(rel["y"]), short(rel["z"]))
        sem = side_gu.at[place[1] % 4] if kind == GU else side_down.at[ORDER.index(place) // 2]
        start_unit(kind, color, rel, sem, {"c": other})

    def at(color, first, second):
        one, two = AXES[color]
        return {one: first, two: second}

    def stage(kind, n):
        if n in (0, 1):
            for color in (0, 1):
                for step in (1, -1):
                    push(kind, color, at(color, 0, 0), AXES[color][n], step)
                if n == 1:
                    side(kind, color, at(color, 0, 0))
        if n == 2:
            arrived(kind, 0)
            arrived(kind, 1)
            for f in (-1, 1):
                for color in (0, 1):
                    push(kind, color, at(color, f, 0), AXES[color][0], -f, (f + 1) // 2)
        if n == 4:
            arrived(kind, 3)
        for f in {2: (-1, 1), 4: (2,)}.get(n, ()):
            for color in (0, 1):
                for step in (1, -1):
                    push(kind, color, at(color, f, 0), AXES[color][1], step)
                side(kind, color, at(color, f, 0))
        for number, first in {3: ((2, 0),), 5: ((4, -1),), 8: ((5, 1),), 6: ((7, 2),)}.get(n, ()):
            arrived(kind, number)
            for s in (-1, 1):
                for color in (0, 1):
                    push(kind, color, at(color, first, s), AXES[color][1], -s, (s + 1) // 2)
            for s in (-1, 1):
                for color in (0, 1):
                    side(kind, color, at(color, first, s))
        for number, firsts in {8: ((6, (0,)),), 6: ((8, (-1, 1)),), 7: ((9, (2,)),)}.get(n, ()):
            arrived(kind, number)
            for first in firsts:
                for color in (0, 1):
                    side(kind, color, at(color, first, 2))

    stage(GU, 0)

    def skip_copy(source, slot, rows, sem, step):
        return pltpu.make_async_remote_copy(
            src_ref=source, dst_ref=SK.at[slot, rows, :],
            send_sem=skip_send.at[0], recv_sem=skip_sem.at[sem],
            device_id={"x": wrap(x + step)}, device_id_type=MESH,
        )

    arrive(skip_ref, in_sem.at[4])
    for i, step in enumerate((1, -1)):
        skip_copy(skip_ref, x, pl.ds(0, 128), i, step).start()

    def skip_arrived(slot, rows, sem):
        arrive(SK.at[slot, rows, :], skip_sem.at[sem])

    def skip_relay(part):
        left, right = wrap(x - 1), wrap(x + 1)
        first, second = pl.ds(part * 32, 32), pl.ds(64 + part * 32, 32)
        if part == 0:
            skip_arrived(left, pl.ds(0, 128), 0)
            skip_arrived(right, pl.ds(0, 128), 1)
        skip_copy(SK.at[left, first, :], left, first, 2 + part, 1).start()
        skip_copy(SK.at[right, second, :], right, second, 2 + part, -1).start()

    i256 = lax.broadcasted_iota(jnp.int32, (256, 256), 0)
    j256 = lax.broadcasted_iota(jnp.int32, (256, 256), 1)
    causal = jnp.logical_and(i256 >= j256, i256 // BLOCK == j256 // BLOCK)
    triangle = jnp.where(causal, 1.0, 0.0).astype(BF16)
    upper_half = lax.broadcasted_iota(jnp.int32, (128, 128), 0) < BLOCK
    arrive(RV, in_sem.at[1])
    arrive(surge_ref, in_sem.at[2])
    arrive(slack_ref, in_sem.at[3])
    closings = []
    for s in range(4):
        rows = slice(s * 256, (s + 1) * 256)
        ig = slack_ref[...] * jax.nn.sigmoid(-r_ref[rows].astype(F32))
        lf = jnp.log1p(-ig) + surge_ref[rows]
        high = lf.astype(BF16)
        rest = lf - high.astype(F32)
        mid = rest.astype(BF16)
        low = (rest - mid.astype(F32)).astype(BF16)
        parts = mm(triangle, jnp.concatenate([high, mid, low], axis=1))
        cum = parts[:, :128] + parts[:, 128:256] + parts[:, 256:]
        CUM[rows] = cum
        IG[rows] = ig
        blocks = cum.reshape(4, BLOCK, HD)
        last = blocks[:, BLOCK - 1 : BLOCK, :]
        closings += [last[b] for b in range(4)]
        keys = (ig * jnp.exp(last - blocks).reshape(256, HD)).astype(BF16)
        for p in range(2):
            pair = keys[p * 128 : (p + 1) * 128]
            none = jnp.zeros_like(pair)
            both = jnp.concatenate(
                [jnp.where(upper_half, pair, none), jnp.where(upper_half, none, pair)], axis=1
            )
            grown = tn(v_ref[s * 256 + p * 128 : s * 256 + (p + 1) * 128], both)
            DS[s * 4 + p * 2] = grown[:, :128]
            DS[s * 4 + p * 2 + 1] = grown[:, 128:]
    state = jnp.zeros((HD, HD), F32)
    passed = jnp.zeros((1, HD), F32)
    offsets = []
    for b in range(16):
        SB[b] = state.astype(BF16)
        offsets.append(passed)
        state = state * jnp.exp(closings[b]) + DS[b]
        passed = passed + closings[b]
    STR[0, 0:128] = state.astype(BF16)
    which = lax.broadcasted_iota(jnp.int32, (16, HD), 0)

    def spread(value):
        high = value.astype(BF16)
        rest = value - high.astype(F32)
        mid = rest.astype(BF16)
        low = rest - mid.astype(F32)
        rows = jnp.where(which == 2, low, 0.0)
        rows = jnp.where(which == 1, mid.astype(F32), rows)
        return jnp.where(which == 0, high.astype(F32), rows).astype(BF16)

    def joined(rows):
        rows = rows.astype(F32)
        return rows[0:1] + rows[1:2] + rows[2:3]

    STR[0, 128:144] = spread(passed)

    for k in range(1, 4):
        pltpu.make_async_remote_copy(
            src_ref=STR.at[0], dst_ref=STR.at[k],
            send_sem=state_send.at[0], recv_sem=state_recv.at[k - 1],
            device_id={"y": wrap(y + k)}, device_id_type=MESH,
        ).start()

    for n in range(8):
        source = emission_ref.at[:, pl.ds(n * 256, 256)]
        pltpu.make_async_copy(source, EB.at[n], e_sem.at[0]).start()
    stage(GU, 1)
    SK[x] = skip_ref[...]
    arrive(QE, in_sem.at[5])
    arrive(gain_ref, in_sem.at[6])
    arrive(norm_gain_ref, in_sem.at[7])
    for s in range(4):
        rows = slice(s * 256, (s + 1) * 256)
        q = q_ref[rows].astype(F32)
        qa = q * jax.nn.sigmoid(q)
        cum = CUM[rows]
        ig = IG[rows]
        blocks = cum.reshape(4, BLOCK, HD)
        middle = blocks[:, BLOCK // 2 : BLOCK // 2 + 1, :]
        centred = (blocks - middle).reshape(256, HD)
        left = (qa * jnp.exp(centred)).astype(BF16)
        right = (ig * jnp.exp(-centred)).astype(BF16)
        scores = jnp.where(causal, nt(left, right), 0.0).astype(BF16)
        local = mm(scores, v_ref[rows])
        faded = qa * jnp.exp(cum)
        faded_by = jnp.concatenate([offsets[s * 4 + b].reshape(1, 1, HD) for b in range(4)], axis=0)
        QC[rows] = (qa * jnp.exp(blocks + faded_by).reshape(256, HD)).astype(BF16)
        faded = faded.astype(BF16)
        for p in range(2):
            pair = faded[p * 128 : (p + 1) * 128]
            none = jnp.zeros_like(pair)
            both = jnp.concatenate(
                [jnp.where(upper_half, pair, none), jnp.where(upper_half, none, pair)], axis=1
            )
            b = s * 4 + p * 2
            carried = nt(both, jnp.concatenate([SB[b], SB[b + 1]], axis=1))
            OL[s * 256 + p * 128 : s * 256 + (p + 1) * 128] = local[p * 128 : (p + 1) * 128] + carried
        emission = e_ref[rows].astype(F32)
        GT[rows] = gain_ref[...] * emission * jax.nn.sigmoid(emission)

    for k in range(1, 4):
        arrive(STR.at[k], state_recv.at[k - 1])
    plane = jnp.zeros((HD, HD), F32)
    plane_log = jnp.zeros((1, HD), F32)
    before, before_log = plane, plane_log
    for yy in range(4):
        slot = wrap(y - yy)
        before = jnp.where(y == yy, plane, before)
        before_log = jnp.where(y == yy, plane_log, before_log)
        log = joined(STR[slot, 128:144])
        plane = plane * jnp.exp(log) + STR[slot, 0:128].astype(F32)
        plane_log = plane_log + log
    TOT[0, 0:128] = plane.astype(BF16)
    TOT[0, 128:144] = spread(plane_log)

    def total_copy(k):
        return pltpu.make_async_remote_copy(
            src_ref=TOT.at[0], dst_ref=TOT.at[k],
            send_sem=total_send.at[k - 1], recv_sem=total_recv.at[k - 1],
            device_id={"z": wrap(z + k)}, device_id_type=MESH,
        )

    for k in range(1, 4):

        @pl.when(z + k < 4)
        def _():
            total_copy(k).start()

        @pl.when(z < k)
        def _():
            TOT[k] = jnp.zeros((144, HD), BF16)

    stage(GU, 2)
    for k in range(1, 4):

        @pl.when(z >= k)
        def _():
            arrive(TOT.at[k], total_recv.at[k - 1])

    since = before_log
    for k in range(1, 4):
        before = before + TOT[k, 0:128].astype(F32) * jnp.exp(since)
        since = since + joined(TOT[k, 128:144])
    incoming = before.astype(BF16)
    for s in range(4):
        rows = slice(s * 256, (s + 1) * 256)
        o = OL[rows] + nt(QC[rows], incoming)
        squares = jnp.mean(o * o, axis=-1, keepdims=True)
        mixed = (o * lax.rsqrt(squares + EPSILON) * GT[rows]).astype(BF16)
        for core in (0, 1):
            MIXS[core, s * 128 : (s + 1) * 128] = mixed[core * 128 : (core + 1) * 128]

    head = x * 2 + c
    MX[head] = MIXS[c]

    def mix_copy(source, slab, sem, device):
        pltpu.make_async_remote_copy(
            src_ref=source, dst_ref=MX.at[slab],
            send_sem=mix_send.at[0], recv_sem=mix_recv.at[sem],
            device_id=device, device_id_type=MESH,
        ).start()

    for i, step in enumerate((1, -1)):
        for core in (0, 1):
            mix_copy(MIXS.at[core], head, i * 2 + c, {"x": wrap(x + step), "c": jnp.int32(core)})
    mix_copy(MIXS.at[other], head, 4, {"c": other})

    def mix_arrived(slab, sem):
        arrive(MX.at[slab], mix_recv.at[sem])

    stage(GU, 3)
    skip_relay(0)
    stage(GU, 4)
    left, right = wrap(x - 1), wrap(x + 1)
    mix_arrived(left * 2, 0)
    mix_copy(MX.at[left * 2], left * 2, 5, {"x": right})
    mix_arrived(right * 2 + 1, 3)
    mix_copy(MX.at[right * 2 + 1], right * 2 + 1, 6, {"x": left})
    skip_relay(1)
    stage(GU, 5)
    stage(GU, 8)
    arrive(EB, e_sem.at[0])
    opposite = wrap(x + 2)
    mix_arrived(left * 2 + 1, 1)
    mix_arrived(right * 2, 2)
    mix_arrived(x * 2 + other, 4)
    mix_arrived(opposite * 2, 5)
    mix_arrived(opposite * 2 + 1, 6)

    def project(n, carry):
        mixed = jnp.concatenate([MX[h] for h in range(8)], axis=1)
        ACC[n] = mm(mixed, EB[n])
        return carry

    lax.fori_loop(0, 4, project, 0, unroll=True)
    lax.fori_loop(4, 8, project, 0, unroll=True)
    stage(DOWN, 0)
    skip_arrived(opposite, pl.ds(0, 64), 2)
    skip_arrived(opposite, pl.ds(64, 64), 3)
    SSQ[...] = jnp.zeros((ROWS, 128), F32)

    def add(n, carry):
        skipped = SK[:, :, pl.ds(pl.multiple_of(n * 256, 256), 256)].reshape(ROWS, 256)
        stream = (skipped.astype(F32) + ACC[n]).astype(BF16)
        STREAM[n] = stream
        wide = stream.astype(F32)
        wide = wide * wide
        SSQ[...] += wide[:, :128] + wide[:, 128:]
        return carry

    lax.fori_loop(0, 8, add, 0)
    scale = lax.rsqrt(jnp.sum(SSQ[...], axis=1, keepdims=True) * (1.0 / D) + EPSILON)

    for n in range(8):
        gain = norm_gain_ref[:, n * 256 : (n + 1) * 256]
        NORM[n] = (STREAM[n].astype(F32) * scale * gain).astype(BF16)

    def await_sides(dz):
        arrive(units(GU, 8), side_gu.at[dz % 4])

    lane = lax.broadcasted_iota(jnp.int32, (ROWS, 128), 1)

    def silu(a):
        return a * jax.nn.sigmoid(a)

    def gate_up(planes, first, last, begin=0, end=6):
        places = [wrap(z + dz) for dz in planes]
        rows = [
            [pl.ds(pl.multiple_of(h * D + p * 512, 512), 512) for p in places] for h in (0, 1)
        ]

        def partial(weights):
            normed = [NORM[p * 2 + i] for p in places for i in (0, 1)]
            return mm(jnp.concatenate(normed, axis=1), jnp.concatenate(weights, axis=0))

        def tile(j, carry):
            columns = pl.ds(pl.multiple_of(j * 256, 256), 256)
            for h in (0, 1):
                t = h * 5 + j
                part = partial([W[deep, columns] for deep in rows[h]])
                if not first:
                    part = part + ACC[t]
                if not last:
                    ACC[t] = part
                else:
                    HID[t] = (silu(part[:, :128]) * part[:, 128:]).astype(BF16)
            return carry

        lax.fori_loop(begin, min(end, 5), tile, 0, unroll=True)
        if end < 6:
            return
        part = partial(
            [
                jnp.concatenate([W[one, 1280:1408], W[two, 1280:1408]], axis=1)
                for one, two in zip(*rows)
            ]
        )
        if not first:
            part = part + ACC[10]
        if not last:
            ACC[10] = part
        else:
            a, b = part[:, :128], part[:, 128:]
            gates = jnp.where(lane < 64, a, pltpu.roll(b, 64, 1))
            ups = jnp.where(lane < 64, pltpu.roll(a, 64, 1), b)
            HID[10] = (silu(gates) * ups).astype(BF16)

    def chunk(xi):
        return pl.ds(pl.multiple_of(xi * 128, 128), 128)

    def column_of(i):
        dy, dz = ORDER[i]
        return wrap(z + dz) * 4 + wrap(y + dy)

    def down(i):
        arrive(units(DOWN, 4), side_down.at[i])

        def block(at_column):
            one, two = at_column, 16 + at_column
            return jnp.concatenate(
                [DN[one, 0:640], DN[two, 0:640], DN[one, 640:704], DN[two, 640:704]], axis=0
            )

        weights = jnp.concatenate([block(column_of(2 * i)), block(column_of(2 * i + 1))], axis=1)
        hidden = jnp.concatenate([HID[t] for t in range(11)], axis=1)
        res = RES.at[i % 2]
        res[...] = mm(hidden, weights)
        far = res[chunk(opposite)].astype(BF16)
        for half, step in enumerate((1, -1)):
            OPPS[i, half] = far[:, half * 128 : (half + 1) * 128]
            pltpu.make_async_remote_copy(
                src_ref=OPPS.at[i, half], dst_ref=OPPR.at[i, half],
                send_sem=opp_send.at[0], recv_sem=opp_recv.at[i],
                device_id={"x": wrap(x + step)}, device_id_type=MESH,
            ).start()
        OWN[i] = res[chunk(x)]
        PN[0, i] = res[chunk(right)]
        PN[1, i] = res[chunk(left)]

    def hand_on(i):
        arrive(OPPR.at[i], opp_recv.at[i])
        for half, step in enumerate((1, -1)):
            mine = slice(half * 128, (half + 1) * 128)
            rest = slice(128 - half * 128, 256 - half * 128)
            NBS[i, half, :, mine] = (PN[half, i, :, mine] + OPPR[i, half].astype(F32)).astype(BF16)
            NBS[i, half, :, rest] = PN[half, i, :, rest].astype(BF16)
            pltpu.make_async_remote_copy(
                src_ref=NBS.at[i, half], dst_ref=NBR.at[i, half],
                send_sem=nb_send.at[0], recv_sem=nb_recv.at[i],
                device_id={"x": wrap(x + step)}, device_id_type=MESH,
            ).start()

    def finish(i):
        arrive(NBR.at[i], nb_recv.at[i])
        summed = OWN[i] + NBR[i, 0].astype(F32) + NBR[i, 1].astype(F32)
        for half in (0, 1):
            column = column_of(2 * i + half)
            lanes = pl.ds(pl.multiple_of(lax.rem(column, 2) * 128, 128), 128)
            stream = STREAM[column // 2, chunk(x), lanes].astype(F32)
            columns = pl.ds(pl.multiple_of(column * 128, 128), 128)
            out_ref[:, columns] = (stream + summed[:, half * 128 : (half + 1) * 128]).astype(BF16)

    stage(DOWN, 1)
    await_sides(0)
    gate_up((0,), True, False)
    stage(GU, 6)
    await_sides(-1)
    await_sides(1)
    stage(DOWN, 2)
    gate_up((-1, 1), False, False, 0, 3)
    stage(DOWN, 3)
    gate_up((-1, 1), False, False, 3, 6)
    stage(GU, 7)
    await_sides(2)
    stage(DOWN, 4)
    gate_up((2,), False, True)
    down(0)
    stage(DOWN, 5)
    down(1)
    stage(DOWN, 8)
    down(2)
    hand_on(0)
    stage(DOWN, 6)
    down(3)
    hand_on(1)
    down(4)
    hand_on(2)
    stage(DOWN, 7)
    down(5)
    hand_on(3)
    down(6)
    hand_on(4)
    down(7)
    hand_on(5)
    finish(0)
    hand_on(6)
    finish(1)
    finish(2)
    hand_on(7)
    finish(3)
    finish(4)
    finish(5)
    finish(6)
    finish(7)

    for kind in (GU, DOWN):
        arrive(units(kind, counts[kind] // 2), w_send.at[kind])
    arrive(STR.at[pl.ds(0, 3)], state_send.at[0])
    arrive(SK.at[pl.ds(0, 3)], skip_send.at[0])
    arrive(MX.at[pl.ds(0, 7)], mix_send.at[0])
    arrive(OPPS, opp_send.at[0])
    arrive(NBS, nb_send.at[0])
    for k in range(1, 4):

        @pl.when(z + k < 4)
        def _():
            total_copy(k).wait_send()


def on_device(skip, q, r, v, e, slack, surge, gain, emission, norm_gain, gate, up, down):
    vmem = pl.BlockSpec(memory_space=pltpu.VMEM)
    dma = pltpu.SemaphoreType.DMA
    return pl.pallas_call(
        kernel,
        out_shape=jax.ShapeDtypeStruct((128, D), BF16),
        in_specs=[pl.BlockSpec(memory_space=pltpu.HBM)] * 13,
        out_specs=vmem,
        scratch_shapes=[
            pltpu.VMEM((128, D), BF16),
            pltpu.VMEM((2, TOK, HD), BF16),
            pltpu.VMEM((2, TOK, HD), BF16),
            pltpu.VMEM((1, HD), F32),
            pltpu.VMEM((TOK, HD), F32),
            pltpu.VMEM((1, HD), F32),
            pltpu.VMEM((1, D), F32),
            pltpu.VMEM((3, 704, 128), BF16),
            pltpu.VMEM((2 * D, 1408), BF16),
            pltpu.VMEM((32, 704, 128), BF16),
            pltpu.VMEM((8, 1024, 256), BF16),
            pltpu.VMEM((4, 128, D), BF16),
            pltpu.VMEM((8, ROWS, 128), BF16),
            pltpu.VMEM((2, ROWS, 128), BF16),
            pltpu.VMEM((8, ROWS, 256), BF16),
            pltpu.VMEM((8, ROWS, 256), BF16),
            pltpu.VMEM((11, ROWS, 256), F32),
            pltpu.VMEM((11, ROWS, 128), BF16),
            pltpu.VMEM((ROWS, 128), F32),
            pltpu.VMEM((2, ROWS, 256), F32),
            pltpu.VMEM((TOK, HD), F32),
            pltpu.VMEM((TOK, HD), F32),
            pltpu.VMEM((16, HD, HD), F32),
            pltpu.VMEM((16, HD, HD), BF16),
            pltpu.VMEM((4, 144, HD), BF16),
            pltpu.VMEM((4, 144, HD), BF16),
            pltpu.VMEM((TOK, HD), F32),
            pltpu.VMEM((TOK, HD), BF16),
            pltpu.VMEM((TOK, HD), F32),
            pltpu.VMEM((8, 2, 128, 128), BF16),
            pltpu.VMEM((8, 2, 128, 128), BF16),
            pltpu.VMEM((8, 128, 256), F32),
            pltpu.VMEM((2, 8, 128, 256), F32),
            pltpu.VMEM((8, 2, 128, 256), BF16),
            pltpu.VMEM((8, 2, 128, 256), BF16),
            dma((2, 10)),
            dma((4,)),
            dma((8,)),
            dma((2,)),
            dma((3,)),
            dma((1,)),
            dma((3,)),
            dma((3,)),
            dma((4,)),
            dma((1,)),
            dma((7,)),
            dma((1,)),
            dma((1,)),
            dma((8,)),
            dma((8,)),
            dma((1,)),
            dma((8,)),
            dma((1,)),
        ],
        compiler_params=pltpu.CompilerParams(
            collective_id=0, has_side_effects=True, vmem_limit_bytes=54000000
        ),
        name="layer",
    )(
        *(
            pltpu.with_memory_space_constraint(a, pltpu.HBM)
            for a in (skip, q, r, v, e, slack.reshape(1, -1), surge, gain.reshape(1, -1), emission,
                      norm_gain.reshape(1, -1), gate.T, up.T, down)
        )
    )


def solution(mesh):
    split = Mesh(mesh.devices.reshape(4, 4, 4, 2), ("z", "y", "x", "c"))
    sp, tp = ("z", "y"), ("x", "c")
    return jax.shard_map(
        on_device,
        mesh=split,
        in_specs=(
            P(sp + tp, None),
            P(sp, tp),
            P(sp, tp),
            P(sp, tp),
            P(sp, tp),
            P(tp),
            P(sp, tp),
            P(tp),
            P(),
            P(),
            P(sp, tp),
            P(sp, tp),
            P(tp, sp),
        ),
        out_specs=P(sp + tp, None),
        check_vma=False,
    )
```

```python
import functools

import jax
import jax.numpy as jnp
from jax import lax
from jax.experimental import pallas as pl
from jax.experimental.pallas import tpu as pltpu
from jax.sharding import Mesh
from jax.sharding import PartitionSpec as P

MESH = pl.DeviceIdType.MESH
F32 = jnp.float32
BF16 = jnp.bfloat16
EPSILON = 1e-06
HD = 128
BLOCK = 64
TOK = 1024
ROWS = 512
D = 2048
GU, DOWN = 0, 1


def wrap(value, n=4):
    return lax.rem(value + n, n)


def nt(a, b):
    return lax.dot_general(a, b, (((1,), (1,)), ((), ())), preferred_element_type=F32)


def tn(a, b):
    return lax.dot_general(a, b, (((0,), (0,)), ((), ())), preferred_element_type=F32)


def mm(a, b):
    return jnp.dot(a, b, preferred_element_type=F32)


def kernel(
    skip_in, q_in, r_in, v_in, e_in, slack_in, surge_in, gain_in, emission_ref,
    norm_gain_in, gate_in, up_in, down_in,
    out_ref,
    skip_ref, QE, RV, slack_ref, surge_ref, gain_ref, norm_gain_ref, OWNED,
    W, DN, EB, SK, MX, MIXS, STREAM, NORM, ACC, HID, SSQ, RES,
    CUM, IG, DS, SB, STR, TOT, OL, QC, GT,
    OPPS, OPPR, OWN, PN, NBS, NBR,
    w_recv, side_gu, side_down, w_send, state_recv, state_send, total_recv, total_send,
    skip_sem, skip_send, mix_recv, mix_send, e_sem, in_sem, opp_recv, opp_send, nb_recv, nb_send,
):
    z, y, x, c = (lax.axis_index(name) for name in ("z", "y", "x", "c"))
    sp = z * 4 + y
    other = 1 - c
    q_ref, e_ref, r_ref, v_ref = QE.at[0], QE.at[1], RV.at[0], RV.at[1]
    gate_ref, up_ref, down_ref = (OWNED.at[i] for i in range(3))

    def arrive(ref, sem):
        pltpu.make_async_copy(ref, ref, sem).wait()

    barrier = pltpu.get_barrier_semaphore()
    for k in range(1, 4):
        pl.semaphore_signal(barrier, inc=1, device_id={"y": wrap(y + k)}, device_id_type=MESH)
        pl.semaphore_signal(barrier, inc=1, device_id={"z": wrap(z + k)}, device_id_type=MESH)
    for step in (1, -1):
        for core in (0, 1):
            pl.semaphore_signal(barrier, inc=1, device_id={"x": wrap(x + step), "c": jnp.int32(core)}, device_id_type=MESH)
    pl.semaphore_signal(barrier, inc=1, device_id={"c": other}, device_id_type=MESH)

    def load(source, target, sem):
        pltpu.make_async_copy(source, target, in_sem.at[sem]).start()

    load(gate_in, gate_ref, 0)
    load(up_in, up_ref, 0)
    load(down_in, down_ref, 0)
    load(r_in, r_ref, 1)
    load(v_in, v_ref, 1)
    load(surge_in, surge_ref, 2)
    load(slack_in, slack_ref, 3)
    load(skip_in, skip_ref, 4)
    load(q_in, q_ref, 5)
    load(e_in, e_ref, 5)
    load(gain_in, gain_ref, 6)
    load(norm_gain_in, norm_gain_ref, 7)

    arrive(OWNED, in_sem.at[0])
    own_rows = pl.ds(pl.multiple_of(c * D + sp * 128, 128), 128)
    for j in range(5):
        W[own_rows, j * 256 : j * 256 + 128] = gate_ref[j * 128 : (j + 1) * 128].T
        W[own_rows, j * 256 + 128 : (j + 1) * 256] = up_ref[j * 128 : (j + 1) * 128].T
    W[own_rows, 1280:1408] = jnp.concatenate([gate_ref[640:704], up_ref[640:704]], axis=0).T
    DN[c * 16 + sp] = down_ref[...]

    pl.semaphore_wait(barrier, 11)

    AXES = {0: ("y", "z"), 1: ("z", "y")}
    ORDER = (
        (0, 0), (1, 0), (-1, 0), (0, 1), (0, -1), (2, 0), (0, 2), (1, 1),
        (-1, -1), (1, -1), (-1, 1), (2, 1), (2, -1), (1, 2), (-1, 2), (2, 2),
    )
    here = {"z": z, "y": y}

    def short(offset):
        return (offset + 1) % 4 - 1

    def unit(kind, color, rel, half):
        origin = wrap(z + rel["z"]) * 4 + wrap(y + rel["y"])
        size, skipped = (1, 0) if half is None else (2, half)
        if kind == GU:
            start = pl.multiple_of(c * D + origin * 128 + color * 64 + skipped * 32, 32)
            return W.at[pl.ds(start, 64 // size), :]
        return DN.at[c * 16 + origin, pl.ds(color * 352 + skipped * 176, 352 // size), :]

    def units(kind, count):
        return W.at[pl.ds(0, 64 * count), :] if kind == GU else DN.at[pl.ds(0, count // 2)]

    counts = {GU: 0, DOWN: 0}

    def lot(color, rel):
        one, two = AXES[color]
        first, second = short(rel[one]), short(rel[two])
        if second == 0:
            return {-1: 0, 1: 1, 2: 3}[first]
        if second == 2:
            return {0: 6, -1: 8, 1: 8, 2: 9}[first]
        return {0: 2, -1: 4, 1: 5, 2: 7}[first]

    LOTS = (2, 2, 4, 2, 4, 4, 2, 4, 4, 2)

    def arrived(kind, number):
        arrive(units(kind, LOTS[number]), w_recv.at[kind, number])

    def start_unit(kind, color, rel, recv_sem, device, half=None):
        ref = unit(kind, color, rel, half)
        pltpu.make_async_remote_copy(
            src_ref=ref, dst_ref=ref, send_sem=w_send.at[kind], recv_sem=recv_sem,
            device_id=device, device_id_type=MESH,
        ).start()
        counts[kind] += 2 if half is None else 1

    def push(kind, color, rel, axis, step, half=None):
        there = dict(rel)
        there[axis] = rel[axis] - step
        sem = w_recv.at[kind, lot(color, there)]
        start_unit(kind, color, rel, sem, {axis: wrap(here[axis] + step)}, half)

    def side(kind, color, rel):
        place = (short(rel["y"]), short(rel["z"]))
        sem = side_gu.at[place[1] % 4] if kind == GU else side_down.at[ORDER.index(place) // 2]
        start_unit(kind, color, rel, sem, {"c": other})

    def at(color, first, second):
        one, two = AXES[color]
        return {one: first, two: second}

    def stage(kind, n):
        if n in (0, 1):
            for color in (0, 1):
                for step in (1, -1):
                    push(kind, color, at(color, 0, 0), AXES[color][n], step)
                if n == 1:
                    side(kind, color, at(color, 0, 0))
        if n == 2:
            arrived(kind, 0)
            arrived(kind, 1)
            for f in (-1, 1):
                for color in (0, 1):
                    push(kind, color, at(color, f, 0), AXES[color][0], -f, (f + 1) // 2)
        if n == 4:
            arrived(kind, 3)
        for f in {2: (-1, 1), 4: (2,)}.get(n, ()):
            for color in (0, 1):
                for step in (1, -1):
                    push(kind, color, at(color, f, 0), AXES[color][1], step)
                side(kind, color, at(color, f, 0))
        for number, first in {3: ((2, 0),), 5: ((4, -1),), 8: ((5, 1),), 6: ((7, 2),)}.get(n, ()):
            arrived(kind, number)
            for s in (-1, 1):
                for color in (0, 1):
                    push(kind, color, at(color, first, s), AXES[color][1], -s, (s + 1) // 2)
            for s in (-1, 1):
                for color in (0, 1):
                    side(kind, color, at(color, first, s))
        for number, firsts in {8: ((6, (0,)),), 6: ((8, (-1, 1)),), 7: ((9, (2,)),)}.get(n, ()):
            arrived(kind, number)
            for first in firsts:
                for color in (0, 1):
                    side(kind, color, at(color, first, 2))

    stage(GU, 0)

    def skip_copy(source, slot, rows, sem, step):
        return pltpu.make_async_remote_copy(
            src_ref=source, dst_ref=SK.at[slot, rows, :],
            send_sem=skip_send.at[0], recv_sem=skip_sem.at[sem],
            device_id={"x": wrap(x + step)}, device_id_type=MESH,
        )

    arrive(skip_ref, in_sem.at[4])
    for i, step in enumerate((1, -1)):
        skip_copy(skip_ref, x, pl.ds(0, 128), i, step).start()

    def skip_arrived(slot, rows, sem):
        arrive(SK.at[slot, rows, :], skip_sem.at[sem])

    def skip_relay(part):
        left, right = wrap(x - 1), wrap(x + 1)
        first, second = pl.ds(part * 32, 32), pl.ds(64 + part * 32, 32)
        if part == 0:
            skip_arrived(left, pl.ds(0, 128), 0)
            skip_arrived(right, pl.ds(0, 128), 1)
        skip_copy(SK.at[left, first, :], left, first, 2 + part, 1).start()
        skip_copy(SK.at[right, second, :], right, second, 2 + part, -1).start()

    i256 = lax.broadcasted_iota(jnp.int32, (256, 256), 0)
    j256 = lax.broadcasted_iota(jnp.int32, (256, 256), 1)
    causal = jnp.logical_and(i256 >= j256, i256 // BLOCK == j256 // BLOCK)
    triangle = jnp.where(causal, 1.0, 0.0).astype(BF16)
    upper_half = lax.broadcasted_iota(jnp.int32, (128, 128), 0) < BLOCK
    arrive(RV, in_sem.at[1])
    arrive(surge_ref, in_sem.at[2])
    arrive(slack_ref, in_sem.at[3])
    closings = []
    for s in range(4):
        rows = slice(s * 256, (s + 1) * 256)
        ig = slack_ref[...] * jax.nn.sigmoid(-r_ref[rows].astype(F32))
        lf = jnp.log1p(-ig) + surge_ref[rows]
        high = lf.astype(BF16)
        rest = lf - high.astype(F32)
        mid = rest.astype(BF16)
        low = (rest - mid.astype(F32)).astype(BF16)
        parts = mm(triangle, jnp.concatenate([high, mid, low], axis=1))
        cum = parts[:, :128] + parts[:, 128:256] + parts[:, 256:]
        CUM[rows] = cum
        IG[rows] = ig
        blocks = cum.reshape(4, BLOCK, HD)
        last = blocks[:, BLOCK - 1 : BLOCK, :]
        closings += [last[b] for b in range(4)]
        keys = (ig * jnp.exp(last - blocks).reshape(256, HD)).astype(BF16)
        for p in range(2):
            pair = keys[p * 128 : (p + 1) * 128]
            none = jnp.zeros_like(pair)
            both = jnp.concatenate(
                [jnp.where(upper_half, pair, none), jnp.where(upper_half, none, pair)], axis=1
            )
            grown = tn(v_ref[s * 256 + p * 128 : s * 256 + (p + 1) * 128], both)
            DS[s * 4 + p * 2] = grown[:, :128]
            DS[s * 4 + p * 2 + 1] = grown[:, 128:]
    state = jnp.zeros((HD, HD), F32)
    passed = jnp.zeros((1, HD), F32)
    offsets = []
    for b in range(16):
        SB[b] = state.astype(BF16)
        offsets.append(passed)
        state = state * jnp.exp(closings[b]) + DS[b]
        passed = passed + closings[b]
    STR[0, 0:128] = state.astype(BF16)
    which = lax.broadcasted_iota(jnp.int32, (16, HD), 0)

    def spread(value):
        high = value.astype(BF16)
        rest = value - high.astype(F32)
        mid = rest.astype(BF16)
        low = rest - mid.astype(F32)
        rows = jnp.where(which == 2, low, 0.0)
        rows = jnp.where(which == 1, mid.astype(F32), rows)
        return jnp.where(which == 0, high.astype(F32), rows).astype(BF16)

    def joined(rows):
        rows = rows.astype(F32)
        return rows[0:1] + rows[1:2] + rows[2:3]

    STR[0, 128:144] = spread(passed)

    for k in range(1, 4):
        pltpu.make_async_remote_copy(
            src_ref=STR.at[0], dst_ref=STR.at[k],
            send_sem=state_send.at[0], recv_sem=state_recv.at[k - 1],
            device_id={"y": wrap(y + k)}, device_id_type=MESH,
        ).start()

    for n in range(8):
        source = emission_ref.at[:, pl.ds(n * 256, 256)]
        pltpu.make_async_copy(source, EB.at[n], e_sem.at[0]).start()
    stage(GU, 1)
    SK[x] = skip_ref[...]
    arrive(QE, in_sem.at[5])
    arrive(gain_ref, in_sem.at[6])
    arrive(norm_gain_ref, in_sem.at[7])
    for s in range(4):
        rows = slice(s * 256, (s + 1) * 256)
        q = q_ref[rows].astype(F32)
        qa = q * jax.nn.sigmoid(q)
        cum = CUM[rows]
        ig = IG[rows]
        blocks = cum.reshape(4, BLOCK, HD)
        middle = blocks[:, BLOCK // 2 : BLOCK // 2 + 1, :]
        centred = (blocks - middle).reshape(256, HD)
        left = (qa * jnp.exp(centred)).astype(BF16)
        right = (ig * jnp.exp(-centred)).astype(BF16)
        scores = jnp.where(causal, nt(left, right), 0.0).astype(BF16)
        local = mm(scores, v_ref[rows])
        faded = qa * jnp.exp(cum)
        faded_by = jnp.concatenate([offsets[s * 4 + b].reshape(1, 1, HD) for b in range(4)], axis=0)
        QC[rows] = (qa * jnp.exp(blocks + faded_by).reshape(256, HD)).astype(BF16)
        faded = faded.astype(BF16)
        for p in range(2):
            pair = faded[p * 128 : (p + 1) * 128]
            none = jnp.zeros_like(pair)
            both = jnp.concatenate(
                [jnp.where(upper_half, pair, none), jnp.where(upper_half, none, pair)], axis=1
            )
            b = s * 4 + p * 2
            carried = nt(both, jnp.concatenate([SB[b], SB[b + 1]], axis=1))
            OL[s * 256 + p * 128 : s * 256 + (p + 1) * 128] = local[p * 128 : (p + 1) * 128] + carried
        emission = e_ref[rows].astype(F32)
        GT[rows] = gain_ref[...] * emission * jax.nn.sigmoid(emission)

    for k in range(1, 4):
        arrive(STR.at[k], state_recv.at[k - 1])
    plane = jnp.zeros((HD, HD), F32)
    plane_log = jnp.zeros((1, HD), F32)
    before, before_log = plane, plane_log
    for yy in range(4):
        slot = wrap(y - yy)
        before = jnp.where(y == yy, plane, before)
        before_log = jnp.where(y == yy, plane_log, before_log)
        log = joined(STR[slot, 128:144])
        plane = plane * jnp.exp(log) + STR[slot, 0:128].astype(F32)
        plane_log = plane_log + log
    TOT[0, 0:128] = plane.astype(BF16)
    TOT[0, 128:144] = spread(plane_log)

    def total_copy(k):
        return pltpu.make_async_remote_copy(
            src_ref=TOT.at[0], dst_ref=TOT.at[k],
            send_sem=total_send.at[k - 1], recv_sem=total_recv.at[k - 1],
            device_id={"z": wrap(z + k)}, device_id_type=MESH,
        )

    for k in range(1, 4):

        @pl.when(z + k < 4)
        def _():
            total_copy(k).start()

        @pl.when(z < k)
        def _():
            TOT[k] = jnp.zeros((144, HD), BF16)

    stage(GU, 2)
    for k in range(1, 4):

        @pl.when(z >= k)
        def _():
            arrive(TOT.at[k], total_recv.at[k - 1])

    since = before_log
    for k in range(1, 4):
        before = before + TOT[k, 0:128].astype(F32) * jnp.exp(since)
        since = since + joined(TOT[k, 128:144])
    incoming = before.astype(BF16)
    for s in range(4):
        rows = slice(s * 256, (s + 1) * 256)
        o = OL[rows] + nt(QC[rows], incoming)
        squares = jnp.mean(o * o, axis=-1, keepdims=True)
        mixed = (o * lax.rsqrt(squares + EPSILON) * GT[rows]).astype(BF16)
        for core in (0, 1):
            MIXS[core, s * 128 : (s + 1) * 128] = mixed[core * 128 : (core + 1) * 128]

    head = x * 2 + c
    MX[head] = MIXS[c]

    def mix_copy(source, slab, sem, device):
        pltpu.make_async_remote_copy(
            src_ref=source, dst_ref=MX.at[slab],
            send_sem=mix_send.at[0], recv_sem=mix_recv.at[sem],
            device_id=device, device_id_type=MESH,
        ).start()

    for i, step in enumerate((1, -1)):
        for core in (0, 1):
            mix_copy(MIXS.at[core], head, i * 2 + c, {"x": wrap(x + step), "c": jnp.int32(core)})
    mix_copy(MIXS.at[other], head, 4, {"c": other})

    def mix_arrived(slab, sem):
        arrive(MX.at[slab], mix_recv.at[sem])

    stage(GU, 3)
    skip_relay(0)
    stage(GU, 4)
    left, right = wrap(x - 1), wrap(x + 1)
    mix_arrived(left * 2, 0)
    mix_copy(MX.at[left * 2], left * 2, 5, {"x": right})
    mix_arrived(right * 2 + 1, 3)
    mix_copy(MX.at[right * 2 + 1], right * 2 + 1, 6, {"x": left})
    skip_relay(1)
    stage(GU, 5)
    stage(GU, 8)
    arrive(EB, e_sem.at[0])
    opposite = wrap(x + 2)
    mix_arrived(left * 2 + 1, 1)
    mix_arrived(right * 2, 2)
    mix_arrived(x * 2 + other, 4)
    mix_arrived(opposite * 2, 5)
    mix_arrived(opposite * 2 + 1, 6)

    def project(n, carry):
        mixed = jnp.concatenate([MX[h] for h in range(8)], axis=1)
        ACC[n] = mm(mixed, EB[n])
        return carry

    lax.fori_loop(0, 4, project, 0, unroll=True)
    lax.fori_loop(4, 8, project, 0, unroll=True)
    stage(DOWN, 0)
    skip_arrived(opposite, pl.ds(0, 64), 2)
    skip_arrived(opposite, pl.ds(64, 64), 3)
    SSQ[...] = jnp.zeros((ROWS, 128), F32)

    def add(n, carry):
        skipped = SK[:, :, pl.ds(pl.multiple_of(n * 256, 256), 256)].reshape(ROWS, 256)
        stream = (skipped.astype(F32) + ACC[n]).astype(BF16)
        STREAM[n] = stream
        wide = stream.astype(F32)
        wide = wide * wide
        SSQ[...] += wide[:, :128] + wide[:, 128:]
        return carry

    lax.fori_loop(0, 8, add, 0)
    scale = lax.rsqrt(jnp.sum(SSQ[...], axis=1, keepdims=True) * (1.0 / D) + EPSILON)

    for n in range(8):
        gain = norm_gain_ref[:, n * 256 : (n + 1) * 256]
        NORM[n] = (STREAM[n].astype(F32) * scale * gain).astype(BF16)

    def await_sides(dz):
        arrive(units(GU, 8), side_gu.at[dz % 4])

    def chunk(xi):
        return pl.ds(pl.multiple_of(xi * 128, 128), 128)

    def silu(a):
        return a * jax.nn.sigmoid(a)

    def gate_up(planes, first, last, begin=0, end=6, chunks=(0, 1, 2, 3)):
        places = [wrap(z + dz) for dz in planes]
        rows = [
            [pl.ds(pl.multiple_of(h * D + p * 512, 512), 512) for p in places] for h in (0, 1)
        ]

        def some(ref, t):
            if len(chunks) == 4:
                return ref[t]
            return jnp.concatenate([ref[t, chunk(wrap(x + k))] for k in chunks], axis=0)

        def put(ref, t, value):
            if len(chunks) == 4:
                ref[t] = value
                return
            for n, k in enumerate(chunks):
                ref[t, chunk(wrap(x + k))] = value[n * 128 : (n + 1) * 128]

        def partial(weights):
            normed = [some(NORM, p * 2 + i) for p in places for i in (0, 1)]
            return mm(jnp.concatenate(normed, axis=1), jnp.concatenate(weights, axis=0))

        def tile(j, carry):
            columns = pl.ds(pl.multiple_of(j * 256, 256), 256)
            for h in (0, 1):
                t = h * 5 + j
                part = partial([W[deep, columns] for deep in rows[h]])
                if not first:
                    part = part + some(ACC, t)
                if not last:
                    put(ACC, t, part)
                else:
                    put(HID, t, (silu(part[:, :128]) * part[:, 128:]).astype(BF16))
            return carry

        lax.fori_loop(begin, min(end, 5), tile, 0, unroll=True)
        if end < 6:
            return
        part = partial(
            [
                jnp.concatenate([W[one, 1280:1408], W[two, 1280:1408]], axis=1)
                for one, two in zip(*rows)
            ]
        )
        if not first:
            part = part + some(ACC, 10)
        if not last:
            put(ACC, 10, part)
        else:
            lane = lax.broadcasted_iota(jnp.int32, (128 * len(chunks), 128), 1)
            a, b = part[:, :128], part[:, 128:]
            gates = jnp.where(lane < 64, a, pltpu.roll(b, 64, 1))
            ups = jnp.where(lane < 64, pltpu.roll(a, 64, 1), b)
            put(HID, 10, (silu(gates) * ups).astype(BF16))

    def column_of(i):
        dy, dz = ORDER[i]
        return wrap(z + dz) * 4 + wrap(y + dy)

    def down_weights(i):
        def block(at_column):
            one, two = at_column, 16 + at_column
            return jnp.concatenate(
                [DN[one, 0:640], DN[two, 0:640], DN[one, 640:704], DN[two, 640:704]], axis=0
            )

        return jnp.concatenate([block(column_of(2 * i)), block(column_of(2 * i + 1))], axis=1)

    def send_far(i, far):
        for half, step in enumerate((1, -1)):
            OPPS[i, half] = far[:, half * 128 : (half + 1) * 128].astype(BF16)
            pltpu.make_async_remote_copy(
                src_ref=OPPS.at[i, half], dst_ref=OPPR.at[i, half],
                send_sem=opp_send.at[0], recv_sem=opp_recv.at[i],
                device_id={"x": wrap(x + step)}, device_id_type=MESH,
            ).start()

    def down(i):
        arrive(units(DOWN, 4), side_down.at[i])
        res = RES.at[i % 2]
        res[...] = mm(jnp.concatenate([HID[t] for t in range(11)], axis=1), down_weights(i))
        send_far(i, res[chunk(opposite)])
        OWN[i] = res[chunk(x)]
        PN[0, i] = res[chunk(right)]
        PN[1, i] = res[chunk(left)]

    def down_far(i):
        arrive(units(DOWN, 4), side_down.at[i])
        hidden = jnp.concatenate([HID[t, chunk(opposite)] for t in range(11)], axis=1)
        send_far(i, mm(hidden, down_weights(i)))

    def down_near(i):
        hidden = [
            jnp.concatenate([HID[t, chunk(k)] for t in range(11)], axis=1) for k in (x, right, left)
        ]
        near = mm(jnp.concatenate(hidden, axis=0), down_weights(i))
        OWN[i] = near[:128]
        PN[0, i] = near[128:256]
        PN[1, i] = near[256:]

    def hand_on(i):
        arrive(OPPR.at[i], opp_recv.at[i])
        for half, step in enumerate((1, -1)):
            mine = slice(half * 128, (half + 1) * 128)
            rest = slice(128 - half * 128, 256 - half * 128)
            NBS[i, half, :, mine] = (PN[half, i, :, mine] + OPPR[i, half].astype(F32)).astype(BF16)
            NBS[i, half, :, rest] = PN[half, i, :, rest].astype(BF16)
            pltpu.make_async_remote_copy(
                src_ref=NBS.at[i, half], dst_ref=NBR.at[i, half],
                send_sem=nb_send.at[0], recv_sem=nb_recv.at[i],
                device_id={"x": wrap(x + step)}, device_id_type=MESH,
            ).start()

    def finish(i):
        arrive(NBR.at[i], nb_recv.at[i])
        summed = OWN[i] + NBR[i, 0].astype(F32) + NBR[i, 1].astype(F32)
        for half in (0, 1):
            column = column_of(2 * i + half)
            lanes = pl.ds(pl.multiple_of(lax.rem(column, 2) * 128, 128), 128)
            stream = STREAM[column // 2, chunk(x), lanes].astype(F32)
            columns = pl.ds(pl.multiple_of(column * 128, 128), 128)
            out_ref[:, columns] = (stream + summed[:, half * 128 : (half + 1) * 128]).astype(BF16)

    stage(DOWN, 1)
    await_sides(0)
    gate_up((0,), True, False)
    stage(GU, 6)
    await_sides(-1)
    await_sides(1)
    stage(DOWN, 2)
    gate_up((-1, 1), False, False, 0, 3)
    stage(GU, 7)
    stage(DOWN, 3)
    gate_up((-1, 1), False, False, 3, 6)
    await_sides(2)
    stage(DOWN, 4)
    gate_up((2,), False, True, chunks=(2,))
    down_far(0)
    down_far(1)
    gate_up((2,), False, True, chunks=(0, 1, -1))
    stage(DOWN, 5)
    down_near(0)
    stage(DOWN, 8)
    down_near(1)
    hand_on(0)
    down(2)
    stage(DOWN, 6)
    hand_on(1)
    down(3)
    down(4)
    hand_on(2)
    stage(DOWN, 7)
    down(5)
    hand_on(3)
    down(6)
    hand_on(4)
    down(7)
    hand_on(5)
    finish(0)
    hand_on(6)
    finish(1)
    finish(2)
    hand_on(7)
    finish(3)
    finish(4)
    finish(5)
    finish(6)
    finish(7)

    for kind in (GU, DOWN):
        arrive(units(kind, counts[kind] // 2), w_send.at[kind])
    arrive(STR.at[pl.ds(0, 3)], state_send.at[0])
    arrive(SK.at[pl.ds(0, 3)], skip_send.at[0])
    arrive(MX.at[pl.ds(0, 7)], mix_send.at[0])
    arrive(OPPS, opp_send.at[0])
    arrive(NBS, nb_send.at[0])
    for k in range(1, 4):

        @pl.when(z + k < 4)
        def _():
            total_copy(k).wait_send()


def on_device(skip, q, r, v, e, slack, surge, gain, emission, norm_gain, gate, up, down):
    vmem = pl.BlockSpec(memory_space=pltpu.VMEM)
    dma = pltpu.SemaphoreType.DMA
    return pl.pallas_call(
        kernel,
        out_shape=jax.ShapeDtypeStruct((128, D), BF16),
        in_specs=[pl.BlockSpec(memory_space=pltpu.HBM)] * 13,
        out_specs=vmem,
        scratch_shapes=[
            pltpu.VMEM((128, D), BF16),
            pltpu.VMEM((2, TOK, HD), BF16),
            pltpu.VMEM((2, TOK, HD), BF16),
            pltpu.VMEM((1, HD), F32),
            pltpu.VMEM((TOK, HD), F32),
            pltpu.VMEM((1, HD), F32),
            pltpu.VMEM((1, D), F32),
            pltpu.VMEM((3, 704, 128), BF16),
            pltpu.VMEM((2 * D, 1408), BF16),
            pltpu.VMEM((32, 704, 128), BF16),
            pltpu.VMEM((8, 1024, 256), BF16),
            pltpu.VMEM((4, 128, D), BF16),
            pltpu.VMEM((8, ROWS, 128), BF16),
            pltpu.VMEM((2, ROWS, 128), BF16),
            pltpu.VMEM((8, ROWS, 256), BF16),
            pltpu.VMEM((8, ROWS, 256), BF16),
            pltpu.VMEM((11, ROWS, 256), F32),
            pltpu.VMEM((11, ROWS, 128), BF16),
            pltpu.VMEM((ROWS, 128), F32),
            pltpu.VMEM((2, ROWS, 256), F32),
            pltpu.VMEM((TOK, HD), F32),
            pltpu.VMEM((TOK, HD), F32),
            pltpu.VMEM((16, HD, HD), F32),
            pltpu.VMEM((16, HD, HD), BF16),
            pltpu.VMEM((4, 144, HD), BF16),
            pltpu.VMEM((4, 144, HD), BF16),
            pltpu.VMEM((TOK, HD), F32),
            pltpu.VMEM((TOK, HD), BF16),
            pltpu.VMEM((TOK, HD), F32),
            pltpu.VMEM((8, 2, 128, 128), BF16),
            pltpu.VMEM((8, 2, 128, 128), BF16),
            pltpu.VMEM((8, 128, 256), F32),
            pltpu.VMEM((2, 8, 128, 256), F32),
            pltpu.VMEM((8, 2, 128, 256), BF16),
            pltpu.VMEM((8, 2, 128, 256), BF16),
            dma((2, 10)),
            dma((4,)),
            dma((8,)),
            dma((2,)),
            dma((3,)),
            dma((1,)),
            dma((3,)),
            dma((3,)),
            dma((4,)),
            dma((1,)),
            dma((7,)),
            dma((1,)),
            dma((1,)),
            dma((8,)),
            dma((8,)),
            dma((1,)),
            dma((8,)),
            dma((1,)),
        ],
        compiler_params=pltpu.CompilerParams(
            collective_id=0, has_side_effects=True, vmem_limit_bytes=54000000
        ),
        name="layer",
    )(
        *(
            pltpu.with_memory_space_constraint(a, pltpu.HBM)
            for a in (skip, q, r, v, e, slack.reshape(1, -1), surge, gain.reshape(1, -1), emission,
                      norm_gain.reshape(1, -1), gate.T, up.T, down)
        )
    )


def solution(mesh):
    split = Mesh(mesh.devices.reshape(4, 4, 4, 2), ("z", "y", "x", "c"))
    sp, tp = ("z", "y"), ("x", "c")
    return jax.shard_map(
        on_device,
        mesh=split,
        in_specs=(
            P(sp + tp, None),
            P(sp, tp),
            P(sp, tp),
            P(sp, tp),
            P(sp, tp),
            P(tp),
            P(sp, tp),
            P(tp),
            P(),
            P(),
            P(sp, tp),
            P(sp, tp),
            P(tp, sp),
        ),
        out_specs=P(sp + tp, None),
        check_vma=False,
    )
```

```python
import functools

import jax
import jax.numpy as jnp
from jax import lax
from jax.experimental import pallas as pl
from jax.experimental.pallas import tpu as pltpu
from jax.sharding import Mesh
from jax.sharding import PartitionSpec as P

MESH = pl.DeviceIdType.MESH
F32 = jnp.float32
BF16 = jnp.bfloat16
EPSILON = 1e-06
HD = 128
BLOCK = 64
TOK = 1024
ROWS = 512
D = 2048
GU, DOWN = 0, 1


def wrap(value, n=4):
    return lax.rem(value + n, n)


def nt(a, b):
    return lax.dot_general(a, b, (((1,), (1,)), ((), ())), preferred_element_type=F32)


def tn(a, b):
    return lax.dot_general(a, b, (((0,), (0,)), ((), ())), preferred_element_type=F32)


def mm(a, b):
    return jnp.dot(a, b, preferred_element_type=F32)


def kernel(
    skip_in, q_in, r_in, v_in, e_in, slack_in, surge_in, gain_in, emission_ref,
    norm_gain_in, gate_in, up_in, down_in,
    out_ref,
    skip_ref, QE, RV, slack_ref, surge_ref, gain_ref, norm_gain_ref, OWNED,
    W, DN, EB, SK, MX, MIXS, STREAM, NORM, ACC, HID, SSQ, RES,
    CUM, IG, DS, SB, STR, TOT, OL, QC, GT,
    OPPS, OPPR, OWN, PN, NBS, NBR,
    w_recv, side_gu, side_down, w_send, state_recv, state_send, total_recv, total_send,
    skip_sem, skip_send, mix_recv, mix_send, e_sem, in_sem, opp_recv, opp_send, nb_recv, nb_send,
):
    z, y, x, c = (lax.axis_index(name) for name in ("z", "y", "x", "c"))
    sp = z * 4 + y
    other = 1 - c
    q_ref, e_ref, r_ref, v_ref = QE.at[0], QE.at[1], RV.at[0], RV.at[1]
    gate_ref, up_ref, down_ref = (OWNED.at[i] for i in range(3))

    def arrive(ref, sem):
        pltpu.make_async_copy(ref, ref, sem).wait()

    barrier = pltpu.get_barrier_semaphore()
    for k in range(1, 4):
        pl.semaphore_signal(barrier, inc=1, device_id={"y": wrap(y + k)}, device_id_type=MESH)
        pl.semaphore_signal(barrier, inc=1, device_id={"z": wrap(z + k)}, device_id_type=MESH)
    for step in (1, -1):
        for core in (0, 1):
            pl.semaphore_signal(barrier, inc=1, device_id={"x": wrap(x + step), "c": jnp.int32(core)}, device_id_type=MESH)
    pl.semaphore_signal(barrier, inc=1, device_id={"c": other}, device_id_type=MESH)

    def load(source, target, sem):
        pltpu.make_async_copy(source, target, in_sem.at[sem]).start()

    load(gate_in, gate_ref, 0)
    load(up_in, up_ref, 0)
    load(down_in, down_ref, 0)
    load(r_in, r_ref, 1)
    load(v_in, v_ref, 1)
    load(surge_in, surge_ref, 2)
    load(slack_in, slack_ref, 3)
    load(skip_in, skip_ref, 4)
    load(q_in, q_ref, 5)
    load(e_in, e_ref, 5)
    load(gain_in, gain_ref, 6)
    load(norm_gain_in, norm_gain_ref, 7)

    arrive(OWNED, in_sem.at[0])
    own_rows = pl.ds(pl.multiple_of(c * D + sp * 128, 128), 128)
    for j in range(5):
        W[own_rows, j * 256 : j * 256 + 128] = gate_ref[j * 128 : (j + 1) * 128].T
        W[own_rows, j * 256 + 128 : (j + 1) * 256] = up_ref[j * 128 : (j + 1) * 128].T
    W[own_rows, 1280:1408] = jnp.concatenate([gate_ref[640:704], up_ref[640:704]], axis=0).T
    DN[c * 16 + sp] = down_ref[...]

    pl.semaphore_wait(barrier, 11)

    AXES = {0: ("y", "z"), 1: ("z", "y")}
    ORDER = (
        (0, 0), (1, 0), (-1, 0), (0, 1), (0, -1), (-1, -1), (1, 1), (1, -1),
        (-1, 1), (2, 0), (0, 2), (2, 1), (2, -1), (1, 2), (-1, 2), (2, 2),
    )
    here = {"z": z, "y": y}

    def short(offset):
        return (offset + 1) % 4 - 1

    def unit(kind, color, rel, half):
        origin = wrap(z + rel["z"]) * 4 + wrap(y + rel["y"])
        size, skipped = (1, 0) if half is None else (2, half)
        if kind == GU:
            start = pl.multiple_of(c * D + origin * 128 + color * 64 + skipped * 32, 32)
            return W.at[pl.ds(start, 64 // size), :]
        return DN.at[c * 16 + origin, pl.ds(color * 352 + skipped * 176, 352 // size), :]

    def units(kind, count):
        return W.at[pl.ds(0, 64 * count), :] if kind == GU else DN.at[pl.ds(0, count // 2)]

    counts = {GU: 0, DOWN: 0}

    def lot(color, rel):
        one, two = AXES[color]
        first, second = short(rel[one]), short(rel[two])
        if second == 0:
            return {-1: 0, 1: 1, 2: 3}[first]
        if second == 2:
            return {0: 6, -1: 8, 1: 8, 2: 9}[first]
        return {0: 2, -1: 4, 1: 5, 2: 7}[first]

    LOTS = (2, 2, 4, 2, 4, 4, 2, 4, 4, 2)

    def arrived(kind, number):
        arrive(units(kind, LOTS[number]), w_recv.at[kind, number])

    def start_unit(kind, color, rel, recv_sem, device, half=None):
        ref = unit(kind, color, rel, half)
        pltpu.make_async_remote_copy(
            src_ref=ref, dst_ref=ref, send_sem=w_send.at[kind], recv_sem=recv_sem,
            device_id=device, device_id_type=MESH,
        ).start()
        counts[kind] += 2 if half is None else 1

    def push(kind, color, rel, axis, step, half=None):
        there = dict(rel)
        there[axis] = rel[axis] - step
        sem = w_recv.at[kind, lot(color, there)]
        start_unit(kind, color, rel, sem, {axis: wrap(here[axis] + step)}, half)

    def side(kind, color, rel):
        place = (short(rel["y"]), short(rel["z"]))
        sem = side_gu.at[place[1] % 4] if kind == GU else side_down.at[ORDER.index(place) // 2]
        start_unit(kind, color, rel, sem, {"c": other})

    def at(color, first, second):
        one, two = AXES[color]
        return {one: first, two: second}

    def stage(kind, n):
        if n in (0, 1):
            for color in (0, 1):
                for step in (1, -1):
                    push(kind, color, at(color, 0, 0), AXES[color][n], step)
                if n == 1:
                    side(kind, color, at(color, 0, 0))
        if n == 2:
            arrived(kind, 0)
            arrived(kind, 1)
            for f in (-1, 1):
                for color in (0, 1):
                    push(kind, color, at(color, f, 0), AXES[color][0], -f, (f + 1) // 2)
        if n == 4:
            arrived(kind, 3)
        for f in {2: (-1, 1), 4: (2,)}.get(n, ()):
            for color in (0, 1):
                for step in (1, -1):
                    push(kind, color, at(color, f, 0), AXES[color][1], step)
                side(kind, color, at(color, f, 0))
        for number, first in {3: ((2, 0),), 5: ((4, -1),), 8: ((5, 1),), 6: ((7, 2),)}.get(n, ()):
            arrived(kind, number)
            for s in (-1, 1):
                for color in (0, 1):
                    push(kind, color, at(color, first, s), AXES[color][1], -s, (s + 1) // 2)
            for s in (-1, 1):
                for color in (0, 1):
                    side(kind, color, at(color, first, s))
        for number, firsts in {8: ((6, (0,)),), 6: ((8, (-1, 1)),), 7: ((9, (2,)),)}.get(n, ()):
            arrived(kind, number)
            for first in firsts:
                for color in (0, 1):
                    side(kind, color, at(color, first, 2))

    own = at(0, 0, 0)
    for step in (1, -1):
        push(GU, 0, own, "y", step, 0)
        push(GU, 1, own, "z", step)

    def skip_copy(source, slot, rows, sem, step):
        return pltpu.make_async_remote_copy(
            src_ref=source, dst_ref=SK.at[slot, rows, :],
            send_sem=skip_send.at[0], recv_sem=skip_sem.at[sem],
            device_id={"x": wrap(x + step)}, device_id_type=MESH,
        )

    arrive(skip_ref, in_sem.at[4])
    for i, step in enumerate((1, -1)):
        skip_copy(skip_ref, x, pl.ds(0, 128), i, step).start()

    def skip_arrived(slot, rows, sem):
        arrive(SK.at[slot, rows, :], skip_sem.at[sem])

    def skip_relay(part):
        left, right = wrap(x - 1), wrap(x + 1)
        first, second = pl.ds(part * 32, 32), pl.ds(64 + part * 32, 32)
        if part == 0:
            skip_arrived(left, pl.ds(0, 128), 0)
            skip_arrived(right, pl.ds(0, 128), 1)
        skip_copy(SK.at[left, first, :], left, first, 2 + part, 1).start()
        skip_copy(SK.at[right, second, :], right, second, 2 + part, -1).start()

    i256 = lax.broadcasted_iota(jnp.int32, (256, 256), 0)
    j256 = lax.broadcasted_iota(jnp.int32, (256, 256), 1)
    causal = jnp.logical_and(i256 >= j256, i256 // BLOCK == j256 // BLOCK)
    triangle = jnp.where(causal, 1.0, 0.0).astype(BF16)
    upper_half = lax.broadcasted_iota(jnp.int32, (128, 128), 0) < BLOCK
    arrive(RV, in_sem.at[1])
    arrive(surge_ref, in_sem.at[2])
    arrive(slack_ref, in_sem.at[3])
    closings = []
    for s in range(4):
        rows = slice(s * 256, (s + 1) * 256)
        ig = slack_ref[...] * jax.nn.sigmoid(-r_ref[rows].astype(F32))
        lf = jnp.log1p(-ig) + surge_ref[rows]
        high = lf.astype(BF16)
        rest = lf - high.astype(F32)
        mid = rest.astype(BF16)
        low = (rest - mid.astype(F32)).astype(BF16)
        parts = mm(triangle, jnp.concatenate([high, mid, low], axis=1))
        cum = parts[:, :128] + parts[:, 128:256] + parts[:, 256:]
        CUM[rows] = cum
        IG[rows] = ig
        blocks = cum.reshape(4, BLOCK, HD)
        last = blocks[:, BLOCK - 1 : BLOCK, :]
        closings += [last[b] for b in range(4)]
        keys = (ig * jnp.exp(last - blocks).reshape(256, HD)).astype(BF16)
        for p in range(2):
            pair = keys[p * 128 : (p + 1) * 128]
            none = jnp.zeros_like(pair)
            both = jnp.concatenate(
                [jnp.where(upper_half, pair, none), jnp.where(upper_half, none, pair)], axis=1
            )
            grown = tn(v_ref[s * 256 + p * 128 : s * 256 + (p + 1) * 128], both)
            DS[s * 4 + p * 2] = grown[:, :128]
            DS[s * 4 + p * 2 + 1] = grown[:, 128:]
    state = jnp.zeros((HD, HD), F32)
    passed = jnp.zeros((1, HD), F32)
    offsets = []
    for b in range(16):
        SB[b] = state.astype(BF16)
        offsets.append(passed)
        state = state * jnp.exp(closings[b]) + DS[b]
        passed = passed + closings[b]
    STR[0, 0:128] = state.astype(BF16)
    which = lax.broadcasted_iota(jnp.int32, (16, HD), 0)

    def spread(value):
        high = value.astype(BF16)
        rest = value - high.astype(F32)
        mid = rest.astype(BF16)
        low = rest - mid.astype(F32)
        rows = jnp.where(which == 2, low, 0.0)
        rows = jnp.where(which == 1, mid.astype(F32), rows)
        return jnp.where(which == 0, high.astype(F32), rows).astype(BF16)

    def joined(rows):
        rows = rows.astype(F32)
        return rows[0:1] + rows[1:2] + rows[2:3]

    STR[0, 128:144] = spread(passed)

    for k in range(1, 4):
        pltpu.make_async_remote_copy(
            src_ref=STR.at[0], dst_ref=STR.at[k],
            send_sem=state_send.at[0], recv_sem=state_recv.at[k - 1],
            device_id={"y": wrap(y + k)}, device_id_type=MESH,
        ).start()

    for n in range(8):
        source = emission_ref.at[:, pl.ds(n * 256, 256)]
        pltpu.make_async_copy(source, EB.at[n], e_sem.at[0]).start()
    for step in (1, -1):
        push(GU, 0, own, "y", step, 1)
        push(GU, 1, own, "y", step)
        push(GU, 0, own, "z", step, 0)
    SK[x] = skip_ref[...]
    arrive(QE, in_sem.at[5])
    arrive(gain_ref, in_sem.at[6])
    arrive(norm_gain_ref, in_sem.at[7])
    for s in range(4):
        rows = slice(s * 256, (s + 1) * 256)
        q = q_ref[rows].astype(F32)
        qa = q * jax.nn.sigmoid(q)
        cum = CUM[rows]
        ig = IG[rows]
        blocks = cum.reshape(4, BLOCK, HD)
        middle = blocks[:, BLOCK // 2 : BLOCK // 2 + 1, :]
        centred = (blocks - middle).reshape(256, HD)
        left = (qa * jnp.exp(centred)).astype(BF16)
        right = (ig * jnp.exp(-centred)).astype(BF16)
        scores = jnp.where(causal, nt(left, right), 0.0).astype(BF16)
        local = mm(scores, v_ref[rows])
        faded = qa * jnp.exp(cum)
        faded_by = jnp.concatenate([offsets[s * 4 + b].reshape(1, 1, HD) for b in range(4)], axis=0)
        QC[rows] = (qa * jnp.exp(blocks + faded_by).reshape(256, HD)).astype(BF16)
        faded = faded.astype(BF16)
        for p in range(2):
            pair = faded[p * 128 : (p + 1) * 128]
            none = jnp.zeros_like(pair)
            both = jnp.concatenate(
                [jnp.where(upper_half, pair, none), jnp.where(upper_half, none, pair)], axis=1
            )
            b = s * 4 + p * 2
            carried = nt(both, jnp.concatenate([SB[b], SB[b + 1]], axis=1))
            OL[s * 256 + p * 128 : s * 256 + (p + 1) * 128] = local[p * 128 : (p + 1) * 128] + carried
        emission = e_ref[rows].astype(F32)
        GT[rows] = gain_ref[...] * emission * jax.nn.sigmoid(emission)

    for k in range(1, 4):
        arrive(STR.at[k], state_recv.at[k - 1])
    plane = jnp.zeros((HD, HD), F32)
    plane_log = jnp.zeros((1, HD), F32)
    before, before_log = plane, plane_log
    for yy in range(4):
        slot = wrap(y - yy)
        before = jnp.where(y == yy, plane, before)
        before_log = jnp.where(y == yy, plane_log, before_log)
        log = joined(STR[slot, 128:144])
        plane = plane * jnp.exp(log) + STR[slot, 0:128].astype(F32)
        plane_log = plane_log + log
    TOT[0, 0:128] = plane.astype(BF16)
    TOT[0, 128:144] = spread(plane_log)

    def total_copy(k):
        return pltpu.make_async_remote_copy(
            src_ref=TOT.at[0], dst_ref=TOT.at[k],
            send_sem=total_send.at[k - 1], recv_sem=total_recv.at[k - 1],
            device_id={"z": wrap(z + k)}, device_id_type=MESH,
        )

    for k in range(1, 4):

        @pl.when(z + k < 4)
        def _():
            total_copy(k).start()

        @pl.when(z < k)
        def _():
            TOT[k] = jnp.zeros((144, HD), BF16)

    for step in (1, -1):
        push(GU, 0, own, "z", step, 1)
    for color in (0, 1):
        side(GU, color, own)
    stage(GU, 2)
    for k in range(1, 4):

        @pl.when(z >= k)
        def _():
            arrive(TOT.at[k], total_recv.at[k - 1])

    since = before_log
    for k in range(1, 4):
        before = before + TOT[k, 0:128].astype(F32) * jnp.exp(since)
        since = since + joined(TOT[k, 128:144])
    incoming = before.astype(BF16)
    for s in range(4):
        rows = slice(s * 256, (s + 1) * 256)
        o = OL[rows] + nt(QC[rows], incoming)
        squares = jnp.mean(o * o, axis=-1, keepdims=True)
        mixed = (o * lax.rsqrt(squares + EPSILON) * GT[rows]).astype(BF16)
        for core in (0, 1):
            MIXS[core, s * 128 : (s + 1) * 128] = mixed[core * 128 : (core + 1) * 128]

    head = x * 2 + c
    MX[head] = MIXS[c]

    def mix_copy(source, slab, sem, device):
        pltpu.make_async_remote_copy(
            src_ref=source, dst_ref=MX.at[slab],
            send_sem=mix_send.at[0], recv_sem=mix_recv.at[sem],
            device_id=device, device_id_type=MESH,
        ).start()

    for i, step in enumerate((1, -1)):
        for core in (0, 1):
            mix_copy(MIXS.at[core], head, i * 2 + c, {"x": wrap(x + step), "c": jnp.int32(core)})
    mix_copy(MIXS.at[other], head, 4, {"c": other})

    def mix_arrived(slab, sem):
        arrive(MX.at[slab], mix_recv.at[sem])

    stage(GU, 3)
    skip_relay(0)
    stage(GU, 4)
    left, right = wrap(x - 1), wrap(x + 1)
    mix_arrived(left * 2, 0)
    mix_copy(MX.at[left * 2], left * 2, 5, {"x": right})
    mix_arrived(right * 2 + 1, 3)
    mix_copy(MX.at[right * 2 + 1], right * 2 + 1, 6, {"x": left})
    skip_relay(1)
    stage(GU, 5)
    stage(GU, 8)
    stage(DOWN, 0)
    arrive(EB, e_sem.at[0])
    opposite = wrap(x + 2)
    mix_arrived(left * 2 + 1, 1)
    mix_arrived(right * 2, 2)
    mix_arrived(x * 2 + other, 4)
    mix_arrived(opposite * 2, 5)
    mix_arrived(opposite * 2 + 1, 6)

    def project(n, carry):
        mixed = jnp.concatenate([MX[h] for h in range(8)], axis=1)
        ACC[n] = mm(mixed, EB[n])
        return carry

    lax.fori_loop(0, 4, project, 0, unroll=True)
    lax.fori_loop(4, 8, project, 0, unroll=True)
    skip_arrived(opposite, pl.ds(0, 64), 2)
    skip_arrived(opposite, pl.ds(64, 64), 3)
    SSQ[...] = jnp.zeros((ROWS, 128), F32)

    def add(n, carry):
        skipped = SK[:, :, pl.ds(pl.multiple_of(n * 256, 256), 256)].reshape(ROWS, 256)
        stream = (skipped.astype(F32) + ACC[n]).astype(BF16)
        STREAM[n] = stream
        wide = stream.astype(F32)
        wide = wide * wide
        SSQ[...] += wide[:, :128] + wide[:, 128:]
        return carry

    lax.fori_loop(0, 8, add, 0)
    scale = lax.rsqrt(jnp.sum(SSQ[...], axis=1, keepdims=True) * (1.0 / D) + EPSILON)

    for n in range(8):
        gain = norm_gain_ref[:, n * 256 : (n + 1) * 256]
        NORM[n] = (STREAM[n].astype(F32) * scale * gain).astype(BF16)

    def await_sides(dz):
        arrive(units(GU, 8), side_gu.at[dz % 4])

    def chunk(xi):
        return pl.ds(pl.multiple_of(xi * 128, 128), 128)

    def silu(a):
        return a * jax.nn.sigmoid(a)

    def gate_up(planes, first, last, begin=0, end=6, chunks=(0, 1, 2, 3)):
        places = [wrap(z + dz) for dz in planes]
        rows = [
            [pl.ds(pl.multiple_of(h * D + p * 512, 512), 512) for p in places] for h in (0, 1)
        ]

        def some(ref, t):
            if len(chunks) == 4:
                return ref[t]
            return jnp.concatenate([ref[t, chunk(wrap(x + k))] for k in chunks], axis=0)

        def put(ref, t, value):
            if len(chunks) == 4:
                ref[t] = value
                return
            for n, k in enumerate(chunks):
                ref[t, chunk(wrap(x + k))] = value[n * 128 : (n + 1) * 128]

        def partial(weights):
            normed = [some(NORM, p * 2 + i) for p in places for i in (0, 1)]
            return mm(jnp.concatenate(normed, axis=1), jnp.concatenate(weights, axis=0))

        def tile(j, carry):
            columns = pl.ds(pl.multiple_of(j * 256, 256), 256)
            for h in (0, 1):
                t = h * 5 + j
                part = partial([W[deep, columns] for deep in rows[h]])
                if not first:
                    part = part + some(ACC, t)
                if not last:
                    put(ACC, t, part)
                else:
                    put(HID, t, (silu(part[:, :128]) * part[:, 128:]).astype(BF16))
            return carry

        lax.fori_loop(begin, min(end, 5), tile, 0, unroll=True)
        if end < 6:
            return
        part = partial(
            [
                jnp.concatenate([W[one, 1280:1408], W[two, 1280:1408]], axis=1)
                for one, two in zip(*rows)
            ]
        )
        if not first:
            part = part + some(ACC, 10)
        if not last:
            put(ACC, 10, part)
        else:
            lane = lax.broadcasted_iota(jnp.int32, (128 * len(chunks), 128), 1)
            a, b = part[:, :128], part[:, 128:]
            gates = jnp.where(lane < 64, a, pltpu.roll(b, 64, 1))
            ups = jnp.where(lane < 64, pltpu.roll(a, 64, 1), b)
            put(HID, 10, (silu(gates) * ups).astype(BF16))

    def column_of(i):
        dy, dz = ORDER[i]
        return wrap(z + dz) * 4 + wrap(y + dy)

    def down_weights(i):
        def block(at_column):
            one, two = at_column, 16 + at_column
            return jnp.concatenate(
                [DN[one, 0:640], DN[two, 0:640], DN[one, 640:704], DN[two, 640:704]], axis=0
            )

        return jnp.concatenate([block(column_of(2 * i)), block(column_of(2 * i + 1))], axis=1)

    def send_far(i, far):
        for half, step in enumerate((1, -1)):
            OPPS[i, half] = far[:, half * 128 : (half + 1) * 128].astype(BF16)
            pltpu.make_async_remote_copy(
                src_ref=OPPS.at[i, half], dst_ref=OPPR.at[i, half],
                send_sem=opp_send.at[0], recv_sem=opp_recv.at[i],
                device_id={"x": wrap(x + step)}, device_id_type=MESH,
            ).start()

    def send_half(i, half, columns):
        pltpu.make_async_remote_copy(
            src_ref=NBS.at[i, half, columns], dst_ref=NBR.at[i, half, columns],
            send_sem=nb_send.at[0], recv_sem=nb_recv.at[i],
            device_id={"x": wrap(x + 1 - 2 * half)}, device_id_type=MESH,
        ).start()

    def send_near(i, near):
        for half in (0, 1):
            rest = 1 - half
            NBS[i, half, rest] = near[half][:, rest * 128 : (rest + 1) * 128].astype(BF16)
            send_half(i, half, rest)
            PN[half, i] = near[half][:, half * 128 : (half + 1) * 128]

    def down(i):
        arrive(units(DOWN, 4), side_down.at[i])
        res = RES.at[i % 2]
        res[...] = mm(jnp.concatenate([HID[t] for t in range(11)], axis=1), down_weights(i))
        send_far(i, res[chunk(opposite)])
        OWN[i] = res[chunk(x)]
        send_near(i, (res[chunk(right)], res[chunk(left)]))

    def down_far(i):
        arrive(units(DOWN, 4), side_down.at[i])
        hidden = jnp.concatenate([HID[t, chunk(opposite)] for t in range(11)], axis=1)
        send_far(i, mm(hidden, down_weights(i)))

    def down_near(i):
        hidden = [
            jnp.concatenate([HID[t, chunk(k)] for t in range(11)], axis=1) for k in (x, right, left)
        ]
        near = mm(jnp.concatenate(hidden, axis=0), down_weights(i))
        OWN[i] = near[:128]
        send_near(i, (near[128:256], near[256:]))

    def hand_on(i):
        arrive(OPPR.at[i], opp_recv.at[i])
        for half in (0, 1):
            NBS[i, half, half] = (PN[half, i] + OPPR[i, half].astype(F32)).astype(BF16)
            send_half(i, half, half)

    def finish(i):
        arrive(NBR.at[i], nb_recv.at[i])
        for half in (0, 1):
            column = column_of(2 * i + half)
            lanes = pl.ds(pl.multiple_of(lax.rem(column, 2) * 128, 128), 128)
            stream = STREAM[column // 2, chunk(x), lanes].astype(F32)
            summed = OWN[i, :, half * 128 : (half + 1) * 128]
            summed = summed + NBR[i, 0, half].astype(F32) + NBR[i, 1, half].astype(F32)
            columns = pl.ds(pl.multiple_of(column * 128, 128), 128)
            out_ref[:, columns] = (stream + summed).astype(BF16)

    stage(DOWN, 1)
    await_sides(0)
    gate_up((0,), True, False)
    stage(GU, 6)
    await_sides(-1)
    await_sides(1)
    stage(DOWN, 2)
    gate_up((-1, 1), False, False, 0, 3)
    stage(GU, 7)
    stage(DOWN, 3)
    gate_up((-1, 1), False, False, 3, 6)
    await_sides(2)
    gate_up((2,), False, True, chunks=(2,))
    down_far(0)
    down_far(1)
    stage(DOWN, 4)
    stage(DOWN, 5)
    gate_up((2,), False, True, chunks=(0, 1, -1))
    down_near(0)
    stage(DOWN, 8)
    down_near(1)
    hand_on(0)
    down(2)
    down(3)
    hand_on(1)
    stage(DOWN, 6)
    down(4)
    hand_on(2)
    down(5)
    hand_on(3)
    stage(DOWN, 7)
    down(6)
    hand_on(4)
    down(7)
    hand_on(5)
    finish(0)
    hand_on(6)
    finish(1)
    finish(2)
    hand_on(7)
    finish(3)
    finish(4)
    finish(5)
    finish(6)
    finish(7)

    for kind in (GU, DOWN):
        arrive(units(kind, counts[kind] // 2), w_send.at[kind])
    arrive(STR.at[pl.ds(0, 3)], state_send.at[0])
    arrive(SK.at[pl.ds(0, 3)], skip_send.at[0])
    arrive(MX.at[pl.ds(0, 7)], mix_send.at[0])
    arrive(OPPS, opp_send.at[0])
    arrive(NBS, nb_send.at[0])
    for k in range(1, 4):

        @pl.when(z + k < 4)
        def _():
            total_copy(k).wait_send()


def on_device(skip, q, r, v, e, slack, surge, gain, emission, norm_gain, gate, up, down):
    vmem = pl.BlockSpec(memory_space=pltpu.VMEM)
    dma = pltpu.SemaphoreType.DMA
    return pl.pallas_call(
        kernel,
        out_shape=jax.ShapeDtypeStruct((128, D), BF16),
        in_specs=[pl.BlockSpec(memory_space=pltpu.HBM)] * 13,
        out_specs=vmem,
        scratch_shapes=[
            pltpu.VMEM((128, D), BF16),
            pltpu.VMEM((2, TOK, HD), BF16),
            pltpu.VMEM((2, TOK, HD), BF16),
            pltpu.VMEM((1, HD), F32),
            pltpu.VMEM((TOK, HD), F32),
            pltpu.VMEM((1, HD), F32),
            pltpu.VMEM((1, D), F32),
            pltpu.VMEM((3, 704, 128), BF16),
            pltpu.VMEM((2 * D, 1408), BF16),
            pltpu.VMEM((32, 704, 128), BF16),
            pltpu.VMEM((8, 1024, 256), BF16),
            pltpu.VMEM((4, 128, D), BF16),
            pltpu.VMEM((8, ROWS, 128), BF16),
            pltpu.VMEM((2, ROWS, 128), BF16),
            pltpu.VMEM((8, ROWS, 256), BF16),
            pltpu.VMEM((8, ROWS, 256), BF16),
            pltpu.VMEM((11, ROWS, 256), F32),
            pltpu.VMEM((11, ROWS, 128), BF16),
            pltpu.VMEM((ROWS, 128), F32),
            pltpu.VMEM((2, ROWS, 256), F32),
            pltpu.VMEM((TOK, HD), F32),
            pltpu.VMEM((TOK, HD), F32),
            pltpu.VMEM((16, HD, HD), F32),
            pltpu.VMEM((16, HD, HD), BF16),
            pltpu.VMEM((4, 144, HD), BF16),
            pltpu.VMEM((4, 144, HD), BF16),
            pltpu.VMEM((TOK, HD), F32),
            pltpu.VMEM((TOK, HD), BF16),
            pltpu.VMEM((TOK, HD), F32),
            pltpu.VMEM((8, 2, 128, 128), BF16),
            pltpu.VMEM((8, 2, 128, 128), BF16),
            pltpu.VMEM((8, 128, 256), F32),
            pltpu.VMEM((2, 8, 128, 128), F32),
            pltpu.VMEM((8, 2, 2, 128, 128), BF16),
            pltpu.VMEM((8, 2, 2, 128, 128), BF16),
            dma((2, 10)),
            dma((4,)),
            dma((8,)),
            dma((2,)),
            dma((3,)),
            dma((1,)),
            dma((3,)),
            dma((3,)),
            dma((4,)),
            dma((1,)),
            dma((7,)),
            dma((1,)),
            dma((1,)),
            dma((8,)),
            dma((8,)),
            dma((1,)),
            dma((8,)),
            dma((1,)),
        ],
        compiler_params=pltpu.CompilerParams(
            collective_id=0, has_side_effects=True, vmem_limit_bytes=54000000
        ),
        name="layer",
    )(
        *(
            pltpu.with_memory_space_constraint(a, pltpu.HBM)
            for a in (skip, q, r, v, e, slack.reshape(1, -1), surge, gain.reshape(1, -1), emission,
                      norm_gain.reshape(1, -1), gate.T, up.T, down)
        )
    )


def solution(mesh):
    split = Mesh(mesh.devices.reshape(4, 4, 4, 2), ("z", "y", "x", "c"))
    sp, tp = ("z", "y"), ("x", "c")
    return jax.shard_map(
        on_device,
        mesh=split,
        in_specs=(
            P(sp + tp, None),
            P(sp, tp),
            P(sp, tp),
            P(sp, tp),
            P(sp, tp),
            P(tp),
            P(sp, tp),
            P(tp),
            P(),
            P(),
            P(sp, tp),
            P(sp, tp),
            P(tp, sp),
        ),
        out_specs=P(sp + tp, None),
        check_vma=False,
    )
```

```python
import functools

import jax
import jax.numpy as jnp
from jax import lax
from jax.experimental import pallas as pl
from jax.experimental.pallas import tpu as pltpu
from jax.sharding import Mesh
from jax.sharding import PartitionSpec as P

MESH = pl.DeviceIdType.MESH
F32 = jnp.float32
BF16 = jnp.bfloat16
EPSILON = 1e-06
HD = 128
BLOCK = 64
TOK = 1024
ROWS = 512
D = 2048
GU, DOWN = 0, 1


def wrap(value, n=4):
    return lax.rem(value + n, n)


def nt(a, b):
    return lax.dot_general(a, b, (((1,), (1,)), ((), ())), preferred_element_type=F32)


def tn(a, b):
    return lax.dot_general(a, b, (((0,), (0,)), ((), ())), preferred_element_type=F32)


def mm(a, b):
    return jnp.dot(a, b, preferred_element_type=F32)


def kernel(
    skip_in, q_in, r_in, v_in, e_in, slack_in, surge_in, gain_in, emission_ref,
    norm_gain_in, gate_in, up_in, down_in,
    out_ref,
    skip_ref, QE, RV, slack_ref, surge_ref, gain_ref, norm_gain_ref, OWNED,
    W, DN, EB, SK, MX, MIXS, STREAM, NORM, ACC, HID, SSQ, RES,
    CUM, IG, DS, SB, STR, TOT, OL, QC, GT,
    OPPS, OPPR, OWN, PN, NBS, NBR,
    w_recv, side_gu, side_down, w_send, state_recv, state_send, total_recv, total_send,
    skip_sem, skip_send, mix_recv, mix_send, e_sem, in_sem, opp_recv, opp_send, nb_recv, nb_send,
):
    z, y, x, c = (lax.axis_index(name) for name in ("z", "y", "x", "c"))
    sp = z * 4 + y
    other = 1 - c
    q_ref, e_ref, r_ref, v_ref = QE.at[0], QE.at[1], RV.at[0], RV.at[1]
    gate_ref, up_ref, down_ref = (OWNED.at[i] for i in range(3))

    def arrive(ref, sem):
        pltpu.make_async_copy(ref, ref, sem).wait()

    barrier = pltpu.get_barrier_semaphore()
    for k in range(1, 4):
        pl.semaphore_signal(barrier, inc=1, device_id={"y": wrap(y + k)}, device_id_type=MESH)
        pl.semaphore_signal(barrier, inc=1, device_id={"z": wrap(z + k)}, device_id_type=MESH)
    for step in (1, -1):
        for core in (0, 1):
            pl.semaphore_signal(barrier, inc=1, device_id={"x": wrap(x + step), "c": jnp.int32(core)}, device_id_type=MESH)
    pl.semaphore_signal(barrier, inc=1, device_id={"c": other}, device_id_type=MESH)

    def load(source, target, sem):
        pltpu.make_async_copy(source, target, in_sem.at[sem]).start()

    load(gate_in, gate_ref, 0)
    load(up_in, up_ref, 0)
    load(down_in, down_ref, 0)
    load(r_in, r_ref, 1)
    load(v_in, v_ref, 1)
    load(surge_in, surge_ref, 2)
    load(slack_in, slack_ref, 3)
    load(skip_in, skip_ref, 4)
    load(q_in, q_ref, 5)
    load(e_in, e_ref, 5)
    load(gain_in, gain_ref, 6)
    load(norm_gain_in, norm_gain_ref, 7)

    arrive(OWNED, in_sem.at[0])
    own_rows = pl.ds(pl.multiple_of(c * D + sp * 128, 128), 128)
    for j in range(5):
        W[own_rows, j * 256 : j * 256 + 128] = gate_ref[j * 128 : (j + 1) * 128].T
        W[own_rows, j * 256 + 128 : (j + 1) * 256] = up_ref[j * 128 : (j + 1) * 128].T
    W[own_rows, 1280:1408] = jnp.concatenate([gate_ref[640:704], up_ref[640:704]], axis=0).T
    DN[c * 16 + sp] = down_ref[...]

    pl.semaphore_wait(barrier, 11)

    AXES = {0: ("y", "z"), 1: ("z", "y")}
    ORDER = (
        (0, 0), (1, 0), (-1, 0), (0, 1), (0, -1), (-1, -1), (1, 1), (1, -1),
        (-1, 1), (2, 0), (0, 2), (2, 1), (2, -1), (1, 2), (-1, 2), (2, 2),
    )
    here = {"z": z, "y": y}

    def short(offset):
        return (offset + 1) % 4 - 1

    def unit(kind, color, rel, half):
        origin = wrap(z + rel["z"]) * 4 + wrap(y + rel["y"])
        size, skipped = (1, 0) if half is None else (2, half)
        if kind == GU:
            start = pl.multiple_of(c * D + origin * 128 + color * 64 + skipped * 32, 32)
            return W.at[pl.ds(start, 64 // size), :]
        return DN.at[c * 16 + origin, pl.ds(color * 352 + skipped * 176, 352 // size), :]

    def units(kind, count):
        return W.at[pl.ds(0, 64 * count), :] if kind == GU else DN.at[pl.ds(0, count // 2)]

    counts = {GU: 0, DOWN: 0}

    def lot(color, rel):
        one, two = AXES[color]
        first, second = short(rel[one]), short(rel[two])
        if second == 0:
            return {-1: 0, 1: 1, 2: 3}[first]
        if second == 2:
            return {0: 6, -1: 8, 1: 8, 2: 9}[first]
        return {0: 2, -1: 4, 1: 5, 2: 7}[first]

    LOTS = (2, 2, 4, 2, 4, 4, 2, 4, 4, 2)

    def arrived(kind, number):
        arrive(units(kind, LOTS[number]), w_recv.at[kind, number])

    def start_unit(kind, color, rel, recv_sem, device, half=None):
        ref = unit(kind, color, rel, half)
        pltpu.make_async_remote_copy(
            src_ref=ref, dst_ref=ref, send_sem=w_send.at[kind], recv_sem=recv_sem,
            device_id=device, device_id_type=MESH,
        ).start()
        counts[kind] += 2 if half is None else 1

    def push(kind, color, rel, axis, step, half=None):
        there = dict(rel)
        there[axis] = rel[axis] - step
        sem = w_recv.at[kind, lot(color, there)]
        start_unit(kind, color, rel, sem, {axis: wrap(here[axis] + step)}, half)

    def side(kind, color, rel):
        place = (short(rel["y"]), short(rel["z"]))
        if kind == GU:
            late = (place[0] == 2) + (place[1] == 2)
            sem = side_gu.at[1 if late == 1 and 0 not in place else late if 0 not in place else 0]
        else:
            sem = side_down.at[ORDER.index(place) // 2]
        start_unit(kind, color, rel, sem, {"c": other})

    def at(color, first, second):
        one, two = AXES[color]
        return {one: first, two: second}

    def stage(kind, n):
        if n in (0, 1):
            for color in (0, 1):
                for step in (1, -1):
                    push(kind, color, at(color, 0, 0), AXES[color][n], step)
                if n == 1:
                    side(kind, color, at(color, 0, 0))
        if n == 2:
            arrived(kind, 0)
            arrived(kind, 1)
            for f in (-1, 1):
                for color in (0, 1):
                    push(kind, color, at(color, f, 0), AXES[color][0], -f, (f + 1) // 2)
        if n == 4:
            arrived(kind, 3)
        for f in {2: (-1, 1), 4: (2,)}.get(n, ()):
            for color in (0, 1):
                for step in (1, -1):
                    push(kind, color, at(color, f, 0), AXES[color][1], step)
                side(kind, color, at(color, f, 0))
        for number, first in {3: ((2, 0),), 5: ((4, -1),), 8: ((5, 1),), 6: ((7, 2),)}.get(n, ()):
            arrived(kind, number)
            for s in (-1, 1):
                for color in (0, 1):
                    push(kind, color, at(color, first, s), AXES[color][1], -s, (s + 1) // 2)
            for s in (-1, 1):
                for color in (0, 1):
                    side(kind, color, at(color, first, s))
        for number, firsts in {8: ((6, (0,)),), 6: ((8, (-1, 1)),), 7: ((9, (2,)),)}.get(n, ()):
            arrived(kind, number)
            for first in firsts:
                for color in (0, 1):
                    side(kind, color, at(color, first, 2))

    own = at(0, 0, 0)
    for step in (1, -1):
        push(GU, 0, own, "y", step, 0)
        push(GU, 1, own, "z", step)

    def skip_copy(source, slot, rows, sem, step):
        return pltpu.make_async_remote_copy(
            src_ref=source, dst_ref=SK.at[slot, rows, :],
            send_sem=skip_send.at[0], recv_sem=skip_sem.at[sem],
            device_id={"x": wrap(x + step)}, device_id_type=MESH,
        )

    arrive(skip_ref, in_sem.at[4])
    for i, step in enumerate((1, -1)):
        skip_copy(skip_ref, x, pl.ds(0, 128), i, step).start()

    def skip_arrived(slot, rows, sem):
        arrive(SK.at[slot, rows, :], skip_sem.at[sem])

    def skip_relay(part):
        left, right = wrap(x - 1), wrap(x + 1)
        first, second = pl.ds(part * 32, 32), pl.ds(64 + part * 32, 32)
        if part == 0:
            skip_arrived(left, pl.ds(0, 128), 0)
            skip_arrived(right, pl.ds(0, 128), 1)
        skip_copy(SK.at[left, first, :], left, first, 2 + part, 1).start()
        skip_copy(SK.at[right, second, :], right, second, 2 + part, -1).start()

    i256 = lax.broadcasted_iota(jnp.int32, (256, 256), 0)
    j256 = lax.broadcasted_iota(jnp.int32, (256, 256), 1)
    causal = jnp.logical_and(i256 >= j256, i256 // BLOCK == j256 // BLOCK)
    triangle = jnp.where(causal, 1.0, 0.0).astype(BF16)
    upper_half = lax.broadcasted_iota(jnp.int32, (128, 128), 0) < BLOCK
    arrive(RV, in_sem.at[1])
    arrive(surge_ref, in_sem.at[2])
    arrive(slack_ref, in_sem.at[3])
    closings = []
    for s in range(4):
        rows = slice(s * 256, (s + 1) * 256)
        ig = slack_ref[...] * jax.nn.sigmoid(-r_ref[rows].astype(F32))
        lf = jnp.log1p(-ig) + surge_ref[rows]
        high = lf.astype(BF16)
        rest = lf - high.astype(F32)
        mid = rest.astype(BF16)
        low = (rest - mid.astype(F32)).astype(BF16)
        parts = mm(triangle, jnp.concatenate([high, mid, low], axis=1))
        cum = parts[:, :128] + parts[:, 128:256] + parts[:, 256:]
        CUM[rows] = cum
        IG[rows] = ig
        blocks = cum.reshape(4, BLOCK, HD)
        last = blocks[:, BLOCK - 1 : BLOCK, :]
        closings += [last[b] for b in range(4)]
        keys = (ig * jnp.exp(last - blocks).reshape(256, HD)).astype(BF16)
        for p in range(2):
            pair = keys[p * 128 : (p + 1) * 128]
            none = jnp.zeros_like(pair)
            both = jnp.concatenate(
                [jnp.where(upper_half, pair, none), jnp.where(upper_half, none, pair)], axis=1
            )
            grown = tn(v_ref[s * 256 + p * 128 : s * 256 + (p + 1) * 128], both)
            DS[s * 4 + p * 2] = grown[:, :128]
            DS[s * 4 + p * 2 + 1] = grown[:, 128:]
    state = jnp.zeros((HD, HD), F32)
    passed = jnp.zeros((1, HD), F32)
    offsets = []
    for b in range(16):
        SB[b] = state.astype(BF16)
        offsets.append(passed)
        state = state * jnp.exp(closings[b]) + DS[b]
        passed = passed + closings[b]
    STR[0, 0:128] = state.astype(BF16)
    which = lax.broadcasted_iota(jnp.int32, (16, HD), 0)

    def spread(value):
        high = value.astype(BF16)
        rest = value - high.astype(F32)
        mid = rest.astype(BF16)
        low = rest - mid.astype(F32)
        rows = jnp.where(which == 2, low, 0.0)
        rows = jnp.where(which == 1, mid.astype(F32), rows)
        return jnp.where(which == 0, high.astype(F32), rows).astype(BF16)

    def joined(rows):
        rows = rows.astype(F32)
        return rows[0:1] + rows[1:2] + rows[2:3]

    STR[0, 128:144] = spread(passed)

    for k in range(1, 4):
        pltpu.make_async_remote_copy(
            src_ref=STR.at[0], dst_ref=STR.at[k],
            send_sem=state_send.at[0], recv_sem=state_recv.at[k - 1],
            device_id={"y": wrap(y + k)}, device_id_type=MESH,
        ).start()

    for n in range(8):
        source = emission_ref.at[:, pl.ds(n * 256, 256)]
        pltpu.make_async_copy(source, EB.at[n], e_sem.at[0]).start()
    for step in (1, -1):
        push(GU, 0, own, "y", step, 1)
        push(GU, 1, own, "y", step)
        push(GU, 0, own, "z", step, 0)
    SK[x] = skip_ref[...]
    arrive(QE, in_sem.at[5])
    arrive(gain_ref, in_sem.at[6])
    arrive(norm_gain_ref, in_sem.at[7])
    for s in range(4):
        rows = slice(s * 256, (s + 1) * 256)
        q = q_ref[rows].astype(F32)
        qa = q * jax.nn.sigmoid(q)
        cum = CUM[rows]
        ig = IG[rows]
        blocks = cum.reshape(4, BLOCK, HD)
        middle = blocks[:, BLOCK // 2 : BLOCK // 2 + 1, :]
        centred = (blocks - middle).reshape(256, HD)
        left = (qa * jnp.exp(centred)).astype(BF16)
        right = (ig * jnp.exp(-centred)).astype(BF16)
        scores = jnp.where(causal, nt(left, right), 0.0).astype(BF16)
        local = mm(scores, v_ref[rows])
        faded = qa * jnp.exp(cum)
        faded_by = jnp.concatenate([offsets[s * 4 + b].reshape(1, 1, HD) for b in range(4)], axis=0)
        QC[rows] = (qa * jnp.exp(blocks + faded_by).reshape(256, HD)).astype(BF16)
        faded = faded.astype(BF16)
        for p in range(2):
            pair = faded[p * 128 : (p + 1) * 128]
            none = jnp.zeros_like(pair)
            both = jnp.concatenate(
                [jnp.where(upper_half, pair, none), jnp.where(upper_half, none, pair)], axis=1
            )
            b = s * 4 + p * 2
            carried = nt(both, jnp.concatenate([SB[b], SB[b + 1]], axis=1))
            OL[s * 256 + p * 128 : s * 256 + (p + 1) * 128] = local[p * 128 : (p + 1) * 128] + carried
        emission = e_ref[rows].astype(F32)
        GT[rows] = gain_ref[...] * emission * jax.nn.sigmoid(emission)

    for k in range(1, 4):
        arrive(STR.at[k], state_recv.at[k - 1])
    plane = jnp.zeros((HD, HD), F32)
    plane_log = jnp.zeros((1, HD), F32)
    before, before_log = plane, plane_log
    for yy in range(4):
        slot = wrap(y - yy)
        before = jnp.where(y == yy, plane, before)
        before_log = jnp.where(y == yy, plane_log, before_log)
        log = joined(STR[slot, 128:144])
        plane = plane * jnp.exp(log) + STR[slot, 0:128].astype(F32)
        plane_log = plane_log + log
    TOT[0, 0:128] = plane.astype(BF16)
    TOT[0, 128:144] = spread(plane_log)

    def total_copy(k):
        return pltpu.make_async_remote_copy(
            src_ref=TOT.at[0], dst_ref=TOT.at[k],
            send_sem=total_send.at[k - 1], recv_sem=total_recv.at[k - 1],
            device_id={"z": wrap(z + k)}, device_id_type=MESH,
        )

    for k in range(1, 4):

        @pl.when(z + k < 4)
        def _():
            total_copy(k).start()

        @pl.when(z < k)
        def _():
            TOT[k] = jnp.zeros((144, HD), BF16)

    for step in (1, -1):
        push(GU, 0, own, "z", step, 1)
    for color in (0, 1):
        side(GU, color, own)
    stage(GU, 2)
    for k in range(1, 4):

        @pl.when(z >= k)
        def _():
            arrive(TOT.at[k], total_recv.at[k - 1])

    since = before_log
    for k in range(1, 4):
        before = before + TOT[k, 0:128].astype(F32) * jnp.exp(since)
        since = since + joined(TOT[k, 128:144])
    incoming = before.astype(BF16)
    for s in range(4):
        rows = slice(s * 256, (s + 1) * 256)
        o = OL[rows] + nt(QC[rows], incoming)
        squares = jnp.mean(o * o, axis=-1, keepdims=True)
        mixed = (o * lax.rsqrt(squares + EPSILON) * GT[rows]).astype(BF16)
        for core in (0, 1):
            MIXS[core, s * 128 : (s + 1) * 128] = mixed[core * 128 : (core + 1) * 128]

    head = x * 2 + c
    MX[head] = MIXS[c]

    def mix_copy(source, slab, sem, device):
        pltpu.make_async_remote_copy(
            src_ref=source, dst_ref=MX.at[slab],
            send_sem=mix_send.at[0], recv_sem=mix_recv.at[sem],
            device_id=device, device_id_type=MESH,
        ).start()

    for i, step in enumerate((1, -1)):
        for core in (0, 1):
            mix_copy(MIXS.at[core], head, i * 2 + c, {"x": wrap(x + step), "c": jnp.int32(core)})
    mix_copy(MIXS.at[other], head, 4, {"c": other})

    def mix_arrived(slab, sem):
        arrive(MX.at[slab], mix_recv.at[sem])

    stage(GU, 3)
    skip_relay(0)
    stage(GU, 4)
    left, right = wrap(x - 1), wrap(x + 1)
    mix_arrived(left * 2, 0)
    mix_copy(MX.at[left * 2], left * 2, 5, {"x": right})
    mix_arrived(right * 2 + 1, 3)
    mix_copy(MX.at[right * 2 + 1], right * 2 + 1, 6, {"x": left})
    skip_relay(1)
    stage(GU, 5)
    stage(GU, 8)
    stage(DOWN, 0)
    stage(DOWN, 1)
    arrive(EB, e_sem.at[0])
    opposite = wrap(x + 2)
    mix_arrived(left * 2 + 1, 1)
    mix_arrived(right * 2, 2)
    mix_arrived(x * 2 + other, 4)
    mix_arrived(opposite * 2, 5)
    mix_arrived(opposite * 2 + 1, 6)

    def project(n, carry):
        mixed = jnp.concatenate([MX[h] for h in range(8)], axis=1)
        ACC[n] = mm(mixed, EB[n])
        return carry

    lax.fori_loop(0, 4, project, 0, unroll=True)
    lax.fori_loop(4, 8, project, 0, unroll=True)
    skip_arrived(opposite, pl.ds(0, 64), 2)
    skip_arrived(opposite, pl.ds(64, 64), 3)
    SSQ[...] = jnp.zeros((ROWS, 128), F32)

    def add(n, carry):
        skipped = SK[:, :, pl.ds(pl.multiple_of(n * 256, 256), 256)].reshape(ROWS, 256)
        stream = (skipped.astype(F32) + ACC[n]).astype(BF16)
        STREAM[n] = stream
        wide = stream.astype(F32)
        wide = wide * wide
        SSQ[...] += wide[:, :128] + wide[:, 128:]
        return carry

    lax.fori_loop(0, 8, add, 0)
    scale = lax.rsqrt(jnp.sum(SSQ[...], axis=1, keepdims=True) * (1.0 / D) + EPSILON)

    for n in range(8):
        gain = norm_gain_ref[:, n * 256 : (n + 1) * 256]
        NORM[n] = (STREAM[n].astype(F32) * scale * gain).astype(BF16)

    def await_sides(group):
        arrive(units(GU, (22, 8, 2)[group]), side_gu.at[group])

    def chunk(xi):
        return pl.ds(pl.multiple_of(xi * 128, 128), 128)

    def silu(a):
        return a * jax.nn.sigmoid(a)

    def gate_up(planes, first, last, begin=0, end=6, chunks=(0, 1, 2, 3)):
        tiles, rows = [], ([], [])
        for part in planes:
            if isinstance(part, int):
                place = wrap(z + part)
                tiles += [(place * 2, slice(None)), (place * 2 + 1, slice(None))]
                start, size = place * 512, 512
            else:
                place = wrap(z + part[1]) * 4 + wrap(y + part[0])
                lanes = pl.ds(pl.multiple_of(lax.rem(place, 2) * 128, 128), 128)
                tiles.append((place // 2, lanes))
                start, size = place * 128, 128
            for h in (0, 1):
                rows[h].append(pl.ds(pl.multiple_of(h * D + start, 128), size))

        def some(ref, t, lanes=slice(None)):
            if len(chunks) == 4:
                return ref[t, :, lanes]
            return jnp.concatenate([ref[t, chunk(wrap(x + k)), lanes] for k in chunks], axis=0)

        def put(ref, t, value):
            if len(chunks) == 4:
                ref[t] = value
                return
            for n, k in enumerate(chunks):
                ref[t, chunk(wrap(x + k))] = value[n * 128 : (n + 1) * 128]

        def partial(weights):
            normed = [some(NORM, t, lanes) for t, lanes in tiles]
            return mm(jnp.concatenate(normed, axis=1), jnp.concatenate(weights, axis=0))

        def tile(j, carry):
            columns = pl.ds(pl.multiple_of(j * 256, 256), 256)
            for h in (0, 1):
                t = h * 5 + j
                part = partial([W[deep, columns] for deep in rows[h]])
                if not first:
                    part = part + some(ACC, t)
                if not last:
                    put(ACC, t, part)
                else:
                    put(HID, t, (silu(part[:, :128]) * part[:, 128:]).astype(BF16))
            return carry

        lax.fori_loop(begin, min(end, 5), tile, 0, unroll=True)
        if end < 6:
            return
        part = partial(
            [
                jnp.concatenate([W[one, 1280:1408], W[two, 1280:1408]], axis=1)
                for one, two in zip(*rows)
            ]
        )
        if not first:
            part = part + some(ACC, 10)
        if not last:
            put(ACC, 10, part)
        else:
            lane = lax.broadcasted_iota(jnp.int32, (128 * len(chunks), 128), 1)
            a, b = part[:, :128], part[:, 128:]
            gates = jnp.where(lane < 64, a, pltpu.roll(b, 64, 1))
            ups = jnp.where(lane < 64, pltpu.roll(a, 64, 1), b)
            put(HID, 10, (silu(gates) * ups).astype(BF16))

    def column_of(i):
        dy, dz = ORDER[i]
        return wrap(z + dz) * 4 + wrap(y + dy)

    def down_weights(i):
        def block(at_column):
            one, two = at_column, 16 + at_column
            return jnp.concatenate(
                [DN[one, 0:640], DN[two, 0:640], DN[one, 640:704], DN[two, 640:704]], axis=0
            )

        return jnp.concatenate([block(column_of(2 * i)), block(column_of(2 * i + 1))], axis=1)

    def send_far(i, far):
        for half, step in enumerate((1, -1)):
            OPPS[i, half] = far[:, half * 128 : (half + 1) * 128].astype(BF16)
            pltpu.make_async_remote_copy(
                src_ref=OPPS.at[i, half], dst_ref=OPPR.at[i, half],
                send_sem=opp_send.at[0], recv_sem=opp_recv.at[i],
                device_id={"x": wrap(x + step)}, device_id_type=MESH,
            ).start()

    def send_half(i, half, columns):
        pltpu.make_async_remote_copy(
            src_ref=NBS.at[i, half, columns], dst_ref=NBR.at[i, half, columns],
            send_sem=nb_send.at[0], recv_sem=nb_recv.at[i],
            device_id={"x": wrap(x + 1 - 2 * half)}, device_id_type=MESH,
        ).start()

    def send_near(i, near):
        for half in (0, 1):
            rest = 1 - half
            NBS[i, half, rest] = near[half][:, rest * 128 : (rest + 1) * 128].astype(BF16)
            send_half(i, half, rest)
            PN[half, i] = near[half][:, half * 128 : (half + 1) * 128]

    def down(i):
        arrive(units(DOWN, 4), side_down.at[i])
        res = RES.at[i % 2]
        res[...] = mm(jnp.concatenate([HID[t] for t in range(11)], axis=1), down_weights(i))
        send_far(i, res[chunk(opposite)])
        OWN[i] = res[chunk(x)]
        send_near(i, (res[chunk(right)], res[chunk(left)]))

    def down_far(i):
        arrive(units(DOWN, 4), side_down.at[i])
        hidden = jnp.concatenate([HID[t, chunk(opposite)] for t in range(11)], axis=1)
        send_far(i, mm(hidden, down_weights(i)))

    def down_near(i):
        hidden = [
            jnp.concatenate([HID[t, chunk(k)] for t in range(11)], axis=1) for k in (x, right, left)
        ]
        near = mm(jnp.concatenate(hidden, axis=0), down_weights(i))
        OWN[i] = near[:128]
        send_near(i, (near[128:256], near[256:]))

    def hand_on(i):
        arrive(OPPR.at[i], opp_recv.at[i])
        for half in (0, 1):
            NBS[i, half, half] = (PN[half, i] + OPPR[i, half].astype(F32)).astype(BF16)
            send_half(i, half, half)

    def finish(i):
        arrive(NBR.at[i], nb_recv.at[i])
        for half in (0, 1):
            column = column_of(2 * i + half)
            lanes = pl.ds(pl.multiple_of(lax.rem(column, 2) * 128, 128), 128)
            stream = STREAM[column // 2, chunk(x), lanes].astype(F32)
            summed = OWN[i, :, half * 128 : (half + 1) * 128]
            summed = summed + NBR[i, 0, half].astype(F32) + NBR[i, 1, half].astype(F32)
            columns = pl.ds(pl.multiple_of(column * 128, 128), 128)
            out_ref[:, columns] = (stream + summed).astype(BF16)

    await_sides(0)
    gate_up((0, (0, -1), (-1, -1), (1, -1), (0, 1), (-1, 1), (1, 1), (0, 2)), True, False, 0, 3)
    stage(GU, 6)
    gate_up((0, (0, -1), (-1, -1), (1, -1), (0, 1), (-1, 1), (1, 1), (0, 2)), True, False, 3, 6)
    stage(DOWN, 2)
    await_sides(1)
    gate_up(((2, -1), (2, 1), (-1, 2), (1, 2)), False, False, 0, 3)
    stage(GU, 7)
    gate_up(((2, -1), (2, 1), (-1, 2), (1, 2)), False, False, 3, 6)
    stage(DOWN, 3)
    await_sides(2)
    gate_up(((2, 2),), False, True, chunks=(2,))
    down_far(0)
    down_far(1)
    stage(DOWN, 4)
    gate_up(((2, 2),), False, True, chunks=(0, 1, -1))
    down_near(0)
    stage(DOWN, 5)
    down_near(1)
    hand_on(0)
    stage(DOWN, 8)
    down(2)
    down(3)
    hand_on(1)
    down(4)
    stage(DOWN, 6)
    hand_on(2)
    down(5)
    hand_on(3)
    down(6)
    stage(DOWN, 7)
    hand_on(4)
    down(7)
    hand_on(5)
    finish(0)
    hand_on(6)
    finish(1)
    finish(2)
    hand_on(7)
    finish(3)
    finish(4)
    finish(5)
    finish(6)
    finish(7)

    for kind in (GU, DOWN):
        arrive(units(kind, counts[kind] // 2), w_send.at[kind])
    arrive(STR.at[pl.ds(0, 3)], state_send.at[0])
    arrive(SK.at[pl.ds(0, 3)], skip_send.at[0])
    arrive(MX.at[pl.ds(0, 7)], mix_send.at[0])
    arrive(OPPS, opp_send.at[0])
    arrive(NBS, nb_send.at[0])
    for k in range(1, 4):

        @pl.when(z + k < 4)
        def _():
            total_copy(k).wait_send()


def on_device(skip, q, r, v, e, slack, surge, gain, emission, norm_gain, gate, up, down):
    vmem = pl.BlockSpec(memory_space=pltpu.VMEM)
    dma = pltpu.SemaphoreType.DMA
    return pl.pallas_call(
        kernel,
        out_shape=jax.ShapeDtypeStruct((128, D), BF16),
        in_specs=[pl.BlockSpec(memory_space=pltpu.HBM)] * 13,
        out_specs=vmem,
        scratch_shapes=[
            pltpu.VMEM((128, D), BF16),
            pltpu.VMEM((2, TOK, HD), BF16),
            pltpu.VMEM((2, TOK, HD), BF16),
            pltpu.VMEM((1, HD), F32),
            pltpu.VMEM((TOK, HD), F32),
            pltpu.VMEM((1, HD), F32),
            pltpu.VMEM((1, D), F32),
            pltpu.VMEM((3, 704, 128), BF16),
            pltpu.VMEM((2 * D, 1408), BF16),
            pltpu.VMEM((32, 704, 128), BF16),
            pltpu.VMEM((8, 1024, 256), BF16),
            pltpu.VMEM((4, 128, D), BF16),
            pltpu.VMEM((8, ROWS, 128), BF16),
            pltpu.VMEM((2, ROWS, 128), BF16),
            pltpu.VMEM((8, ROWS, 256), BF16),
            pltpu.VMEM((8, ROWS, 256), BF16),
            pltpu.VMEM((11, ROWS, 256), F32),
            pltpu.VMEM((11, ROWS, 128), BF16),
            pltpu.VMEM((ROWS, 128), F32),
            pltpu.VMEM((2, ROWS, 256), F32),
            pltpu.VMEM((TOK, HD), F32),
            pltpu.VMEM((TOK, HD), F32),
            pltpu.VMEM((16, HD, HD), F32),
            pltpu.VMEM((16, HD, HD), BF16),
            pltpu.VMEM((4, 144, HD), BF16),
            pltpu.VMEM((4, 144, HD), BF16),
            pltpu.VMEM((TOK, HD), F32),
            pltpu.VMEM((TOK, HD), BF16),
            pltpu.VMEM((TOK, HD), F32),
            pltpu.VMEM((8, 2, 128, 128), BF16),
            pltpu.VMEM((8, 2, 128, 128), BF16),
            pltpu.VMEM((8, 128, 256), F32),
            pltpu.VMEM((2, 8, 128, 128), F32),
            pltpu.VMEM((8, 2, 2, 128, 128), BF16),
            pltpu.VMEM((8, 2, 2, 128, 128), BF16),
            dma((2, 10)),
            dma((3,)),
            dma((8,)),
            dma((2,)),
            dma((3,)),
            dma((1,)),
            dma((3,)),
            dma((3,)),
            dma((4,)),
            dma((1,)),
            dma((7,)),
            dma((1,)),
            dma((1,)),
            dma((8,)),
            dma((8,)),
            dma((1,)),
            dma((8,)),
            dma((1,)),
        ],
        compiler_params=pltpu.CompilerParams(
            collective_id=0, has_side_effects=True, vmem_limit_bytes=54000000
        ),
        name="layer",
    )(
        *(
            pltpu.with_memory_space_constraint(a, pltpu.HBM)
            for a in (skip, q, r, v, e, slack.reshape(1, -1), surge, gain.reshape(1, -1), emission,
                      norm_gain.reshape(1, -1), gate.T, up.T, down)
        )
    )


def solution(mesh):
    split = Mesh(mesh.devices.reshape(4, 4, 4, 2), ("z", "y", "x", "c"))
    sp, tp = ("z", "y"), ("x", "c")
    return jax.shard_map(
        on_device,
        mesh=split,
        in_specs=(
            P(sp + tp, None),
            P(sp, tp),
            P(sp, tp),
            P(sp, tp),
            P(sp, tp),
            P(tp),
            P(sp, tp),
            P(tp),
            P(),
            P(),
            P(sp, tp),
            P(sp, tp),
            P(tp, sp),
        ),
        out_specs=P(sp + tp, None),
        check_vma=False,
    )
```

```python
import functools

import jax
import jax.numpy as jnp
from jax import lax
from jax.experimental import pallas as pl
from jax.experimental.pallas import tpu as pltpu
from jax.sharding import Mesh
from jax.sharding import PartitionSpec as P

MESH = pl.DeviceIdType.MESH
F32 = jnp.float32
BF16 = jnp.bfloat16
EPSILON = 1e-06
HD = 128
BLOCK = 64
TOK = 1024
ROWS = 512
D = 2048
GU, DOWN = 0, 1


def wrap(value, n=4):
    return lax.rem(value + n, n)


def nt(a, b):
    return lax.dot_general(a, b, (((1,), (1,)), ((), ())), preferred_element_type=F32)


def tn(a, b):
    return lax.dot_general(a, b, (((0,), (0,)), ((), ())), preferred_element_type=F32)


def mm(a, b):
    return jnp.dot(a, b, preferred_element_type=F32)


def kernel(
    skip_in, q_in, r_in, v_in, e_in, slack_in, surge_in, gain_in, emission_ref,
    norm_gain_in, gate_in, up_in, down_in,
    out_ref,
    skip_ref, QE, RV, slack_ref, surge_ref, gain_ref, norm_gain_ref, OWNED,
    W, DN, EB, SK, MX, MIXS, STREAM, NORM, ACC, HID, SSQ, RES,
    CUM, IG, DS, SB, STR, TOT, OL, QC, GT,
    OPPS, OPPR, OWN, PN, NBS, NBR,
    w_recv, side_gu, side_down, w_send, state_recv, state_send, total_recv, total_send,
    skip_sem, skip_send, mix_recv, mix_send, e_sem, in_sem, opp_recv, opp_send, nb_recv, nb_send,
):
    z, y, x, c = (lax.axis_index(name) for name in ("z", "y", "x", "c"))
    sp = z * 4 + y
    other = 1 - c
    q_ref, e_ref, r_ref, v_ref = QE.at[0], QE.at[1], RV.at[0], RV.at[1]
    gate_ref, up_ref, down_ref = (OWNED.at[i] for i in range(3))

    def arrive(ref, sem):
        pltpu.make_async_copy(ref, ref, sem).wait()

    barrier = pltpu.get_barrier_semaphore()
    for k in range(1, 4):
        pl.semaphore_signal(barrier, inc=1, device_id={"y": wrap(y + k)}, device_id_type=MESH)
        pl.semaphore_signal(barrier, inc=1, device_id={"z": wrap(z + k)}, device_id_type=MESH)
    for step in (1, -1):
        for core in (0, 1):
            pl.semaphore_signal(barrier, inc=1, device_id={"x": wrap(x + step), "c": jnp.int32(core)}, device_id_type=MESH)
    pl.semaphore_signal(barrier, inc=1, device_id={"c": other}, device_id_type=MESH)

    def load(source, target, sem):
        pltpu.make_async_copy(source, target, in_sem.at[sem]).start()

    load(gate_in, gate_ref, 0)
    load(up_in, up_ref, 0)
    load(down_in, down_ref, 0)
    load(r_in, r_ref, 1)
    load(v_in, v_ref, 1)
    load(surge_in, surge_ref, 2)
    load(slack_in, slack_ref, 3)
    load(skip_in, skip_ref, 4)
    load(q_in, q_ref, 5)
    load(e_in, e_ref, 5)
    load(gain_in, gain_ref, 6)
    load(norm_gain_in, norm_gain_ref, 7)

    arrive(OWNED, in_sem.at[0])
    own_rows = pl.ds(pl.multiple_of(c * D + sp * 128, 128), 128)
    for j in range(5):
        W[own_rows, j * 256 : j * 256 + 128] = gate_ref[j * 128 : (j + 1) * 128].T
        W[own_rows, j * 256 + 128 : (j + 1) * 256] = up_ref[j * 128 : (j + 1) * 128].T
    W[own_rows, 1280:1408] = jnp.concatenate([gate_ref[640:704], up_ref[640:704]], axis=0).T
    DN[c * 16 + sp] = down_ref[...]

    pl.semaphore_wait(barrier, 11)

    AXES = {0: ("y", "z"), 1: ("z", "y")}
    ORDER = (
        (0, 0), (1, 0), (-1, 0), (0, 1), (0, -1), (-1, -1), (1, 1), (1, -1),
        (-1, 1), (2, 0), (0, 2), (2, 1), (2, -1), (1, 2), (-1, 2), (2, 2),
    )
    here = {"z": z, "y": y}

    def short(offset):
        return (offset + 1) % 4 - 1

    def unit(kind, color, rel, half):
        origin = wrap(z + rel["z"]) * 4 + wrap(y + rel["y"])
        size, skipped = (1, 0) if half is None else (2, half)
        if kind == GU:
            start = pl.multiple_of(c * D + origin * 128 + color * 64 + skipped * 32, 32)
            return W.at[pl.ds(start, 64 // size), :]
        return DN.at[c * 16 + origin, pl.ds(color * 352 + skipped * 176, 352 // size), :]

    def units(kind, count):
        return W.at[pl.ds(0, 64 * count), :] if kind == GU else DN.at[pl.ds(0, count // 2)]

    counts = {GU: 0, DOWN: 0}

    def lot(color, rel):
        one, two = AXES[color]
        first, second = short(rel[one]), short(rel[two])
        if second == 0:
            return {-1: 0, 1: 1, 2: 3}[first]
        if second == 2:
            return {0: 6, -1: 8, 1: 8, 2: 9}[first]
        return {0: 2, -1: 4, 1: 5, 2: 7}[first]

    LOTS = (2, 2, 4, 2, 4, 4, 2, 4, 4, 2)

    def arrived(kind, number):
        arrive(units(kind, LOTS[number]), w_recv.at[kind, number])

    def start_unit(kind, color, rel, recv_sem, device, half=None):
        ref = unit(kind, color, rel, half)
        pltpu.make_async_remote_copy(
            src_ref=ref, dst_ref=ref, send_sem=w_send.at[kind], recv_sem=recv_sem,
            device_id=device, device_id_type=MESH,
        ).start()
        counts[kind] += 2 if half is None else 1

    def push(kind, color, rel, axis, step, half=None):
        there = dict(rel)
        there[axis] = rel[axis] - step
        sem = w_recv.at[kind, lot(color, there)]
        start_unit(kind, color, rel, sem, {axis: wrap(here[axis] + step)}, half)

    def side(kind, color, rel):
        place = (short(rel["y"]), short(rel["z"]))
        if kind == GU:
            late = (place[0] == 2) + (place[1] == 2)
            sem = side_gu.at[1 if late == 1 and 0 not in place else late if 0 not in place else 0]
        else:
            sem = side_down.at[ORDER.index(place) // 2]
        start_unit(kind, color, rel, sem, {"c": other})

    def at(color, first, second):
        one, two = AXES[color]
        return {one: first, two: second}

    def stage(kind, n):
        if n in (0, 1):
            for color in (0, 1):
                for step in (1, -1):
                    push(kind, color, at(color, 0, 0), AXES[color][n], step)
                if n == 1:
                    side(kind, color, at(color, 0, 0))
        if n == 2:
            arrived(kind, 0)
            arrived(kind, 1)
            for f in (-1, 1):
                for color in (0, 1):
                    push(kind, color, at(color, f, 0), AXES[color][0], -f, (f + 1) // 2)
        if n == 4:
            arrived(kind, 3)
        for f in {2: (-1, 1), 4: (2,)}.get(n, ()):
            for color in (0, 1):
                for step in (1, -1):
                    push(kind, color, at(color, f, 0), AXES[color][1], step)
                side(kind, color, at(color, f, 0))
        for number, first in {3: ((2, 0),), 5: ((4, -1),), 8: ((5, 1),), 6: ((7, 2),)}.get(n, ()):
            arrived(kind, number)
            for s in (-1, 1):
                for color in (0, 1):
                    push(kind, color, at(color, first, s), AXES[color][1], -s, (s + 1) // 2)
            for s in (-1, 1):
                for color in (0, 1):
                    side(kind, color, at(color, first, s))
        for number, firsts in {8: ((6, (0,)),), 6: ((8, (-1, 1)),), 7: ((9, (2,)),)}.get(n, ()):
            arrived(kind, number)
            for first in firsts:
                for color in (0, 1):
                    side(kind, color, at(color, first, 2))

    own = at(0, 0, 0)
    for step in (1, -1):
        push(GU, 0, own, "y", step, 0)
        push(GU, 1, own, "z", step)

    def skip_copy(source, slot, rows, sem, step):
        return pltpu.make_async_remote_copy(
            src_ref=source, dst_ref=SK.at[slot, rows, :],
            send_sem=skip_send.at[0], recv_sem=skip_sem.at[sem],
            device_id={"x": wrap(x + step)}, device_id_type=MESH,
        )

    arrive(skip_ref, in_sem.at[4])
    for i, step in enumerate((1, -1)):
        skip_copy(skip_ref, x, pl.ds(0, 128), i, step).start()

    def skip_arrived(slot, rows, sem):
        arrive(SK.at[slot, rows, :], skip_sem.at[sem])

    def skip_relay(part):
        left, right = wrap(x - 1), wrap(x + 1)
        first, second = pl.ds(part * 32, 32), pl.ds(64 + part * 32, 32)
        if part == 0:
            skip_arrived(left, pl.ds(0, 128), 0)
            skip_arrived(right, pl.ds(0, 128), 1)
        skip_copy(SK.at[left, first, :], left, first, 2 + part, 1).start()
        skip_copy(SK.at[right, second, :], right, second, 2 + part, -1).start()

    i256 = lax.broadcasted_iota(jnp.int32, (256, 256), 0)
    j256 = lax.broadcasted_iota(jnp.int32, (256, 256), 1)
    causal = jnp.logical_and(i256 >= j256, i256 // BLOCK == j256 // BLOCK)
    triangle = jnp.where(causal, 1.0, 0.0).astype(BF16)
    upper_half = lax.broadcasted_iota(jnp.int32, (128, 128), 0) < BLOCK
    arrive(RV, in_sem.at[1])
    arrive(surge_ref, in_sem.at[2])
    arrive(slack_ref, in_sem.at[3])
    closings = []
    for s in range(4):
        rows = slice(s * 256, (s + 1) * 256)
        ig = slack_ref[...] * jax.nn.sigmoid(-r_ref[rows].astype(F32))
        lf = jnp.log1p(-ig) + surge_ref[rows]
        high = lf.astype(BF16)
        rest = lf - high.astype(F32)
        mid = rest.astype(BF16)
        low = (rest - mid.astype(F32)).astype(BF16)
        parts = mm(triangle, jnp.concatenate([high, mid, low], axis=1))
        cum = parts[:, :128] + parts[:, 128:256] + parts[:, 256:]
        CUM[rows] = cum
        IG[rows] = ig
        blocks = cum.reshape(4, BLOCK, HD)
        last = blocks[:, BLOCK - 1 : BLOCK, :]
        closings += [last[b] for b in range(4)]
        keys = (ig * jnp.exp(last - blocks).reshape(256, HD)).astype(BF16)
        for p in range(2):
            pair = keys[p * 128 : (p + 1) * 128]
            none = jnp.zeros_like(pair)
            both = jnp.concatenate(
                [jnp.where(upper_half, pair, none), jnp.where(upper_half, none, pair)], axis=1
            )
            grown = tn(v_ref[s * 256 + p * 128 : s * 256 + (p + 1) * 128], both)
            DS[s * 4 + p * 2] = grown[:, :128]
            DS[s * 4 + p * 2 + 1] = grown[:, 128:]
    state = jnp.zeros((HD, HD), F32)
    passed = jnp.zeros((1, HD), F32)
    offsets = []
    for b in range(16):
        SB[b] = state.astype(BF16)
        offsets.append(passed)
        state = state * jnp.exp(closings[b]) + DS[b]
        passed = passed + closings[b]
    STR[0, 0:128] = state.astype(BF16)
    which = lax.broadcasted_iota(jnp.int32, (16, HD), 0)

    def spread(value):
        high = value.astype(BF16)
        rest = value - high.astype(F32)
        mid = rest.astype(BF16)
        low = rest - mid.astype(F32)
        rows = jnp.where(which == 2, low, 0.0)
        rows = jnp.where(which == 1, mid.astype(F32), rows)
        return jnp.where(which == 0, high.astype(F32), rows).astype(BF16)

    def joined(rows):
        rows = rows.astype(F32)
        return rows[0:1] + rows[1:2] + rows[2:3]

    STR[0, 128:144] = spread(passed)

    for k in range(1, 4):
        pltpu.make_async_remote_copy(
            src_ref=STR.at[0], dst_ref=STR.at[k],
            send_sem=state_send.at[0], recv_sem=state_recv.at[k - 1],
            device_id={"y": wrap(y + k)}, device_id_type=MESH,
        ).start()

    for n in range(8):
        source = emission_ref.at[:, pl.ds(n * 256, 256)]
        pltpu.make_async_copy(source, EB.at[n], e_sem.at[0]).start()
    for step in (1, -1):
        push(GU, 0, own, "y", step, 1)
        push(GU, 1, own, "y", step)
        push(GU, 0, own, "z", step, 0)
    SK[x] = skip_ref[...]
    arrive(QE, in_sem.at[5])
    arrive(gain_ref, in_sem.at[6])
    arrive(norm_gain_ref, in_sem.at[7])
    for s in range(4):
        rows = slice(s * 256, (s + 1) * 256)
        q = q_ref[rows].astype(F32)
        qa = q * jax.nn.sigmoid(q)
        cum = CUM[rows]
        ig = IG[rows]
        blocks = cum.reshape(4, BLOCK, HD)
        middle = blocks[:, BLOCK // 2 : BLOCK // 2 + 1, :]
        centred = (blocks - middle).reshape(256, HD)
        left = (qa * jnp.exp(centred)).astype(BF16)
        right = (ig * jnp.exp(-centred)).astype(BF16)
        scores = jnp.where(causal, nt(left, right), 0.0).astype(BF16)
        local = mm(scores, v_ref[rows])
        faded = qa * jnp.exp(cum)
        faded_by = jnp.concatenate([offsets[s * 4 + b].reshape(1, 1, HD) for b in range(4)], axis=0)
        QC[rows] = (qa * jnp.exp(blocks + faded_by).reshape(256, HD)).astype(BF16)
        faded = faded.astype(BF16)
        for p in range(2):
            pair = faded[p * 128 : (p + 1) * 128]
            none = jnp.zeros_like(pair)
            both = jnp.concatenate(
                [jnp.where(upper_half, pair, none), jnp.where(upper_half, none, pair)], axis=1
            )
            b = s * 4 + p * 2
            carried = nt(both, jnp.concatenate([SB[b], SB[b + 1]], axis=1))
            OL[s * 256 + p * 128 : s * 256 + (p + 1) * 128] = local[p * 128 : (p + 1) * 128] + carried
        emission = e_ref[rows].astype(F32)
        GT[rows] = gain_ref[...] * emission * jax.nn.sigmoid(emission)

    for k in range(1, 4):
        arrive(STR.at[k], state_recv.at[k - 1])
    plane = jnp.zeros((HD, HD), F32)
    plane_log = jnp.zeros((1, HD), F32)
    before, before_log = plane, plane_log
    for yy in range(4):
        slot = wrap(y - yy)
        before = jnp.where(y == yy, plane, before)
        before_log = jnp.where(y == yy, plane_log, before_log)
        log = joined(STR[slot, 128:144])
        plane = plane * jnp.exp(log) + STR[slot, 0:128].astype(F32)
        plane_log = plane_log + log
    TOT[0, 0:128] = plane.astype(BF16)
    TOT[0, 128:144] = spread(plane_log)

    def total_copy(k):
        return pltpu.make_async_remote_copy(
            src_ref=TOT.at[0], dst_ref=TOT.at[k],
            send_sem=total_send.at[k - 1], recv_sem=total_recv.at[k - 1],
            device_id={"z": wrap(z + k)}, device_id_type=MESH,
        )

    for k in range(1, 4):

        @pl.when(z + k < 4)
        def _():
            total_copy(k).start()

        @pl.when(z < k)
        def _():
            TOT[k] = jnp.zeros((144, HD), BF16)

    for step in (1, -1):
        push(GU, 0, own, "z", step, 1)
    for color in (0, 1):
        side(GU, color, own)
    stage(GU, 2)
    for k in range(1, 4):

        @pl.when(z >= k)
        def _():
            arrive(TOT.at[k], total_recv.at[k - 1])

    since = before_log
    for k in range(1, 4):
        before = before + TOT[k, 0:128].astype(F32) * jnp.exp(since)
        since = since + joined(TOT[k, 128:144])
    incoming = before.astype(BF16)
    for s in range(4):
        rows = slice(s * 256, (s + 1) * 256)
        o = OL[rows] + nt(QC[rows], incoming)
        squares = jnp.mean(o * o, axis=-1, keepdims=True)
        mixed = (o * lax.rsqrt(squares + EPSILON) * GT[rows]).astype(BF16)
        for core in (0, 1):
            MIXS[core, s * 128 : (s + 1) * 128] = mixed[core * 128 : (core + 1) * 128]

    head = x * 2 + c
    MX[head] = MIXS[c]

    def mix_copy(source, slab, sem, device):
        pltpu.make_async_remote_copy(
            src_ref=source, dst_ref=MX.at[slab],
            send_sem=mix_send.at[0], recv_sem=mix_recv.at[sem],
            device_id=device, device_id_type=MESH,
        ).start()

    for i, step in enumerate((1, -1)):
        for core in (0, 1):
            mix_copy(MIXS.at[core], head, i * 2 + c, {"x": wrap(x + step), "c": jnp.int32(core)})
    mix_copy(MIXS.at[other], head, 4, {"c": other})

    def mix_arrived(slab, sem):
        arrive(MX.at[slab], mix_recv.at[sem])

    stage(GU, 3)
    skip_relay(0)
    stage(GU, 4)
    left, right = wrap(x - 1), wrap(x + 1)
    mix_arrived(left * 2, 0)
    mix_copy(MX.at[left * 2], left * 2, 5, {"x": right})
    mix_arrived(right * 2 + 1, 3)
    mix_copy(MX.at[right * 2 + 1], right * 2 + 1, 6, {"x": left})
    skip_relay(1)
    stage(GU, 5)
    stage(GU, 8)
    stage(DOWN, 0)
    stage(DOWN, 1)
    arrive(EB, e_sem.at[0])
    opposite = wrap(x + 2)
    mix_arrived(left * 2 + 1, 1)
    mix_arrived(right * 2, 2)
    mix_arrived(x * 2 + other, 4)
    mix_arrived(opposite * 2, 5)
    mix_arrived(opposite * 2 + 1, 6)

    def project(n, carry):
        mixed = jnp.concatenate([MX[h] for h in range(8)], axis=1)
        ACC[n] = mm(mixed, EB[n])
        return carry

    lax.fori_loop(0, 4, project, 0, unroll=True)
    lax.fori_loop(4, 8, project, 0, unroll=True)
    skip_arrived(opposite, pl.ds(0, 64), 2)
    skip_arrived(opposite, pl.ds(64, 64), 3)
    SSQ[...] = jnp.zeros((ROWS, 128), F32)

    def add(n, carry):
        skipped = SK[:, :, pl.ds(pl.multiple_of(n * 256, 256), 256)].reshape(ROWS, 256)
        stream = (skipped.astype(F32) + ACC[n]).astype(BF16)
        STREAM[n] = stream
        wide = stream.astype(F32)
        wide = wide * wide
        SSQ[...] += wide[:, :128] + wide[:, 128:]
        return carry

    lax.fori_loop(0, 8, add, 0)
    scale = lax.rsqrt(jnp.sum(SSQ[...], axis=1, keepdims=True) * (1.0 / D) + EPSILON)

    for n in range(8):
        gain = norm_gain_ref[:, n * 256 : (n + 1) * 256]
        NORM[n] = (STREAM[n].astype(F32) * scale * gain).astype(BF16)

    def await_sides(group):
        arrive(units(GU, (22, 8, 2)[group]), side_gu.at[group])

    def chunk(xi):
        return pl.ds(pl.multiple_of(xi * 128, 128), 128)

    def silu(a):
        return a * jax.nn.sigmoid(a)

    def gate_up(planes, first, last, begin=0, end=6, chunks=(0, 1, 2, 3)):
        tiles, rows = [], ([], [])
        for part in planes:
            if isinstance(part, int):
                place = wrap(z + part)
                tiles += [(place * 2, slice(None)), (place * 2 + 1, slice(None))]
                start, size = place * 512, 512
            else:
                place = wrap(z + part[1]) * 4 + wrap(y + part[0])
                lanes = pl.ds(pl.multiple_of(lax.rem(place, 2) * 128, 128), 128)
                tiles.append((place // 2, lanes))
                start, size = place * 128, 128
            for h in (0, 1):
                rows[h].append(pl.ds(pl.multiple_of(h * D + start, 128), size))

        def some(ref, t, lanes=slice(None)):
            if len(chunks) == 4:
                return ref[t, :, lanes]
            return jnp.concatenate([ref[t, chunk(wrap(x + k)), lanes] for k in chunks], axis=0)

        def put(ref, t, value):
            if len(chunks) == 4:
                ref[t] = value
                return
            for n, k in enumerate(chunks):
                ref[t, chunk(wrap(x + k))] = value[n * 128 : (n + 1) * 128]

        def partial(weights):
            normed = [some(NORM, t, lanes) for t, lanes in tiles]
            return mm(jnp.concatenate(normed, axis=1), jnp.concatenate(weights, axis=0))

        def tile(j, carry):
            columns = pl.ds(pl.multiple_of(j * 256, 256), 256)
            for h in (0, 1):
                t = h * 5 + j
                part = partial([W[deep, columns] for deep in rows[h]])
                if not first:
                    part = part + some(ACC, t)
                if not last:
                    put(ACC, t, part)
                else:
                    put(HID, t, (silu(part[:, :128]) * part[:, 128:]).astype(BF16))
            return carry

        lax.fori_loop(begin, min(end, 5), tile, 0, unroll=True)
        if end < 6:
            return
        part = partial(
            [
                jnp.concatenate([W[one, 1280:1408], W[two, 1280:1408]], axis=1)
                for one, two in zip(*rows)
            ]
        )
        if not first:
            part = part + some(ACC, 10)
        if not last:
            put(ACC, 10, part)
        else:
            lane = lax.broadcasted_iota(jnp.int32, (128 * len(chunks), 128), 1)
            a, b = part[:, :128], part[:, 128:]
            gates = jnp.where(lane < 64, a, pltpu.roll(b, 64, 1))
            ups = jnp.where(lane < 64, pltpu.roll(a, 64, 1), b)
            put(HID, 10, (silu(gates) * ups).astype(BF16))

    def column_of(i):
        dy, dz = ORDER[i]
        return wrap(z + dz) * 4 + wrap(y + dy)

    def down_weights(i):
        def block(at_column):
            one, two = at_column, 16 + at_column
            return jnp.concatenate(
                [DN[one, 0:640], DN[two, 0:640], DN[one, 640:704], DN[two, 640:704]], axis=0
            )

        return jnp.concatenate([block(column_of(2 * i)), block(column_of(2 * i + 1))], axis=1)

    def send_far(i, far):
        for half, step in enumerate((1, -1)):
            OPPS[i, half] = far[:, half * 128 : (half + 1) * 128].astype(BF16)
            pltpu.make_async_remote_copy(
                src_ref=OPPS.at[i, half], dst_ref=OPPR.at[i, half],
                send_sem=opp_send.at[0], recv_sem=opp_recv.at[i],
                device_id={"x": wrap(x + step)}, device_id_type=MESH,
            ).start()

    def send_half(i, half, columns):
        pltpu.make_async_remote_copy(
            src_ref=NBS.at[i, half, columns], dst_ref=NBR.at[i, half, columns],
            send_sem=nb_send.at[0], recv_sem=nb_recv.at[i],
            device_id={"x": wrap(x + 1 - 2 * half)}, device_id_type=MESH,
        ).start()

    def send_near(i, near):
        for half in (0, 1):
            rest = 1 - half
            NBS[i, half, rest] = near[half][:, rest * 128 : (rest + 1) * 128].astype(BF16)
            send_half(i, half, rest)
            PN[half, i] = near[half][:, half * 128 : (half + 1) * 128]

    def down(i):
        arrive(units(DOWN, 4), side_down.at[i])
        res = RES.at[i % 2]
        res[...] = mm(jnp.concatenate([HID[t] for t in range(11)], axis=1), down_weights(i))
        send_far(i, res[chunk(opposite)])
        OWN[i] = res[chunk(x)]
        send_near(i, (res[chunk(right)], res[chunk(left)]))

    def down_far(i):
        arrive(units(DOWN, 4), side_down.at[i])
        hidden = jnp.concatenate([HID[t, chunk(opposite)] for t in range(11)], axis=1)
        send_far(i, mm(hidden, down_weights(i)))

    def down_near(i):
        hidden = [
            jnp.concatenate([HID[t, chunk(k)] for t in range(11)], axis=1) for k in (x, right, left)
        ]
        near = mm(jnp.concatenate(hidden, axis=0), down_weights(i))
        OWN[i] = near[:128]
        send_near(i, (near[128:256], near[256:]))

    def hand_on(i):
        arrive(OPPR.at[i], opp_recv.at[i])
        for half in (0, 1):
            NBS[i, half, half] = (PN[half, i] + OPPR[i, half].astype(F32)).astype(BF16)
            send_half(i, half, half)

    def finish(i):
        arrive(NBR.at[i], nb_recv.at[i])
        for half in (0, 1):
            column = column_of(2 * i + half)
            lanes = pl.ds(pl.multiple_of(lax.rem(column, 2) * 128, 128), 128)
            stream = STREAM[column // 2, chunk(x), lanes].astype(F32)
            summed = OWN[i, :, half * 128 : (half + 1) * 128]
            summed = summed + NBR[i, 0, half].astype(F32) + NBR[i, 1, half].astype(F32)
            columns = pl.ds(pl.multiple_of(column * 128, 128), 128)
            out_ref[:, columns] = (stream + summed).astype(BF16)

    await_sides(0)
    gate_up((0, (0, -1), (-1, -1), (1, -1), (0, 1), (-1, 1), (1, 1), (0, 2)), True, False, 0, 3)
    stage(GU, 6)
    gate_up((0, (0, -1), (-1, -1), (1, -1), (0, 1), (-1, 1), (1, 1), (0, 2)), True, False, 3, 6)
    stage(DOWN, 2)
    await_sides(1)
    gate_up(((2, -1), (2, 1), (-1, 2), (1, 2)), False, False, 0, 3)
    stage(GU, 7)
    stage(DOWN, 3)
    gate_up(((2, -1), (2, 1), (-1, 2), (1, 2)), False, False, 3, 6)
    await_sides(2)
    gate_up(((2, 2),), False, True, chunks=(2,))
    down_far(0)
    down_far(1)
    stage(DOWN, 4)
    gate_up(((2, 2),), False, True, chunks=(0, 1, -1))
    down_near(0)
    stage(DOWN, 5)
    down_near(1)
    hand_on(0)
    stage(DOWN, 8)
    down(2)
    down(3)
    hand_on(1)
    down(4)
    stage(DOWN, 6)
    hand_on(2)
    down(5)
    hand_on(3)
    down(6)
    stage(DOWN, 7)
    hand_on(4)
    down(7)
    hand_on(5)
    finish(0)
    hand_on(6)
    finish(1)
    finish(2)
    hand_on(7)
    finish(3)
    finish(4)
    finish(5)
    finish(6)
    finish(7)

    for kind in (GU, DOWN):
        arrive(units(kind, counts[kind] // 2), w_send.at[kind])
    arrive(STR.at[pl.ds(0, 3)], state_send.at[0])
    arrive(SK.at[pl.ds(0, 3)], skip_send.at[0])
    arrive(MX.at[pl.ds(0, 7)], mix_send.at[0])
    arrive(OPPS, opp_send.at[0])
    arrive(NBS, nb_send.at[0])
    for k in range(1, 4):

        @pl.when(z + k < 4)
        def _():
            total_copy(k).wait_send()


def on_device(skip, q, r, v, e, slack, surge, gain, emission, norm_gain, gate, up, down):
    vmem = pl.BlockSpec(memory_space=pltpu.VMEM)
    dma = pltpu.SemaphoreType.DMA
    return pl.pallas_call(
        kernel,
        out_shape=jax.ShapeDtypeStruct((128, D), BF16),
        in_specs=[pl.BlockSpec(memory_space=pltpu.HBM)] * 13,
        out_specs=vmem,
        scratch_shapes=[
            pltpu.VMEM((128, D), BF16),
            pltpu.VMEM((2, TOK, HD), BF16),
            pltpu.VMEM((2, TOK, HD), BF16),
            pltpu.VMEM((1, HD), F32),
            pltpu.VMEM((TOK, HD), F32),
            pltpu.VMEM((1, HD), F32),
            pltpu.VMEM((1, D), F32),
            pltpu.VMEM((3, 704, 128), BF16),
            pltpu.VMEM((2 * D, 1408), BF16),
            pltpu.VMEM((32, 704, 128), BF16),
            pltpu.VMEM((8, 1024, 256), BF16),
            pltpu.VMEM((4, 128, D), BF16),
            pltpu.VMEM((8, ROWS, 128), BF16),
            pltpu.VMEM((2, ROWS, 128), BF16),
            pltpu.VMEM((8, ROWS, 256), BF16),
            pltpu.VMEM((8, ROWS, 256), BF16),
            pltpu.VMEM((11, ROWS, 256), F32),
            pltpu.VMEM((11, ROWS, 128), BF16),
            pltpu.VMEM((ROWS, 128), F32),
            pltpu.VMEM((2, ROWS, 256), F32),
            pltpu.VMEM((TOK, HD), F32),
            pltpu.VMEM((TOK, HD), F32),
            pltpu.VMEM((16, HD, HD), F32),
            pltpu.VMEM((16, HD, HD), BF16),
            pltpu.VMEM((4, 144, HD), BF16),
            pltpu.VMEM((4, 144, HD), BF16),
            pltpu.VMEM((TOK, HD), F32),
            pltpu.VMEM((TOK, HD), BF16),
            pltpu.VMEM((TOK, HD), F32),
            pltpu.VMEM((8, 2, 128, 128), BF16),
            pltpu.VMEM((8, 2, 128, 128), BF16),
            pltpu.VMEM((8, 128, 256), F32),
            pltpu.VMEM((2, 8, 128, 128), F32),
            pltpu.VMEM((8, 2, 2, 128, 128), BF16),
            pltpu.VMEM((8, 2, 2, 128, 128), BF16),
            dma((2, 10)),
            dma((3,)),
            dma((8,)),
            dma((2,)),
            dma((3,)),
            dma((1,)),
            dma((3,)),
            dma((3,)),
            dma((4,)),
            dma((1,)),
            dma((7,)),
            dma((1,)),
            dma((1,)),
            dma((8,)),
            dma((8,)),
            dma((1,)),
            dma((8,)),
            dma((1,)),
        ],
        compiler_params=pltpu.CompilerParams(
            collective_id=0, has_side_effects=True, vmem_limit_bytes=54000000
        ),
        name="layer",
    )(
        *(
            pltpu.with_memory_space_constraint(a, pltpu.HBM)
            for a in (skip, q, r, v, e, slack.reshape(1, -1), surge, gain.reshape(1, -1), emission,
                      norm_gain.reshape(1, -1), gate.T, up.T, down)
        )
    )


def solution(mesh):
    split = Mesh(mesh.devices.reshape(4, 4, 4, 2), ("z", "y", "x", "c"))
    sp, tp = ("z", "y"), ("x", "c")
    return jax.shard_map(
        on_device,
        mesh=split,
        in_specs=(
            P(sp + tp, None),
            P(sp, tp),
            P(sp, tp),
            P(sp, tp),
            P(sp, tp),
            P(tp),
            P(sp, tp),
            P(tp),
            P(),
            P(),
            P(sp, tp),
            P(sp, tp),
            P(tp, sp),
        ),
        out_specs=P(sp + tp, None),
        check_vma=False,
    )
```

```python
import functools

import jax
import jax.numpy as jnp
from jax import lax
from jax.experimental import pallas as pl
from jax.experimental.pallas import tpu as pltpu
from jax.sharding import Mesh
from jax.sharding import PartitionSpec as P

MESH = pl.DeviceIdType.MESH
F32 = jnp.float32
BF16 = jnp.bfloat16
EPSILON = 1e-06
HD = 128
BLOCK = 64
TOK = 1024
ROWS = 512
D = 2048
GU, DOWN = 0, 1


def wrap(value, n=4):
    return lax.rem(value + n, n)


def nt(a, b):
    return lax.dot_general(a, b, (((1,), (1,)), ((), ())), preferred_element_type=F32)


def tn(a, b):
    return lax.dot_general(a, b, (((0,), (0,)), ((), ())), preferred_element_type=F32)


def mm(a, b):
    return jnp.dot(a, b, preferred_element_type=F32)


def kernel(
    skip_in, q_in, r_in, v_in, e_in, slack_in, surge_in, gain_in, emission_ref,
    norm_gain_in, gate_in, up_in, down_in,
    out_ref,
    skip_ref, QE, RV, slack_ref, surge_ref, gain_ref, norm_gain_ref, OWNED,
    W, DN, EB, SK, MX, MIXS, STREAM, NORM, ACC, HID, SSQ, RES,
    CUM, IG, DS, SB, STR, TOT, OL, QC, GT,
    OPPS, OPPR, OWN, PN, NBS, NBR,
    w_recv, side_gu, side_down, w_send, state_recv, state_send, total_recv, total_send,
    skip_sem, skip_send, mix_recv, mix_send, e_sem, in_sem, opp_recv, opp_send, nb_recv, nb_send,
):
    z, y, x, c = (lax.axis_index(name) for name in ("z", "y", "x", "c"))
    sp = z * 4 + y
    other = 1 - c
    q_ref, e_ref, r_ref, v_ref = QE.at[0], QE.at[1], RV.at[0], RV.at[1]
    gate_ref, up_ref, down_ref = (OWNED.at[i] for i in range(3))

    def arrive(ref, sem):
        pltpu.make_async_copy(ref, ref, sem).wait()

    barrier = pltpu.get_barrier_semaphore()
    for k in range(1, 4):
        pl.semaphore_signal(barrier, inc=1, device_id={"y": wrap(y + k)}, device_id_type=MESH)
        pl.semaphore_signal(barrier, inc=1, device_id={"z": wrap(z + k)}, device_id_type=MESH)
    for step in (1, -1):
        for core in (0, 1):
            pl.semaphore_signal(barrier, inc=1, device_id={"x": wrap(x + step), "c": jnp.int32(core)}, device_id_type=MESH)
    pl.semaphore_signal(barrier, inc=1, device_id={"c": other}, device_id_type=MESH)

    def load(source, target, sem):
        pltpu.make_async_copy(source, target, in_sem.at[sem]).start()

    load(gate_in, gate_ref, 0)
    load(up_in, up_ref, 0)
    load(down_in, down_ref, 0)
    load(r_in, r_ref, 1)
    load(v_in, v_ref, 1)
    load(surge_in, surge_ref, 2)
    load(slack_in, slack_ref, 3)
    load(skip_in, skip_ref, 4)
    load(q_in, q_ref, 5)
    load(e_in, e_ref, 5)
    load(gain_in, gain_ref, 6)
    load(norm_gain_in, norm_gain_ref, 7)

    arrive(OWNED, in_sem.at[0])
    own_rows = pl.ds(pl.multiple_of(c * D + sp * 128, 128), 128)
    for j in range(5):
        W[own_rows, j * 256 : j * 256 + 128] = gate_ref[j * 128 : (j + 1) * 128].T
        W[own_rows, j * 256 + 128 : (j + 1) * 256] = up_ref[j * 128 : (j + 1) * 128].T
    W[own_rows, 1280:1408] = jnp.concatenate([gate_ref[640:704], up_ref[640:704]], axis=0).T
    DN[c * 16 + sp] = down_ref[...]

    pl.semaphore_wait(barrier, 11)

    AXES = {0: ("y", "z"), 1: ("z", "y")}
    ORDER = (
        (0, 0), (1, 0), (-1, 0), (0, 1), (0, -1), (-1, -1), (1, 1), (1, -1),
        (-1, 1), (2, 0), (0, 2), (2, 1), (2, -1), (1, 2), (-1, 2), (2, 2),
    )
    here = {"z": z, "y": y}

    def short(offset):
        return (offset + 1) % 4 - 1

    def unit(kind, color, rel, half):
        origin = wrap(z + rel["z"]) * 4 + wrap(y + rel["y"])
        size, skipped = (1, 0) if half is None else (2, half)
        if kind == GU:
            start = pl.multiple_of(c * D + origin * 128 + color * 64 + skipped * 32, 32)
            return W.at[pl.ds(start, 64 // size), :]
        return DN.at[c * 16 + origin, pl.ds(color * 352 + skipped * 176, 352 // size), :]

    def units(kind, count):
        return W.at[pl.ds(0, 64 * count), :] if kind == GU else DN.at[pl.ds(0, count // 2)]

    counts = {GU: 0, DOWN: 0}

    def lot(color, rel):
        one, two = AXES[color]
        first, second = short(rel[one]), short(rel[two])
        if second == 0:
            return {-1: 0, 1: 1, 2: 3}[first]
        if second == 2:
            return {0: 6, -1: 8, 1: 8, 2: 9}[first]
        return {0: 2, -1: 4, 1: 5, 2: 7}[first]

    LOTS = (2, 2, 4, 2, 4, 4, 2, 4, 4, 2)

    def arrived(kind, number):
        arrive(units(kind, LOTS[number]), w_recv.at[kind, number])

    def start_unit(kind, color, rel, recv_sem, device, half=None):
        ref = unit(kind, color, rel, half)
        pltpu.make_async_remote_copy(
            src_ref=ref, dst_ref=ref, send_sem=w_send.at[kind], recv_sem=recv_sem,
            device_id=device, device_id_type=MESH,
        ).start()
        counts[kind] += 2 if half is None else 1

    def push(kind, color, rel, axis, step, half=None):
        there = dict(rel)
        there[axis] = rel[axis] - step
        sem = w_recv.at[kind, lot(color, there)]
        start_unit(kind, color, rel, sem, {axis: wrap(here[axis] + step)}, half)

    def side(kind, color, rel):
        place = (short(rel["y"]), short(rel["z"]))
        if kind == GU:
            late = (place[0] == 2) + (place[1] == 2)
            sem = side_gu.at[1 if late == 1 and 0 not in place else late if 0 not in place else 0]
        else:
            sem = side_down.at[ORDER.index(place) // 2]
        start_unit(kind, color, rel, sem, {"c": other})

    def at(color, first, second):
        one, two = AXES[color]
        return {one: first, two: second}

    def stage(kind, n):
        if n in (0, 1):
            for color in (0, 1):
                for step in (1, -1):
                    push(kind, color, at(color, 0, 0), AXES[color][n], step)
                if n == 1:
                    side(kind, color, at(color, 0, 0))
        if n == 2:
            arrived(kind, 0)
            arrived(kind, 1)
            for f in (-1, 1):
                for color in (0, 1):
                    push(kind, color, at(color, f, 0), AXES[color][0], -f, (f + 1) // 2)
        if n == 4:
            arrived(kind, 3)
        for f in {2: (-1, 1), 4: (2,)}.get(n, ()):
            for color in (0, 1):
                for step in (1, -1):
                    push(kind, color, at(color, f, 0), AXES[color][1], step)
                side(kind, color, at(color, f, 0))
        for number, first in {3: ((2, 0),), 5: ((4, -1),), 8: ((5, 1),), 6: ((7, 2),)}.get(n, ()):
            arrived(kind, number)
            for s in (-1, 1):
                for color in (0, 1):
                    push(kind, color, at(color, first, s), AXES[color][1], -s, (s + 1) // 2)
            for s in (-1, 1):
                for color in (0, 1):
                    side(kind, color, at(color, first, s))
        for number, firsts in {8: ((6, (0,)),), 6: ((8, (-1, 1)),), 7: ((9, (2,)),)}.get(n, ()):
            arrived(kind, number)
            for first in firsts:
                for color in (0, 1):
                    side(kind, color, at(color, first, 2))

    own = at(0, 0, 0)
    for step in (1, -1):
        push(GU, 0, own, "y", step, 0)
        push(GU, 1, own, "z", step)

    def skip_copy(source, slot, rows, sem, step):
        return pltpu.make_async_remote_copy(
            src_ref=source, dst_ref=SK.at[slot, rows, :],
            send_sem=skip_send.at[0], recv_sem=skip_sem.at[sem],
            device_id={"x": wrap(x + step)}, device_id_type=MESH,
        )

    arrive(skip_ref, in_sem.at[4])
    for i, step in enumerate((1, -1)):
        skip_copy(skip_ref, x, pl.ds(0, 128), i, step).start()

    def skip_arrived(slot, rows, sem):
        arrive(SK.at[slot, rows, :], skip_sem.at[sem])

    def skip_relay(part):
        left, right = wrap(x - 1), wrap(x + 1)
        first, second = pl.ds(part * 32, 32), pl.ds(64 + part * 32, 32)
        if part == 0:
            skip_arrived(left, pl.ds(0, 128), 0)
            skip_arrived(right, pl.ds(0, 128), 1)
        skip_copy(SK.at[left, first, :], left, first, 2 + part, 1).start()
        skip_copy(SK.at[right, second, :], right, second, 2 + part, -1).start()

    i256 = lax.broadcasted_iota(jnp.int32, (256, 256), 0)
    j256 = lax.broadcasted_iota(jnp.int32, (256, 256), 1)
    causal = jnp.logical_and(i256 >= j256, i256 // BLOCK == j256 // BLOCK)
    triangle = jnp.where(causal, 1.0, 0.0).astype(BF16)
    upper_half = lax.broadcasted_iota(jnp.int32, (128, 128), 0) < BLOCK
    arrive(RV, in_sem.at[1])
    arrive(surge_ref, in_sem.at[2])
    arrive(slack_ref, in_sem.at[3])
    closings = []
    for s in range(4):
        rows = slice(s * 256, (s + 1) * 256)
        ig = slack_ref[...] * jax.nn.sigmoid(-r_ref[rows].astype(F32))
        lf = jnp.log1p(-ig) + surge_ref[rows]
        high = lf.astype(BF16)
        rest = lf - high.astype(F32)
        mid = rest.astype(BF16)
        low = (rest - mid.astype(F32)).astype(BF16)
        parts = mm(triangle, jnp.concatenate([high, mid, low], axis=1))
        cum = parts[:, :128] + parts[:, 128:256] + parts[:, 256:]
        CUM[rows] = cum
        IG[rows] = ig
        blocks = cum.reshape(4, BLOCK, HD)
        last = blocks[:, BLOCK - 1 : BLOCK, :]
        closings += [last[b] for b in range(4)]
        keys = (ig * jnp.exp(last - blocks).reshape(256, HD)).astype(BF16)
        for p in range(2):
            pair = keys[p * 128 : (p + 1) * 128]
            none = jnp.zeros_like(pair)
            both = jnp.concatenate(
                [jnp.where(upper_half, pair, none), jnp.where(upper_half, none, pair)], axis=1
            )
            grown = tn(v_ref[s * 256 + p * 128 : s * 256 + (p + 1) * 128], both)
            DS[s * 4 + p * 2] = grown[:, :128]
            DS[s * 4 + p * 2 + 1] = grown[:, 128:]
    state = jnp.zeros((HD, HD), F32)
    passed = jnp.zeros((1, HD), F32)
    offsets = []
    for b in range(16):
        SB[b] = state.astype(BF16)
        offsets.append(passed)
        state = state * jnp.exp(closings[b]) + DS[b]
        passed = passed + closings[b]
    STR[0, 0:128] = state.astype(BF16)
    which = lax.broadcasted_iota(jnp.int32, (16, HD), 0)

    def spread(value):
        high = value.astype(BF16)
        rest = value - high.astype(F32)
        mid = rest.astype(BF16)
        low = rest - mid.astype(F32)
        rows = jnp.where(which == 2, low, 0.0)
        rows = jnp.where(which == 1, mid.astype(F32), rows)
        return jnp.where(which == 0, high.astype(F32), rows).astype(BF16)

    def joined(rows):
        rows = rows.astype(F32)
        return rows[0:1] + rows[1:2] + rows[2:3]

    STR[0, 128:144] = spread(passed)

    for k in range(1, 4):
        pltpu.make_async_remote_copy(
            src_ref=STR.at[0], dst_ref=STR.at[k],
            send_sem=state_send.at[0], recv_sem=state_recv.at[k - 1],
            device_id={"y": wrap(y + k)}, device_id_type=MESH,
        ).start()

    for n in range(8):
        source = emission_ref.at[:, pl.ds(n * 256, 256)]
        pltpu.make_async_copy(source, EB.at[n], e_sem.at[0]).start()
    for step in (1, -1):
        push(GU, 0, own, "y", step, 1)
        push(GU, 1, own, "y", step)
        push(GU, 0, own, "z", step, 0)
    SK[x] = skip_ref[...]
    arrive(QE, in_sem.at[5])
    arrive(gain_ref, in_sem.at[6])
    arrive(norm_gain_ref, in_sem.at[7])
    for s in range(4):
        rows = slice(s * 256, (s + 1) * 256)
        q = q_ref[rows].astype(F32)
        qa = q * jax.nn.sigmoid(q)
        cum = CUM[rows]
        ig = IG[rows]
        blocks = cum.reshape(4, BLOCK, HD)
        middle = blocks[:, BLOCK // 2 : BLOCK // 2 + 1, :]
        centred = (blocks - middle).reshape(256, HD)
        left = (qa * jnp.exp(centred)).astype(BF16)
        right = (ig * jnp.exp(-centred)).astype(BF16)
        scores = jnp.where(causal, nt(left, right), 0.0).astype(BF16)
        local = mm(scores, v_ref[rows])
        faded = qa * jnp.exp(cum)
        faded_by = jnp.concatenate([offsets[s * 4 + b].reshape(1, 1, HD) for b in range(4)], axis=0)
        QC[rows] = (qa * jnp.exp(blocks + faded_by).reshape(256, HD)).astype(BF16)
        faded = faded.astype(BF16)
        for p in range(2):
            pair = faded[p * 128 : (p + 1) * 128]
            none = jnp.zeros_like(pair)
            both = jnp.concatenate(
                [jnp.where(upper_half, pair, none), jnp.where(upper_half, none, pair)], axis=1
            )
            b = s * 4 + p * 2
            carried = nt(both, jnp.concatenate([SB[b], SB[b + 1]], axis=1))
            OL[s * 256 + p * 128 : s * 256 + (p + 1) * 128] = local[p * 128 : (p + 1) * 128] + carried
        emission = e_ref[rows].astype(F32)
        GT[rows] = gain_ref[...] * emission * jax.nn.sigmoid(emission)

    for k in range(1, 4):
        arrive(STR.at[k], state_recv.at[k - 1])
    plane = jnp.zeros((HD, HD), F32)
    plane_log = jnp.zeros((1, HD), F32)
    before, before_log = plane, plane_log
    for yy in range(4):
        slot = wrap(y - yy)
        before = jnp.where(y == yy, plane, before)
        before_log = jnp.where(y == yy, plane_log, before_log)
        log = joined(STR[slot, 128:144])
        plane = plane * jnp.exp(log) + STR[slot, 0:128].astype(F32)
        plane_log = plane_log + log
    TOT[0, 0:128] = plane.astype(BF16)
    TOT[0, 128:144] = spread(plane_log)

    def total_copy(k):
        return pltpu.make_async_remote_copy(
            src_ref=TOT.at[0], dst_ref=TOT.at[k],
            send_sem=total_send.at[k - 1], recv_sem=total_recv.at[k - 1],
            device_id={"z": wrap(z + k)}, device_id_type=MESH,
        )

    for k in range(1, 4):

        @pl.when(z + k < 4)
        def _():
            total_copy(k).start()

        @pl.when(z < k)
        def _():
            TOT[k] = jnp.zeros((144, HD), BF16)

    for step in (1, -1):
        push(GU, 0, own, "z", step, 1)
    for color in (0, 1):
        side(GU, color, own)
    stage(GU, 2)
    for k in range(1, 4):

        @pl.when(z >= k)
        def _():
            arrive(TOT.at[k], total_recv.at[k - 1])

    since = before_log
    for k in range(1, 4):
        before = before + TOT[k, 0:128].astype(F32) * jnp.exp(since)
        since = since + joined(TOT[k, 128:144])
    incoming = before.astype(BF16)
    for s in range(4):
        rows = slice(s * 256, (s + 1) * 256)
        o = OL[rows] + nt(QC[rows], incoming)
        squares = jnp.mean(o * o, axis=-1, keepdims=True)
        mixed = (o * lax.rsqrt(squares + EPSILON) * GT[rows]).astype(BF16)
        for core in (0, 1):
            MIXS[core, s * 128 : (s + 1) * 128] = mixed[core * 128 : (core + 1) * 128]

    head = x * 2 + c
    MX[head] = MIXS[c]

    def mix_copy(source, slab, sem, device):
        pltpu.make_async_remote_copy(
            src_ref=source, dst_ref=MX.at[slab],
            send_sem=mix_send.at[0], recv_sem=mix_recv.at[sem],
            device_id=device, device_id_type=MESH,
        ).start()

    for i, step in enumerate((1, -1)):
        for core in (0, 1):
            mix_copy(MIXS.at[core], head, i * 2 + c, {"x": wrap(x + step), "c": jnp.int32(core)})
    mix_copy(MIXS.at[other], head, 4, {"c": other})

    def mix_arrived(slab, sem):
        arrive(MX.at[slab], mix_recv.at[sem])

    stage(GU, 3)
    skip_relay(0)
    stage(GU, 4)
    left, right = wrap(x - 1), wrap(x + 1)
    mix_arrived(left * 2, 0)
    mix_copy(MX.at[left * 2], left * 2, 5, {"x": right})
    mix_arrived(right * 2 + 1, 3)
    mix_copy(MX.at[right * 2 + 1], right * 2 + 1, 6, {"x": left})
    skip_relay(1)
    stage(GU, 5)
    stage(GU, 8)
    stage(DOWN, 0)
    stage(DOWN, 1)
    arrive(EB, e_sem.at[0])
    opposite = wrap(x + 2)
    mix_arrived(left * 2 + 1, 1)
    mix_arrived(right * 2, 2)
    mix_arrived(x * 2 + other, 4)
    mix_arrived(opposite * 2, 5)
    mix_arrived(opposite * 2 + 1, 6)

    def project(n, carry):
        mixed = jnp.concatenate([MX[h] for h in range(8)], axis=1)
        ACC[n] = mm(mixed, EB[n])
        return carry

    lax.fori_loop(0, 4, project, 0, unroll=True)
    lax.fori_loop(4, 8, project, 0, unroll=True)
    skip_arrived(opposite, pl.ds(0, 64), 2)
    skip_arrived(opposite, pl.ds(64, 64), 3)
    SSQ[...] = jnp.zeros((ROWS, 128), F32)

    def add(n, carry):
        skipped = SK[:, :, pl.ds(pl.multiple_of(n * 256, 256), 256)].reshape(ROWS, 256)
        stream = (skipped.astype(F32) + ACC[n]).astype(BF16)
        STREAM[n] = stream
        wide = stream.astype(F32)
        wide = wide * wide
        SSQ[...] += wide[:, :128] + wide[:, 128:]
        return carry

    lax.fori_loop(0, 8, add, 0)
    scale = lax.rsqrt(jnp.sum(SSQ[...], axis=1, keepdims=True) * (1.0 / D) + EPSILON)

    for n in range(8):
        gain = norm_gain_ref[:, n * 256 : (n + 1) * 256]
        NORM[n] = (STREAM[n].astype(F32) * scale * gain).astype(BF16)

    def await_sides(group):
        arrive(units(GU, (22, 8, 2)[group]), side_gu.at[group])

    def chunk(xi):
        return pl.ds(pl.multiple_of(xi * 128, 128), 128)

    def silu(a):
        return a * jax.nn.sigmoid(a)

    def gate_up(planes, first, last, begin=0, end=6, chunks=(0, 1, 2, 3)):
        tiles, rows = [], ([], [])
        for part in planes:
            if isinstance(part, int):
                place = wrap(z + part)
                tiles += [(place * 2, slice(None)), (place * 2 + 1, slice(None))]
                start, size = place * 512, 512
            else:
                place = wrap(z + part[1]) * 4 + wrap(y + part[0])
                lanes = pl.ds(pl.multiple_of(lax.rem(place, 2) * 128, 128), 128)
                tiles.append((place // 2, lanes))
                start, size = place * 128, 128
            for h in (0, 1):
                rows[h].append(pl.ds(pl.multiple_of(h * D + start, 128), size))

        def some(ref, t, lanes=slice(None)):
            if len(chunks) == 4:
                return ref[t, :, lanes]
            return jnp.concatenate([ref[t, chunk(wrap(x + k)), lanes] for k in chunks], axis=0)

        def put(ref, t, value):
            if len(chunks) == 4:
                ref[t] = value
                return
            for n, k in enumerate(chunks):
                ref[t, chunk(wrap(x + k))] = value[n * 128 : (n + 1) * 128]

        def partial(weights):
            normed = [some(NORM, t, lanes) for t, lanes in tiles]
            return mm(jnp.concatenate(normed, axis=1), jnp.concatenate(weights, axis=0))

        def tile(j, carry):
            columns = pl.ds(pl.multiple_of(j * 256, 256), 256)
            for h in (0, 1):
                t = h * 5 + j
                part = partial([W[deep, columns] for deep in rows[h]])
                if not first:
                    part = part + some(ACC, t)
                if not last:
                    put(ACC, t, part)
                else:
                    put(HID, t, (silu(part[:, :128]) * part[:, 128:]).astype(BF16))
            return carry

        lax.fori_loop(begin, min(end, 5), tile, 0, unroll=True)
        if end < 6:
            return
        part = partial(
            [
                jnp.concatenate([W[one, 1280:1408], W[two, 1280:1408]], axis=1)
                for one, two in zip(*rows)
            ]
        )
        if not first:
            part = part + some(ACC, 10)
        if not last:
            put(ACC, 10, part)
        else:
            lane = lax.broadcasted_iota(jnp.int32, (128 * len(chunks), 128), 1)
            a, b = part[:, :128], part[:, 128:]
            gates = jnp.where(lane < 64, a, pltpu.roll(b, 64, 1))
            ups = jnp.where(lane < 64, pltpu.roll(a, 64, 1), b)
            put(HID, 10, (silu(gates) * ups).astype(BF16))

    def column_of(i):
        dy, dz = ORDER[i]
        return wrap(z + dz) * 4 + wrap(y + dy)

    def down_weights(i):
        def block(at_column):
            one, two = at_column, 16 + at_column
            return jnp.concatenate(
                [DN[one, 0:640], DN[two, 0:640], DN[one, 640:704], DN[two, 640:704]], axis=0
            )

        return jnp.concatenate([block(column_of(2 * i)), block(column_of(2 * i + 1))], axis=1)

    def send_far(i, far):
        for half, step in enumerate((1, -1)):
            OPPS[i, half] = far[:, half * 128 : (half + 1) * 128].astype(BF16)
            pltpu.make_async_remote_copy(
                src_ref=OPPS.at[i, half], dst_ref=OPPR.at[i, half],
                send_sem=opp_send.at[0], recv_sem=opp_recv.at[i],
                device_id={"x": wrap(x + step)}, device_id_type=MESH,
            ).start()

    def send_half(i, half, columns):
        pltpu.make_async_remote_copy(
            src_ref=NBS.at[i, half, columns], dst_ref=NBR.at[i, half, columns],
            send_sem=nb_send.at[0], recv_sem=nb_recv.at[i],
            device_id={"x": wrap(x + 1 - 2 * half)}, device_id_type=MESH,
        ).start()

    def send_near(i, near):
        for half in (0, 1):
            rest = 1 - half
            NBS[i, half, rest] = near[half][:, rest * 128 : (rest + 1) * 128].astype(BF16)
            send_half(i, half, rest)
            PN[half, i] = near[half][:, half * 128 : (half + 1) * 128]

    def down(i):
        arrive(units(DOWN, 4), side_down.at[i])
        res = RES.at[i % 2]
        res[...] = mm(jnp.concatenate([HID[t] for t in range(11)], axis=1), down_weights(i))
        send_far(i, res[chunk(opposite)])
        OWN[i] = res[chunk(x)]
        send_near(i, (res[chunk(right)], res[chunk(left)]))

    def down_far(i):
        arrive(units(DOWN, 4), side_down.at[i])
        hidden = jnp.concatenate([HID[t, chunk(opposite)] for t in range(11)], axis=1)
        send_far(i, mm(hidden, down_weights(i)))

    def down_near(i):
        hidden = [
            jnp.concatenate([HID[t, chunk(k)] for t in range(11)], axis=1) for k in (x, right, left)
        ]
        near = mm(jnp.concatenate(hidden, axis=0), down_weights(i))
        OWN[i] = near[:128]
        send_near(i, (near[128:256], near[256:]))

    def hand_on(i):
        arrive(OPPR.at[i], opp_recv.at[i])
        for half in (0, 1):
            NBS[i, half, half] = (PN[half, i] + OPPR[i, half].astype(F32)).astype(BF16)
            send_half(i, half, half)

    def finish(i):
        arrive(NBR.at[i], nb_recv.at[i])
        for half in (0, 1):
            column = column_of(2 * i + half)
            lanes = pl.ds(pl.multiple_of(lax.rem(column, 2) * 128, 128), 128)
            stream = STREAM[column // 2, chunk(x), lanes].astype(F32)
            summed = OWN[i, :, half * 128 : (half + 1) * 128]
            summed = summed + NBR[i, 0, half].astype(F32) + NBR[i, 1, half].astype(F32)
            columns = pl.ds(pl.multiple_of(column * 128, 128), 128)
            out_ref[:, columns] = (stream + summed).astype(BF16)

    await_sides(0)
    gate_up((0, (0, -1), (-1, -1), (1, -1), (0, 1), (-1, 1), (1, 1), (0, 2)), True, False, 0, 3)
    stage(GU, 6)
    gate_up((0, (0, -1), (-1, -1), (1, -1), (0, 1), (-1, 1), (1, 1), (0, 2)), True, False, 3, 6)
    stage(DOWN, 2)
    await_sides(1)
    gate_up(((2, -1), (2, 1), (-1, 2), (1, 2)), False, False, 0, 3)
    stage(GU, 7)
    stage(DOWN, 3)
    gate_up(((2, -1), (2, 1), (-1, 2), (1, 2)), False, False, 3, 6)
    await_sides(2)
    gate_up(((2, 2),), False, True, chunks=(2,))
    down_far(0)
    down_far(1)
    stage(DOWN, 4)
    gate_up(((2, 2),), False, True, chunks=(0, 1, -1))
    down_near(0)
    stage(DOWN, 5)
    down_near(1)
    hand_on(0)
    stage(DOWN, 8)
    down(2)
    down(3)
    down(4)
    hand_on(1)
    stage(DOWN, 6)
    hand_on(2)
    down(5)
    hand_on(3)
    down(6)
    stage(DOWN, 7)
    down(7)
    hand_on(4)
    hand_on(5)
    finish(0)
    hand_on(6)
    finish(1)
    finish(2)
    hand_on(7)
    finish(3)
    finish(4)
    finish(5)
    finish(6)
    finish(7)

    for kind in (GU, DOWN):
        arrive(units(kind, counts[kind] // 2), w_send.at[kind])
    arrive(STR.at[pl.ds(0, 3)], state_send.at[0])
    arrive(SK.at[pl.ds(0, 3)], skip_send.at[0])
    arrive(MX.at[pl.ds(0, 7)], mix_send.at[0])
    arrive(OPPS, opp_send.at[0])
    arrive(NBS, nb_send.at[0])
    for k in range(1, 4):

        @pl.when(z + k < 4)
        def _():
            total_copy(k).wait_send()


def on_device(skip, q, r, v, e, slack, surge, gain, emission, norm_gain, gate, up, down):
    vmem = pl.BlockSpec(memory_space=pltpu.VMEM)
    dma = pltpu.SemaphoreType.DMA
    return pl.pallas_call(
        kernel,
        out_shape=jax.ShapeDtypeStruct((128, D), BF16),
        in_specs=[pl.BlockSpec(memory_space=pltpu.HBM)] * 13,
        out_specs=vmem,
        scratch_shapes=[
            pltpu.VMEM((128, D), BF16),
            pltpu.VMEM((2, TOK, HD), BF16),
            pltpu.VMEM((2, TOK, HD), BF16),
            pltpu.VMEM((1, HD), F32),
            pltpu.VMEM((TOK, HD), F32),
            pltpu.VMEM((1, HD), F32),
            pltpu.VMEM((1, D), F32),
            pltpu.VMEM((3, 704, 128), BF16),
            pltpu.VMEM((2 * D, 1408), BF16),
            pltpu.VMEM((32, 704, 128), BF16),
            pltpu.VMEM((8, 1024, 256), BF16),
            pltpu.VMEM((4, 128, D), BF16),
            pltpu.VMEM((8, ROWS, 128), BF16),
            pltpu.VMEM((2, ROWS, 128), BF16),
            pltpu.VMEM((8, ROWS, 256), BF16),
            pltpu.VMEM((8, ROWS, 256), BF16),
            pltpu.VMEM((11, ROWS, 256), F32),
            pltpu.VMEM((11, ROWS, 128), BF16),
            pltpu.VMEM((ROWS, 128), F32),
            pltpu.VMEM((2, ROWS, 256), F32),
            pltpu.VMEM((TOK, HD), F32),
            pltpu.VMEM((TOK, HD), F32),
            pltpu.VMEM((16, HD, HD), F32),
            pltpu.VMEM((16, HD, HD), BF16),
            pltpu.VMEM((4, 144, HD), BF16),
            pltpu.VMEM((4, 144, HD), BF16),
            pltpu.VMEM((TOK, HD), F32),
            pltpu.VMEM((TOK, HD), BF16),
            pltpu.VMEM((TOK, HD), F32),
            pltpu.VMEM((8, 2, 128, 128), BF16),
            pltpu.VMEM((8, 2, 128, 128), BF16),
            pltpu.VMEM((8, 128, 256), F32),
            pltpu.VMEM((2, 8, 128, 128), F32),
            pltpu.VMEM((8, 2, 2, 128, 128), BF16),
            pltpu.VMEM((8, 2, 2, 128, 128), BF16),
            dma((2, 10)),
            dma((3,)),
            dma((8,)),
            dma((2,)),
            dma((3,)),
            dma((1,)),
            dma((3,)),
            dma((3,)),
            dma((4,)),
            dma((1,)),
            dma((7,)),
            dma((1,)),
            dma((1,)),
            dma((8,)),
            dma((8,)),
            dma((1,)),
            dma((8,)),
            dma((1,)),
        ],
        compiler_params=pltpu.CompilerParams(
            collective_id=0, has_side_effects=True, vmem_limit_bytes=54000000
        ),
        name="layer",
    )(
        *(
            pltpu.with_memory_space_constraint(a, pltpu.HBM)
            for a in (skip, q, r, v, e, slack.reshape(1, -1), surge, gain.reshape(1, -1), emission,
                      norm_gain.reshape(1, -1), gate.T, up.T, down)
        )
    )


def solution(mesh):
    split = Mesh(mesh.devices.reshape(4, 4, 4, 2), ("z", "y", "x", "c"))
    sp, tp = ("z", "y"), ("x", "c")
    return jax.shard_map(
        on_device,
        mesh=split,
        in_specs=(
            P(sp + tp, None),
            P(sp, tp),
            P(sp, tp),
            P(sp, tp),
            P(sp, tp),
            P(tp),
            P(sp, tp),
            P(tp),
            P(),
            P(),
            P(sp, tp),
            P(sp, tp),
            P(tp, sp),
        ),
        out_specs=P(sp + tp, None),
        check_vma=False,
    )
```
